32 devices in a mesh: grp: 2 (over y), sp: 8 (over z, core), tp: 2 (over x).
Axes of the slice: x: 2, y: 2, z: 4, core: 2. Of those that a mesh axis runs over, the one named last changes fastest.
Arguments:
- query_plain: bfloat16 [2560, 1024], P(('grp', 'sp'), 'tp'), parts along dimension 0, may hold values from -6 to 6
- query_turn: bfloat16 [2560, 512], P(('grp', 'sp'), 'tp'), parts along dimension 0, may hold values from -40 to 40, as said below
- latent: bfloat16 [2560, 512], P(('grp', 'sp')), parts along dimension 0, may hold values from -6 to 6
- key_turn: bfloat16 [2560, 64], P(('grp', 'sp')), parts along dimension 0, may hold values from -40 to 40, as said below
- latent_norm_scale: bfloat16 [512], replicated, may hold values from 0.099609375 to 1.8984375
- plain_key_matrix: bfloat16 [512, 1024], P(None, 'tp'), may hold values from -0.25 to 0.25
- value_matrix: bfloat16 [512, 1024], P(None, 'tp'), may hold values from -0.25 to 0.25
- residual: bfloat16 [2560, 2048], P(('grp', 'sp', 'tp')), parts along dimension 0, may hold values from -6 to 6
- out_weight: bfloat16 [1024, 2048], replicated, may hold values from -6 to 6
- ffn_gain: bfloat16 [2048], replicated, may hold values from 0.099609375 to 1.8984375
- gate_weight: bfloat16 [8, 2048, 1024], P('sp', None, 'tp'), may hold values from -1 to 1
- up_weight: bfloat16 [8, 2048, 1024], P('sp', None, 'tp'), may hold values from -1 to 1
- down_weight: bfloat16 [8, 1024, 2048], P('sp', 'tp'), may hold values from -0.0625 to 0.0625
- routes: int32 [2560, 4], P(('grp', 'sp', 'tp')), parts along dimension 0, may hold values from 0 to 7, all different within a row; in each aligned block of 80 rows (0 to 79, 80 to 159, ...) at most 60 rows name the same one
- route_weights: float32 [2560, 4], P(('grp', 'sp', 'tp')), parts along dimension 0, may hold values from 0.1 to 0.6
Outputs:
- mixed: bfloat16 [2560, 2048], P(('grp', 'sp', 'tp')), parts along dimension 0
The draws below stay inside these ranges and needn't reach their ends.
There are 2 independent parts, one for each index of `grp`. The reference program is written for one: setup_inputs(seed, part) draws one part's arguments, and reference() takes and returns one part's arrays. A program takes and returns all parts, laid end to end along the dimension named above; an argument that names none is the same for every part. Nothing has to cross between parts.
Inputs may be any that keep to these rules, and one draw needn't show every extreme that they name: `query_turn`: in the hidden draw some rows are large. `key_turn`: in the hidden draw some rows are large. `routes`: each row names 4 different experts. In each aligned block of 80 rows (the rows of one device) no expert is named more than 60 times, a bound that some block reaches.
All inputs are finite; a program needn't handle non-finite values.
Results may differ from the reference program's by a relative error of at most 0.015.
Values may be sent and summed in bfloat16 or wider, within the bound.
A program may use at most 128 MiB of HBM per device.

```python
import math
import jax
import jax.numpy as jnp
import numpy as np
from jax import lax

D = 2048
ATTENTION_HEADS = 8
PLAIN_HEAD_WIDTH = 128
QK_ROPE = 64
VALUE_WIDTH = 128
LATENT_WIDTH = 512
D_EXPERT = 1024
TOP = 4
GRID_W = 64
ROWS_DEV = 80
SEQUENCE_TOKENS = 1280
EXPERTS = 8
CAP = 60
N_SP = 8
N_TP = 2


def draw_query_turn(key, part):
    base = jnp.clip(jax.random.normal(jax.random.fold_in(key, 1), (SEQUENCE_TOKENS, ATTENTION_HEADS * QK_ROPE), jnp.float32), -6.0, 6.0)
    return base.astype(jnp.bfloat16)


def draw_key_turn(key, part):
    base = jnp.clip(jax.random.normal(jax.random.fold_in(key, 2), (SEQUENCE_TOKENS, QK_ROPE), jnp.float32), -6.0, 6.0)
    return base.astype(jnp.bfloat16)


def block_scale(own_key, extent, cuts, least, high):
    loudness, own = 1.0, jax.random.fold_in(own_key, 6)
    for dim, shards_of in cuts:
        steps = jnp.exp(jax.random.uniform(jax.random.fold_in(own, dim), (shards_of,), jnp.float32, least / len(cuts), high / len(cuts)))
        loudness = loudness * jnp.repeat(steps, extent[dim] // shards_of).reshape([-1 if axis == dim else 1 for axis in range(len(extent))])
    return loudness


def shared_out(stream_key, own, number, rows, count, top, reach, skew):
    ranking = jax.random.permutation(stream_key, count)
    crowded, common = shares(count, rows * top, reach, skew, True), shares(count, rows * top, reach, skew, False)
    places = jnp.arange(count)

    def named(sizes, offset_by):
        used = int((sizes > 0).sum())
        fixed = max(1, used // 4)
        passed = fixed + (places - fixed + offset_by * (used - fixed)) % max(1, count - fixed)
        return jnp.zeros((count,), jnp.int32).at[ranking[jnp.where(places < fixed, places, passed)]].set(jnp.asarray(sizes, jnp.int32))

    sizes = jnp.where(number % 4 == 0, named(crowded, number // 4), named(common, number - number // 4 - 1))
    mixed = jax.random.permutation(jax.random.fold_in(own, 3), count)
    source_of, sink = mixed[0:count // 2 * 2:2], mixed[1:count // 2 * 2:2]
    slack = jnp.minimum(sizes[source_of] - 1, reach - sizes[sink]) // 2
    slack = jnp.where((source_of == ranking[0]) | (sink == ranking[0]) | (sizes[sink] == 0), 0, jnp.maximum(slack, 0))
    passed = jax.random.randint(jax.random.fold_in(own, 4), (count // 2,), 0, 1 << 20) % (slack + 1)
    sizes = sizes.at[source_of].add(-passed).at[sink].add(passed)
    members = jnp.searchsorted(jnp.cumsum(sizes), jnp.arange(rows * top), side="right").astype(jnp.int32)
    grid = members.reshape(top, rows).T
    grid = grid[jax.random.permutation(jax.random.fold_in(own, 1), rows)]
    offset_by = jax.random.randint(jax.random.fold_in(own, 2), (rows, 1), 0, top)
    return jnp.take_along_axis(grid, (jnp.arange(top)[None, :] + offset_by) % top, axis=1)


def shares(count, total, most, lean, full):
    loads = [(1 << 20) // math.isqrt(standing ** lean) + 1 for standing in range(1, count + 1)]
    largest = most if full else min(most, max(-(-total // count), total * loads[0] // sum(loads)))
    least = 1 if total - largest >= count - 1 else 0
    given, surplus = [largest] + [least] * (count - 1), total - largest - least * (count - 1)
    while surplus > 0:
        candidates = [i for i in range(1, count) if given[i] < largest] or [i for i in range(1, count) if given[i] < most]
        whole, budget = sum([loads[i] for i in candidates]), surplus
        for i in candidates:
            more = min(most - given[i], max(1, budget * loads[i] // whole), surplus)
            given[i] = given[i] + more
            surplus = surplus - more
    return np.array(given)


def scatter_about(own_key, dims, scale, bound, shards=(), kind=jnp.bfloat16):
    drawn = jax.random.normal(own_key, dims, jnp.float32) * scale
    if len(shards) > 0:
        drawn = block_scale(own_key, dims, shards, -0.22, 0.18) * drawn
    return jnp.clip(drawn, min=-bound, max=bound).astype(kind)


def setup_inputs(seed: int = 0, part: int = 0) -> dict:
    arg_keys = jax.random.split(jax.random.key(seed), 16)
    part_keys = jax.random.split(jax.random.fold_in(arg_keys[15], part), 16)
    query_plain = scatter_about(part_keys[0], (SEQUENCE_TOKENS, ATTENTION_HEADS * PLAIN_HEAD_WIDTH), 1.0, 6.0, ((0, 8), (1, 2)))
    query_turn = draw_query_turn(jax.random.fold_in(jax.random.fold_in(arg_keys[15], part), 71), part)
    latent = scatter_about(part_keys[2], (SEQUENCE_TOKENS, LATENT_WIDTH), 1.0, 6.0, ((0, 8),))
    key_turn = draw_key_turn(jax.random.fold_in(jax.random.fold_in(arg_keys[15], part), 71), part)
    latent_norm_scale = jnp.clip(1.0 + 0.18 * jax.random.normal(arg_keys[4], (LATENT_WIDTH,), jnp.float32), 0.099609375, 1.8984375).astype(jnp.bfloat16)
    plain_key_matrix = scatter_about(arg_keys[5], (LATENT_WIDTH, ATTENTION_HEADS * PLAIN_HEAD_WIDTH), LATENT_WIDTH ** -0.5, 0.25, ((1, 2),))
    value_matrix = scatter_about(arg_keys[6], (LATENT_WIDTH, ATTENTION_HEADS * VALUE_WIDTH), LATENT_WIDTH ** -0.5, 0.25, ((1, 2),))
    residual = scatter_about(part_keys[7], (SEQUENCE_TOKENS, D), 1.0, 6.0, ((0, 16),))
    out_weight = scatter_about(arg_keys[8], (ATTENTION_HEADS * VALUE_WIDTH, D), (16 * (ATTENTION_HEADS * VALUE_WIDTH) ** -0.5), 6.0)
    ffn_gain = jnp.clip(1.0 + 0.18 * jax.random.normal(arg_keys[9], (D,), jnp.float32), 0.099609375, 1.8984375).astype(jnp.bfloat16)
    gate_weight = scatter_about(arg_keys[10], (EXPERTS, D, D_EXPERT), (3 * D ** -0.5), 1.0, ((0, 8), (2, 2)))
    up_weight = scatter_about(arg_keys[11], (EXPERTS, D, D_EXPERT), (3 * D ** -0.5), 1.0, ((0, 8), (2, 2)))
    down_weight = scatter_about(arg_keys[12], (EXPERTS, D_EXPERT, D), (0.15 * D_EXPERT ** -0.5), 0.0625, ((0, 8), (1, 2)))
    routes_keys = jax.random.split(jax.random.fold_in(part_keys[13], 1), SEQUENCE_TOKENS // ROWS_DEV)
    routes_turns = jax.random.permutation(jax.random.fold_in(part_keys[13], 3), SEQUENCE_TOKENS // ROWS_DEV)
    routes = jax.vmap(lambda own, number: shared_out(jax.random.fold_in(part_keys[13], 2), own, number, ROWS_DEV, EXPERTS, TOP, CAP, 1))(routes_keys, routes_turns).reshape((SEQUENCE_TOKENS, TOP))
    route_weights = jnp.clip(0.1 + 0.5 * jax.random.uniform(part_keys[14], (SEQUENCE_TOKENS, TOP), jnp.float32) ** block_scale(part_keys[14], (SEQUENCE_TOKENS, TOP), ((0, 16),), -0.2, 0.2), 0.1, 0.6)
    return dict(query_plain=query_plain, query_turn=query_turn, latent=latent, key_turn=key_turn, latent_norm_scale=latent_norm_scale, plain_key_matrix=plain_key_matrix, value_matrix=value_matrix, residual=residual, out_weight=out_weight, ffn_gain=ffn_gain, gate_weight=gate_weight, up_weight=up_weight, down_weight=down_weight, routes=routes, route_weights=route_weights)


theta = 10000.0
eps = 1e-06
limit = 7.0
slope = 1.702

def turn(vector, row_shift, col_shift):
    width = vector.shape[-1]
    count = width // 4
    half = width // 2
    freqs = theta ** (-jnp.arange(count, dtype=jnp.float32) / count)
    extra = (1,) * (vector.ndim - 2)
    pieces = []
    for portion, shift in ((vector[..., :half], row_shift), (vector[..., half:], col_shift)):
        angle = (shift.astype(jnp.float32)[:, None] * freqs[None, :]).reshape((shift.shape[0],) + extra + (count,))
        lower = portion[..., :count]
        upper = portion[..., count:]
        pieces.append(jnp.concatenate([lower * jnp.cos(angle) - upper * jnp.sin(angle), lower * jnp.sin(angle) + upper * jnp.cos(angle)], axis=-1))
    return jnp.concatenate(pieces, axis=-1)

def norm_scale(values, gain):
    wide = values.astype(jnp.float32)
    return wide * lax.rsqrt(lax.optimization_barrier(jnp.mean(wide * wide, axis=-1, keepdims=True)) + eps) * gain.astype(jnp.float32)

def expert_apply(operands):
    rows, gate_w, up_w, down_w = operands
    gate_pre = jnp.minimum(jnp.dot(rows, gate_w, preferred_element_type=jnp.float32), limit)
    up_pre = jnp.clip(jnp.dot(rows, up_w, preferred_element_type=jnp.float32), -limit, limit)
    active = ((up_pre + 1.0) * gate_pre * jax.nn.sigmoid(slope * gate_pre)).astype(jnp.bfloat16)
    piece = down_w.shape[0] // N_TP
    groups = jnp.einsum('rnp,npd->nrd', active.reshape(rows.shape[0], N_TP, piece).astype(jnp.float32), down_w.reshape(N_TP, piece, down_w.shape[1]).astype(jnp.float32))
    rounded = lax.optimization_barrier(groups.astype(jnp.bfloat16))
    return lax.optimization_barrier(jnp.sum(rounded.astype(jnp.float32), axis=0)).astype(jnp.bfloat16)

def reference(query_plain, query_turn, latent, key_turn, latent_norm_scale, plain_key_matrix, value_matrix, residual, out_weight, ffn_gain, gate_weight, up_weight, down_weight, routes, route_weights):
    place = jnp.arange(SEQUENCE_TOKENS, dtype=jnp.int32)
    grid_row = place // GRID_W
    grid_col = place % GRID_W
    normed_latent = norm_scale(latent, latent_norm_scale).astype(jnp.bfloat16)
    key_plain = jnp.dot(normed_latent, plain_key_matrix, preferred_element_type=jnp.float32).astype(jnp.bfloat16)
    values = jnp.dot(normed_latent, value_matrix, preferred_element_type=jnp.float32).astype(jnp.bfloat16)
    key_rot = turn(key_turn.astype(jnp.float32), grid_row, grid_col).astype(jnp.bfloat16)
    query_rot = turn(query_turn.astype(jnp.float32).reshape(SEQUENCE_TOKENS, ATTENTION_HEADS, QK_ROPE), grid_row, grid_col).astype(jnp.bfloat16)
    plain_heads = jnp.moveaxis(query_plain.reshape(SEQUENCE_TOKENS, ATTENTION_HEADS, PLAIN_HEAD_WIDTH), 1, 0)
    rot_heads = jnp.moveaxis(query_rot, 1, 0)
    key_heads = jnp.moveaxis(key_plain.reshape(SEQUENCE_TOKENS, ATTENTION_HEADS, PLAIN_HEAD_WIDTH), 1, 0)
    value_heads = jnp.moveaxis(values.reshape(SEQUENCE_TOKENS, ATTENTION_HEADS, VALUE_WIDTH), 1, 0)
    scale = (PLAIN_HEAD_WIDTH + QK_ROPE) ** (-0.5)
    block = math.gcd(SEQUENCE_TOKENS, 512)

    def one_head(operands):
        head_plain, head_rot, head_keys, head_values = operands

        def one_block(start):
            block_plain = lax.dynamic_slice_in_dim(head_plain, start, block, 0)
            block_rot = lax.dynamic_slice_in_dim(head_rot, start, block, 0)
            scores = (jnp.einsum('qd,kd->qk', block_plain, head_keys, preferred_element_type=jnp.float32) + jnp.einsum('qd,kd->qk', block_rot, key_rot, preferred_element_type=jnp.float32)) * scale
            peak = lax.optimization_barrier(jnp.max(scores, axis=1, keepdims=True))
            weights = jnp.exp(scores - peak)
            summed = jnp.dot(weights.astype(jnp.bfloat16), head_values, preferred_element_type=jnp.float32)
            return (summed / lax.optimization_barrier(jnp.sum(weights, axis=1, keepdims=True))).astype(jnp.bfloat16)
        starts = jnp.arange(SEQUENCE_TOKENS // block, dtype=jnp.int32) * block
        return lax.map(one_block, starts).reshape(SEQUENCE_TOKENS, VALUE_WIDTH)
    attended = lax.map(one_head, (plain_heads, rot_heads, key_heads, value_heads))
    attended = jnp.moveaxis(attended, 0, 1).reshape(SEQUENCE_TOKENS, ATTENTION_HEADS * VALUE_WIDTH)
    hidden = (residual.astype(jnp.float32) + jnp.dot(attended, out_weight, preferred_element_type=jnp.float32)).astype(jnp.bfloat16)
    normed = norm_scale(hidden, ffn_gain).astype(jnp.bfloat16)
    blocks = N_SP * N_TP
    per_block = routes.reshape(blocks, ROWS_DEV * TOP)
    marks = (per_block[..., None] == jnp.arange(EXPERTS, dtype=jnp.int32)).astype(jnp.int32)
    earlier = jnp.cumsum(marks, axis=1, dtype=jnp.int32) - marks
    slots = lax.optimization_barrier(jnp.sum(earlier * marks, axis=2, dtype=jnp.int32))
    target = ((per_block * blocks + jnp.arange(blocks, dtype=jnp.int32)[:, None]) * CAP + slots).reshape(SEQUENCE_TOKENS * TOP)
    copies = jnp.repeat(normed, TOP, axis=0)
    buffer = jnp.zeros((EXPERTS * blocks * CAP, D), jnp.bfloat16).at[target].set(copies)
    results = lax.map(expert_apply, (buffer.reshape(EXPERTS, blocks * CAP, D), gate_weight, up_weight, down_weight))
    results = results.reshape(EXPERTS * blocks * CAP, D)
    picked = results[target].reshape(SEQUENCE_TOKENS, TOP, D).astype(jnp.float32)
    return (hidden.astype(jnp.float32) + lax.optimization_barrier(jnp.sum(route_weights[..., None] * picked, axis=1))).astype(jnp.bfloat16)
```

```python
import functools

import jax
import jax.numpy as jnp
from jax import lax
from jax.experimental import pallas as pl
from jax.experimental.pallas import tpu as pltpu
from jax.sharding import PartitionSpec as P

PLAIN_HEAD_WIDTH = 128
QK_ROPE = 64
VALUE_WIDTH = 128
GRID_W = 64


theta = 10000.0
eps = 1e-06
limit = 7.0
slope = 1.702
CORES = 2
EARLY_ROWS = 16
VMEM_BYTES = 60 * 2**20


def turn(vector, row_shift, col_shift):
    width = vector.shape[-1]
    count = width // 4
    half = width // 2
    freqs = theta ** (-jnp.arange(count, dtype=jnp.float32) / count)
    extra = (1,) * (vector.ndim - 2)
    pieces = []
    for portion, shift in ((vector[..., :half], row_shift), (vector[..., half:], col_shift)):
        angle = (shift.astype(jnp.float32)[:, None] * freqs[None, :]).reshape(
            (shift.shape[0],) + extra + (count,)
        )
        lower = portion[..., :count]
        upper = portion[..., count:]
        pieces.append(
            jnp.concatenate(
                [
                    lower * jnp.cos(angle) - upper * jnp.sin(angle),
                    lower * jnp.sin(angle) + upper * jnp.cos(angle),
                ],
                axis=-1,
            )
        )
    return jnp.concatenate(pieces, axis=-1)


def norm_scale(values, gain):
    wide = values.astype(jnp.float32)
    return (
        wide
        * lax.rsqrt(jnp.mean(wide * wide, axis=-1, keepdims=True) + eps)
        * gain.astype(jnp.float32)
    )


def expert_active(rows, gate_w, up_w):
    gate_pre = jnp.minimum(jnp.dot(rows, gate_w, preferred_element_type=jnp.float32), limit)
    up_pre = jnp.clip(jnp.dot(rows, up_w, preferred_element_type=jnp.float32), -limit, limit)
    return ((up_pre + 1.0) * gate_pre * jax.nn.sigmoid(slope * gate_pre)).astype(jnp.bfloat16)


def flipped(index, mask):
    out = index
    bit = 1
    while bit <= mask:
        if mask & bit:
            out = out + bit - 2 * bit * ((index // bit) % 2)
        bit *= 2
    return out


def gatherer(chips, group, own, gathered, sems, launch):
    z_send, z_recv, x_send, x_recv, c_send, c_recv = sems
    place = lax.axis_index("sp")
    column = lax.axis_index("tp")
    chip, core = place // CORES, place % CORES
    per_chip = CORES * group
    partner = {"sp": chip * CORES + 1 - core}

    def other(shift):
        return (column + shift) % group

    def slot(k, core_at, column_at):
        return flipped(chip, k) * per_chip + core_at * group + column_at

    def chip_peer(k):
        return {"sp": flipped(chip, k) * CORES + core}

    def remote(src, dst, send_sem, recv_sem, device):
        return pltpu.make_async_remote_copy(
            src_ref=src, dst_ref=dst, send_sem=send_sem, recv_sem=recv_sem, device_id=device
        )

    def greet():
        barrier = pltpu.get_barrier_semaphore()
        pl.semaphore_signal(barrier, inc=1, device_id=partner)
        for k in range(1, chips):
            pl.semaphore_signal(barrier, inc=1, device_id=chip_peer(k))
        for shift in range(1, group):
            pl.semaphore_signal(barrier, inc=1, device_id={"tp": other(shift)})

    def met():
        pl.semaphore_wait(pltpu.get_barrier_semaphore(), chips + group - 1)

    def source(k, back):
        if k == 0 and back == 0:
            return own
        return gathered.at[slot(k, core, other(group - back))]

    def chip_wait(k):
        landed = gathered.at[slot(k, core, column)]
        remote(landed, landed, z_send.at[k], z_recv.at[k], chip_peer(k)).wait_recv()

    def core_copy(k, back):
        return remote(
            source(k, back),
            gathered.at[slot(k, core, other(group - back))],
            c_send.at[k, back],
            c_recv.at[k, back],
            partner,
        )

    def core_wait(k, back):
        landed = gathered.at[slot(k, 1 - core, other(group - back))]
        remote(landed, landed, c_send.at[k, back], c_recv.at[k, back], partner).wait_recv()

    def tp_copy(k, shift):
        return remote(
            source(k, 0),
            gathered.at[slot(k, core, column)],
            x_send.at[k, shift],
            x_recv.at[k, shift],
            {"tp": other(shift)},
        )

    def tp_wait(k, shift):
        landed = gathered.at[slot(k, core, other(group - shift))]
        remote(
            landed, landed, x_send.at[k, shift], x_recv.at[k, shift], {"tp": other(shift)}
        ).wait_recv()

    def spread(k):
        for shift in range(1, group):
            launch(tp_copy(k, shift))
        launch(core_copy(k, 0))

    def begin():
        for k in range(1, chips):
            launch(
                remote(
                    own,
                    gathered.at[slot(0, core, column)],
                    z_send.at[k],
                    z_recv.at[k],
                    chip_peer(k),
                )
            )
        spread(0)

    def step(k):
        if k + 1 < chips:
            chip_wait(k + 1)
            spread(k + 1)
        for shift in range(1, group):
            tp_wait(k, shift)
            launch(core_copy(k, shift))
        for back in range(group):
            core_wait(k, back)

    return greet, met, begin, step, slot, chip_peer, partner, other, remote


def gather_kernel(chips, group, own, gathered, *sems):
    sends = []

    def launch(copy):
        copy.start()
        sends.append(copy)

    greet, met, begin, step, slot = gatherer(chips, group, own, gathered, sems, launch)[:5]
    greet()
    met()
    begin()
    gathered[slot(0, lax.axis_index("sp") % CORES, lax.axis_index("tp"))] = own[...]
    for k in range(chips):
        step(k)
    for copy in sends:
        copy.wait_send()


def gather_sems(chips, group):
    dma = pltpu.SemaphoreType.DMA
    return [dma((chips,))] * 2 + [dma((chips, group))] * 4


def run_gather(rows):
    group = lax.axis_size("tp")
    chips = lax.axis_size("sp") // CORES
    whole = pl.BlockSpec(memory_space=pltpu.VMEM)
    return pl.pallas_call(
        functools.partial(gather_kernel, chips, group),
        out_shape=jax.ShapeDtypeStruct((chips * CORES * group,) + rows.shape, rows.dtype),
        in_specs=[whole],
        out_specs=whole,
        scratch_shapes=gather_sems(chips, group),
        compiler_params=pltpu.CompilerParams(
            collective_id=1, has_side_effects=True, vmem_limit_bytes=VMEM_BYTES // 2
        ),
    )(rows)


def neighbour_order(chips):
    table = []
    for z in range(chips):
        table.append(sorted(range(chips), key=lambda o: (abs(o - z), o if z < chips // 2 else -o)))
    return table


def pick(z, values):
    out = values[0]
    for at in range(1, len(values)):
        out = jnp.where(z == at, values[at], out)
    return out


def experts_kernel(
    chips,
    early,
    attended_ref,
    residual_ref,
    gain_ref,
    share_ref,
    out_hbm,
    gate_hbm,
    up_hbm,
    down_hbm,
    out_ref,
    heads,
    hidden,
    gathered,
    partial,
    from_core,
    from_x,
    from_x_early,
    from_z,
    from_z_early,
    outw_ref,
    gate_ref,
    up_ref,
    down_ref,
    load_sem,
    h_send,
    h_recv,
    gz_send,
    gz_recv,
    gx_send,
    gx_recv,
    gc_send,
    gc_recv,
    rc_send,
    rc_recv,
    rx_send,
    rx_recv,
    rz_send,
    rz_recv,
):
    place = lax.axis_index("sp")
    column = lax.axis_index("tp")
    chip, core = place // CORES, place % CORES
    across = 1 - column
    rows_dev, model_width = hidden.shape
    late = rows_dev - early
    table = neighbour_order(chips)
    order = [chip] + [pick(chip, [table[z][j] for z in range(chips)]) for j in range(1, chips)]
    far = [0] + [
        pick(chip, [abs(table[z][j] - z) for z in range(chips)]) for j in range(1, chips)
    ]
    sends = []
    first_rows = pl.ds(0, early)
    last_rows = pl.ds(early, late)

    def launch(copy, when=None):
        if when is None:
            copy.start()
        else:
            pl.when(when)(copy.start)
        sends.append((copy, when))

    def remote(src, dst, send_sem, recv_sem, device):
        return pltpu.make_async_remote_copy(
            src_ref=src, dst_ref=dst, send_sem=send_sem, recv_sem=recv_sem, device_id=device
        )

    def on_chip(at):
        return {"sp": at * CORES + core}

    partner = {"sp": chip * CORES + 1 - core}
    beside = {"tp": across}

    barrier = pltpu.get_barrier_semaphore()
    pl.semaphore_signal(barrier, inc=1, device_id=partner)
    pl.semaphore_signal(barrier, inc=1, device_id=beside)
    for j in range(1, chips):
        pl.semaphore_signal(barrier, inc=1, device_id=on_chip((chip + j) % chips))
    loads = [
        pltpu.make_async_copy(src, dst, load_sem.at[i])
        for i, (src, dst) in enumerate(
            (
                (out_hbm, outw_ref),
                (gate_hbm, gate_ref),
                (up_hbm, up_ref),
                (down_hbm, down_ref),
            )
        )
    ]
    for load in loads:
        load.start()
    pl.semaphore_wait(barrier, chips + 1)

    swap = remote(attended_ref.at[across], heads.at[column], h_send, h_recv, beside)
    launch(swap)
    heads[column] = attended_ref[column]
    loads[0].wait()
    landed = heads.at[across]
    remote(landed, landed, h_send, h_recv, beside).wait_recv()
    joined = jnp.concatenate([heads[0], heads[1]], axis=1)
    projected = jnp.dot(joined, outw_ref[...], preferred_element_type=jnp.float32)
    mixed = (residual_ref[...].astype(jnp.float32) + projected).astype(jnp.bfloat16)
    gathered[place, column] = norm_scale(mixed, gain_ref[...]).astype(jnp.bfloat16)
    hidden[...] = mixed

    kinds = ((0, last_rows), (0, first_rows), (1, first_rows), (1, last_rows))
    use = [k for k in range(4) if (late if k in (0, 3) else early)]

    def piece(at, core_at, kind):
        flip, rows = kinds[kind]
        return gathered.at[at * CORES + core_at, across if flip else column, rows]

    def gz_copy(at, kind, to, lane):
        ref = piece(at, core, kind)
        return remote(ref, ref, gz_send.at[at, kind, lane], gz_recv.at[at, kind], on_chip(to))

    def gz_wait(at, kind):
        ref = piece(at, core, kind)
        remote(
            ref, ref, gz_send.at[at, kind, 0], gz_recv.at[at, kind], on_chip(at)
        ).wait_recv()

    def gx_copy(at, kind):
        ref = piece(at, core, kind)
        return remote(ref, ref, gx_send.at[at, kind], gx_recv.at[at, kind], beside)

    def gx_wait(at, kind):
        ref = piece(at, core, 3 - kind)
        remote(ref, ref, gx_send.at[at, kind], gx_recv.at[at, kind], beside).wait_recv()

    def gc_copy(at, kind):
        ref = piece(at, core, kind)
        return remote(ref, ref, gc_send.at[at, kind], gc_recv.at[at, kind], partner)

    def gc_wait(at, kind):
        ref = piece(at, 1 - core, kind)
        remote(ref, ref, gc_send.at[at, kind], gc_recv.at[at, kind], partner).wait_recv()

    def both_ways(kind):
        launch(gz_copy(chip, kind, chip - 1, 0), chip > 0)
        launch(gz_copy(chip, kind, chip + 1, 1), chip < chips - 1)

    def begin():
        if early:
            launch(gx_copy(chip, 1))
        if late:
            both_ways(0)
            launch(gx_copy(chip, 0))
        if early:
            both_ways(1)
        for kind in use:
            if kind < 2:
                launch(gc_copy(chip, kind))
        if early:
            gx_wait(chip, 1)
            both_ways(2)
            launch(gc_copy(chip, 2))

    def forward(at, now=None):
        step = jnp.where(at < chip, 1, -1)
        more = jnp.where(at < chip, chip < chips - 1, chip > 0)
        for kind in use:
            if kind == 3:
                continue
            if now is None:
                gz_wait(at, kind)
            else:
                pl.when(now)(functools.partial(gz_wait, at, kind))
            launch(gz_copy(at, kind, chip + step, 0), more if now is None else now & more)
            if kind == 0:
                launch(gx_copy(at, 0), now)
            launch(gc_copy(at, kind), now)

    def crossed(at):
        if late:
            gx_wait(at, 0)
            launch(gc_copy(at, 3))

    def apply(load_from, count, store_to):
        active = expert_active(load_from(gathered).reshape(count, model_width), gate_ref[...], up_ref[...])
        product = jnp.dot(active, down_ref[...], preferred_element_type=jnp.float32)
        store_to((product * load_from(share_ref).reshape(count, 1)).astype(jnp.bfloat16))

    def pair(at):
        return pl.ds(at * CORES, CORES)

    def compute_early(at):
        if not early:
            return
        gc_wait(at, 1)
        gc_wait(at, 2)

        def store(value):
            partial[pair(at), :, first_rows] = value.reshape(CORES, 2, early, model_width)

        apply(lambda ref: ref[pair(at), :, first_rows], 2 * CORES * early, store)
        launch(core_sum_early(at))

    def compute_late(at, kind):
        if not late:
            return
        gc_wait(at, kind)
        side = across if kind else column

        def store(value):
            partial[pair(at), side, last_rows] = value.reshape(CORES, late, model_width)

        apply(lambda ref: ref[pair(at), side, last_rows], CORES * late, store)
        launch(core_sum_late(at, kind))

    def core_sum_early(at):
        return remote(
            partial.at[at * CORES + 1 - core, :, first_rows],
            from_core.at[at, :, first_rows],
            rc_send.at[at, 1],
            rc_recv.at[at, 1],
            partner,
        )

    def core_sum_late(at, kind):
        side = across if kind else column
        return remote(
            partial.at[at * CORES + 1 - core, side, last_rows],
            from_core.at[at, side, last_rows],
            rc_send.at[at, kind],
            rc_recv.at[at, kind],
            partner,
        )

    def x_sum(at):
        return remote(
            partial.at[at * CORES + core, across, last_rows],
            from_x.at[at],
            rx_send.at[at],
            rx_recv.at[at],
            beside,
        )

    def z_sum_early(at, sender):
        return remote(
            partial.at[at * CORES + core, :, first_rows],
            from_z_early.at[sender],
            rz_send.at[at, 0],
            rz_recv.at[sender, 0],
            on_chip(at),
        )

    def z_sum_late(at, sender):
        return remote(
            partial.at[at * CORES + core, column, last_rows],
            from_z.at[sender],
            rz_send.at[at, 1],
            rz_recv.at[sender, 1],
            on_chip(at),
        )

    def wide(value):
        return value.astype(jnp.float32)

    def sum_early(j):
        at = order[j]
        if not early:
            return
        core_sum_early(at).wait_recv()
        mine = at * CORES + core
        partial[mine, :, first_rows] = (
            wide(partial[mine, :, first_rows]) + wide(from_core[at, :, first_rows])
        ).astype(jnp.bfloat16)
        if j:
            launch(z_sum_early(at, chip))

    def sum_late(j, kind):
        at = order[j]
        if not late:
            return
        core_sum_late(at, kind).wait_recv()
        mine = at * CORES + core
        side = across if kind else column
        partial[mine, side, last_rows] = (
            wide(partial[mine, side, last_rows]) + wide(from_core[at, side, last_rows])
        ).astype(jnp.bfloat16)
        if kind:
            launch(x_sum(at))

    def sum_across(j):
        at = order[j]
        if not late:
            return
        x_sum(at).wait_recv()
        mine = at * CORES + core
        partial[mine, column, last_rows] = (
            wide(partial[mine, column, last_rows]) + wide(from_x[at])
        ).astype(jnp.bfloat16)
        if j:
            launch(z_sum_late(at, chip))

    def arrive(distance):
        for j in range(distance, min(2 * distance, chips - 1) + 1):
            if all(abs(table[z][j] - z) == distance for z in range(chips)):
                forward(order[j])
            else:
                forward(order[j], far[j] == distance)

    begin()
    for load in loads[1:]:
        load.wait()
    compute_early(chip)
    compute_late(chip, 0)
    for j in range(chips):
        at = order[j]
        if j == 0:
            arrive(1)
        crossed(at)
        if j:
            compute_early(at)
            compute_late(at, 0)
        compute_late(at, 3)
        sum_early(j)
        sum_late(j, 3)
        sum_late(j, 0)
        if j:
            sum_across(j - 1)
            arrive(j + 1)
    sum_across(chips - 1)
    mine = chip * CORES + core
    if early:
        total = wide(partial[mine, :, first_rows])
        for j in range(1, chips):
            z_sum_early(chip, order[j]).wait_recv()
            total = total + wide(from_z_early[order[j]])
        partial[mine, :, first_rows] = total.astype(jnp.bfloat16)
        last = remote(
            partial.at[mine, across, first_rows],
            from_x_early,
            rx_send.at[chips],
            rx_recv.at[chips],
            beside,
        )
        launch(last)
    if late:
        total = wide(hidden[last_rows]) + wide(partial[mine, column, last_rows])
        for j in range(1, chips):
            z_sum_late(chip, order[j]).wait_recv()
            total = total + wide(from_z[order[j]])
        out_ref[last_rows] = total.astype(jnp.bfloat16)
    if early:
        last.wait_recv()
        out_ref[first_rows] = (
            wide(hidden[first_rows]) + wide(partial[mine, column, first_rows]) + wide(from_x_early[...])
        ).astype(jnp.bfloat16)
    for copy, when in sends:
        if when is None:
            copy.wait_send()
        else:
            pl.when(when)(copy.wait_send)


def run_experts(attended, residual, gain, shares, out_w, gate_w, up_w, down_w):
    chips = lax.axis_size("sp") // CORES
    rows_dev, model_width = residual.shape
    pairs = chips * CORES
    early = EARLY_ROWS if rows_dev > EARLY_ROWS else 0
    late = rows_dev - early
    dma = pltpu.SemaphoreType.DMA
    block = (rows_dev, model_width)
    heads = (2, rows_dev, attended.shape[1])
    whole = pl.BlockSpec(memory_space=pltpu.VMEM)

    def vmem(*shape):
        return pltpu.VMEM(shape, jnp.bfloat16)

    return pl.pallas_call(
        functools.partial(experts_kernel, chips, early),
        out_shape=jax.ShapeDtypeStruct(block, jnp.bfloat16),
        in_specs=[whole] * 4 + [pl.BlockSpec(memory_space=pl.ANY)] * 4,
        out_specs=whole,
        scratch_shapes=[
            vmem(*heads),
            vmem(*block),
            vmem(pairs, 2, *block),
            vmem(pairs, 2, *block),
            vmem(chips, 2, *block),
            vmem(chips, late, model_width),
            vmem(max(early, 16), model_width),
            vmem(chips, late, model_width),
            vmem(chips, 2, max(early, 16), model_width),
            vmem(*out_w.shape),
            vmem(*gate_w.shape),
            vmem(*up_w.shape),
            vmem(*down_w.shape),
            dma((4,)),
            dma,
            dma,
            dma((chips, 3, 2)),
            dma((chips, 3)),
            dma((chips, 2)),
            dma((chips, 2)),
            dma((chips, 4)),
            dma((chips, 4)),
            dma((chips, 4)),
            dma((chips, 4)),
            dma((chips + 1,)),
            dma((chips + 1,)),
            dma((chips, 2)),
            dma((chips, 2)),
        ],
        compiler_params=pltpu.CompilerParams(
            collective_id=0, has_side_effects=True, vmem_limit_bytes=VMEM_BYTES
        ),
    )(
        attended.reshape(heads),
        residual,
        gain.reshape(1, model_width),
        shares.reshape(pairs, 2, rows_dev, 1),
        out_w,
        gate_w,
        up_w,
        down_w,
    )


def experts_fit(rows_dev, model_width):
    group, places = lax.axis_size("tp"), lax.axis_size("sp")
    chips = places // CORES
    if group != 2 or places % CORES or chips & (chips - 1) or rows_dev % 16:
        return False
    return 3 * places * group * rows_dev * model_width * 2 < VMEM_BYTES // 2


def on_device(
    query_plain,
    query_turn,
    latent,
    key_turn,
    latent_norm_scale,
    plain_key_matrix,
    value_matrix,
    residual,
    out_weight,
    ffn_gain,
    gate_weight,
    up_weight,
    down_weight,
    routes,
    route_weights,
):
    tok_dev = latent.shape[0]
    heads_dev = query_plain.shape[1] // PLAIN_HEAD_WIDTH
    model_width = residual.shape[1]
    place = lax.axis_index("sp") * tok_dev + jnp.arange(tok_dev, dtype=jnp.int32)
    grid_row = place // GRID_W
    grid_col = place % GRID_W
    rows_dev, model_width = residual.shape
    group = lax.axis_size("tp")
    count = lax.axis_size("sp")
    fits = experts_fit(rows_dev, model_width)
    expert_ids = jnp.arange(count, dtype=jnp.int32)
    share = jnp.sum(
        route_weights[..., None] * (routes[..., None] == expert_ids).astype(jnp.float32), axis=1
    )
    latent_width = latent.shape[1]
    wide = latent_width + QK_ROPE

    def key_side(latents, turns, at_row, at_col):
        normed_latent = norm_scale(latents, latent_norm_scale).astype(jnp.bfloat16)
        key_rot = turn(turns.astype(jnp.float32), at_row, at_col).astype(jnp.bfloat16)
        return [normed_latent, key_rot]

    if fits:
        first = lax.axis_index("tp") * rows_dev
        high = lax.reduce_precision(share, 8, 7)
        filled = wide + 2 * count
        sent = jnp.concatenate(
            key_side(
                lax.dynamic_slice_in_dim(latent, first, rows_dev, 0),
                lax.dynamic_slice_in_dim(key_turn, first, rows_dev, 0),
                lax.dynamic_slice_in_dim(grid_row, first, rows_dev, 0),
                lax.dynamic_slice_in_dim(grid_col, first, rows_dev, 0),
            )
            + [high.astype(jnp.bfloat16), (share - high).astype(jnp.bfloat16)]
            + [jnp.zeros((rows_dev, -filled % 128), jnp.bfloat16)],
            axis=1,
        )
        everyone = run_gather(sent)
        everyone = everyone.reshape(everyone.shape[0] * rows_dev, everyone.shape[2])
        shares = everyone[:, wide : wide + count].astype(jnp.float32) + everyone[
            :, wide + count : filled
        ].astype(jnp.float32)
    else:
        sent = jnp.concatenate(key_side(latent, key_turn, grid_row, grid_col), axis=1)
        everyone = lax.all_gather(sent, "sp", axis=0, tiled=True)
        shares = lax.all_gather(share, ("sp", "tp"), axis=0, tiled=True)
    own_share = jnp.sum(
        jnp.where(expert_ids[None, :] == lax.axis_index("sp"), shares, 0.0), axis=1, keepdims=True
    )
    all_latent = everyone[:, :latent_width]
    all_rot = everyone[:, latent_width:wide]
    keys = jnp.dot(all_latent, plain_key_matrix, preferred_element_type=jnp.float32).astype(
        jnp.bfloat16
    )
    values = jnp.dot(all_latent, value_matrix, preferred_element_type=jnp.float32).astype(
        jnp.bfloat16
    )
    query_rot = turn(
        query_turn.astype(jnp.float32).reshape(tok_dev, heads_dev, QK_ROPE), grid_row, grid_col
    ).astype(jnp.bfloat16)
    scale = (PLAIN_HEAD_WIDTH + QK_ROPE) ** (-0.5)
    attended = []
    for head in range(heads_dev):
        span = slice(head * PLAIN_HEAD_WIDTH, (head + 1) * PLAIN_HEAD_WIDTH)
        scores = (
            jnp.einsum(
                "qd,kd->qk", query_plain[:, span], keys[:, span], preferred_element_type=jnp.float32
            )
            + jnp.einsum(
                "qd,kd->qk", query_rot[:, head], all_rot, preferred_element_type=jnp.float32
            )
        ) * scale
        weights = jnp.exp(scores - jnp.max(scores, axis=1, keepdims=True))
        summed = jnp.dot(
            weights.astype(jnp.bfloat16),
            values[:, head * VALUE_WIDTH : (head + 1) * VALUE_WIDTH],
            preferred_element_type=jnp.float32,
        )
        attended.append(
            (summed / jnp.sum(weights, axis=1, keepdims=True)).astype(jnp.bfloat16)
        )
    attended = jnp.concatenate(attended, axis=1)
    if fits:
        return run_experts(
            attended,
            residual,
            ffn_gain,
            own_share,
            out_weight,
            gate_weight[0],
            up_weight[0],
            down_weight[0],
        )
    swapped = lax.all_to_all(
        attended.reshape(group, rows_dev, heads_dev * VALUE_WIDTH),
        "tp",
        split_axis=0,
        concat_axis=0,
        tiled=True,
    )
    own_rows = jnp.transpose(swapped, (1, 0, 2)).reshape(rows_dev, group * heads_dev * VALUE_WIDTH)
    projected = jnp.dot(own_rows, out_weight, preferred_element_type=jnp.float32)
    hidden = (residual.astype(jnp.float32) + projected).astype(jnp.bfloat16)
    normed = norm_scale(hidden, ffn_gain).astype(jnp.bfloat16)
    rows = lax.all_gather(normed, ("sp", "tp"), axis=0, tiled=True)
    active = expert_active(rows, gate_weight[0], up_weight[0])
    product = jnp.dot(active, down_weight[0], preferred_element_type=jnp.float32)
    mixture = lax.psum_scatter(
        (own_share * product).astype(jnp.bfloat16),
        ("sp", "tp"),
        scatter_dimension=0,
        tiled=True,
    )
    return (hidden.astype(jnp.float32) + mixture.astype(jnp.float32)).astype(jnp.bfloat16)


def solution(mesh):
    placed = (
        P(("grp", "sp"), "tp"),
        P(("grp", "sp"), "tp"),
        P(("grp", "sp"), None),
        P(("grp", "sp"), None),
        P(),
        P(None, "tp"),
        P(None, "tp"),
        P(("grp", "sp", "tp"), None),
        P(),
        P(),
        P("sp", None, "tp"),
        P("sp", None, "tp"),
        P("sp", "tp", None),
        P(("grp", "sp", "tp"), None),
        P(("grp", "sp", "tp"), None),
    )
    return jax.shard_map(
        on_device,
        mesh=mesh,
        in_specs=placed,
        out_specs=P(("grp", "sp", "tp"), None),
        check_vma=False,
    )
```

```python
import functools

import jax
import jax.numpy as jnp
import numpy as np
from jax import lax
from jax.experimental import pallas as pl
from jax.experimental.pallas import tpu as pltpu
from jax.sharding import PartitionSpec as P

PLAIN_HEAD_WIDTH = 128
QK_ROPE = 64
VALUE_WIDTH = 128
GRID_W = 64


theta = 10000.0
eps = 1e-06
limit = 7.0
slope = 1.702
CORES = 2
EARLY_ROWS = 32
VMEM_BYTES = 60 * 2**20


def turn(vector, row_shift, col_shift):
    width = vector.shape[-1]
    count = width // 4
    half = width // 2
    freqs = theta ** (-jnp.arange(count, dtype=jnp.float32) / count)
    extra = (1,) * (vector.ndim - 2)
    pieces = []
    for portion, shift in ((vector[..., :half], row_shift), (vector[..., half:], col_shift)):
        angle = (shift.astype(jnp.float32)[:, None] * freqs[None, :]).reshape(
            (shift.shape[0],) + extra + (count,)
        )
        lower = portion[..., :count]
        upper = portion[..., count:]
        pieces.append(
            jnp.concatenate(
                [
                    lower * jnp.cos(angle) - upper * jnp.sin(angle),
                    lower * jnp.sin(angle) + upper * jnp.cos(angle),
                ],
                axis=-1,
            )
        )
    return jnp.concatenate(pieces, axis=-1)


def norm_scale(values, gain):
    wide = values.astype(jnp.float32)
    return (
        wide
        * lax.rsqrt(jnp.mean(wide * wide, axis=-1, keepdims=True) + eps)
        * gain.astype(jnp.float32)
    )


def expert_active(rows, gate_w, up_w):
    gate_pre = jnp.minimum(jnp.dot(rows, gate_w, preferred_element_type=jnp.float32), limit)
    up_pre = jnp.clip(jnp.dot(rows, up_w, preferred_element_type=jnp.float32), -limit, limit)
    return ((up_pre + 1.0) * gate_pre * jax.nn.sigmoid(slope * gate_pre)).astype(jnp.bfloat16)


def flipped(index, mask):
    out = index
    bit = 1
    while bit <= mask:
        if mask & bit:
            out = out + bit - 2 * bit * ((index // bit) % 2)
        bit *= 2
    return out


def gatherer(chips, group, own, gathered, sems, launch):
    z_send, z_recv, x_send, x_recv, c_send, c_recv = sems
    place = lax.axis_index("sp")
    column = lax.axis_index("tp")
    chip, core = place // CORES, place % CORES
    per_chip = CORES * group
    partner = {"sp": chip * CORES + 1 - core}

    def other(shift):
        return (column + shift) % group

    def slot(k, core_at, column_at):
        return flipped(chip, k) * per_chip + core_at * group + column_at

    def chip_peer(k):
        return {"sp": flipped(chip, k) * CORES + core}

    def remote(src, dst, send_sem, recv_sem, device):
        return pltpu.make_async_remote_copy(
            src_ref=src, dst_ref=dst, send_sem=send_sem, recv_sem=recv_sem, device_id=device
        )

    def greet():
        barrier = pltpu.get_barrier_semaphore()
        pl.semaphore_signal(barrier, inc=1, device_id=partner)
        for k in range(1, chips):
            pl.semaphore_signal(barrier, inc=1, device_id=chip_peer(k))
        for shift in range(1, group):
            pl.semaphore_signal(barrier, inc=1, device_id={"tp": other(shift)})

    def met():
        pl.semaphore_wait(pltpu.get_barrier_semaphore(), chips + group - 1)

    def source(k, back):
        if k == 0 and back == 0:
            return own
        return gathered.at[slot(k, core, other(group - back))]

    def chip_wait(k):
        landed = gathered.at[slot(k, core, column)]
        remote(landed, landed, z_send.at[k], z_recv.at[k], chip_peer(k)).wait_recv()

    def core_copy(k, back):
        return remote(
            source(k, back),
            gathered.at[slot(k, core, other(group - back))],
            c_send.at[k, back],
            c_recv.at[k, back],
            partner,
        )

    def core_wait(k, back):
        landed = gathered.at[slot(k, 1 - core, other(group - back))]
        remote(landed, landed, c_send.at[k, back], c_recv.at[k, back], partner).wait_recv()

    def tp_copy(k, shift):
        return remote(
            source(k, 0),
            gathered.at[slot(k, core, column)],
            x_send.at[k, shift],
            x_recv.at[k, shift],
            {"tp": other(shift)},
        )

    def tp_wait(k, shift):
        landed = gathered.at[slot(k, core, other(group - shift))]
        remote(
            landed, landed, x_send.at[k, shift], x_recv.at[k, shift], {"tp": other(shift)}
        ).wait_recv()

    def spread(k):
        for shift in range(1, group):
            launch(tp_copy(k, shift))
        launch(core_copy(k, 0))

    def begin():
        for k in range(1, chips):
            launch(
                remote(
                    own,
                    gathered.at[slot(0, core, column)],
                    z_send.at[k],
                    z_recv.at[k],
                    chip_peer(k),
                )
            )
        spread(0)

    def step(k):
        if k + 1 < chips:
            chip_wait(k + 1)
            spread(k + 1)
        for shift in range(1, group):
            tp_wait(k, shift)
            launch(core_copy(k, shift))
        for back in range(group):
            core_wait(k, back)

    return greet, met, begin, step, slot, chip_peer, partner, other, remote


def turn_matrices(shape, width):
    row = lax.broadcasted_iota(jnp.int32, shape, 0)
    col = lax.broadcasted_iota(jnp.int32, shape, 1)
    count = width // 4
    lane = col % 128
    source = (col // 128) * width + lane
    inside = lane < width
    lower = lane % (2 * count) < count
    straight = jnp.where(inside & (row == source), 1.0, 0.0)
    moved = jnp.where(lower, source + count, source - count)
    sign = jnp.where(lower, -1.0, 1.0)
    crossed = jnp.where(inside & (row == moved), sign, 0.0)
    return straight.astype(jnp.bfloat16), crossed.astype(jnp.bfloat16)


def attention_kernel(
    chips,
    group,
    query_ref,
    query_turn_ref,
    latent_ref,
    key_turn_ref,
    gain_ref,
    freqs_ref,
    routes_ref,
    route_weights_ref,
    keyw_hbm,
    valuew_hbm,
    out_ref,
    share_ref,
    own,
    gathered,
    queries,
    cosines,
    sines,
    keyw_ref,
    valuew_ref,
    load_sem,
    *sems,
):
    place = lax.axis_index("sp")
    column = lax.axis_index("tp")
    tokens, latent_width = latent_ref.shape
    rows_dev = own.shape[0]
    heads_dev = query_ref.shape[1] // PLAIN_HEAD_WIDTH
    count = lax.axis_size("sp")
    per_chip = CORES * group
    sends = []

    def launch(copy):
        copy.start()
        sends.append(copy)

    greet, met, begin, step, slot = gatherer(chips, group, own, gathered, sems, launch)[:5]
    greet()
    loads = [
        pltpu.make_async_copy(keyw_hbm, keyw_ref, load_sem.at[0]),
        pltpu.make_async_copy(valuew_hbm, valuew_ref, load_sem.at[1]),
    ]
    for load in loads:
        load.start()

    at = place * tokens + lax.broadcasted_iota(jnp.int32, (tokens, 128), 0)
    lane = lax.broadcasted_iota(jnp.int32, (tokens, 128), 1)
    shift = jnp.where(lane < QK_ROPE // 2, at // GRID_W, at % GRID_W).astype(jnp.float32)
    angle = shift * freqs_ref[...]
    cosines[...] = jnp.cos(angle)
    sines[...] = jnp.sin(angle)

    def turned(vector, matrices, cos, sin):
        straight, crossed = (
            jnp.dot(vector, matrix, preferred_element_type=jnp.float32) for matrix in matrices
        )
        return straight * cos + crossed * sin

    mine = pl.ds(pl.multiple_of(column * rows_dev, 16), rows_dev)
    key_rot = turned(
        key_turn_ref[mine, :],
        turn_matrices((QK_ROPE, 128), QK_ROPE),
        cosines[mine, :],
        sines[mine, :],
    )
    lane = lax.broadcasted_iota(jnp.int32, (rows_dev, 128), 1) - QK_ROPE
    expert = jnp.where(lane < count, lane, lane - count)
    share = jnp.zeros((rows_dev, 128), jnp.float32)
    for k in range(routes_ref.shape[1]):
        share = share + jnp.where(
            routes_ref[:, k : k + 1] == expert, route_weights_ref[:, k : k + 1], 0.0
        )
    high = share.astype(jnp.bfloat16).astype(jnp.float32)
    packed = jnp.where(lane < count, high, share - high)
    packed = jnp.where(lane < 2 * count, packed, 0.0)
    own[:, :latent_width] = norm_scale(latent_ref[mine, :], gain_ref[...]).astype(jnp.bfloat16)
    own[:, latent_width:] = jnp.where(lane < 0, key_rot, packed).astype(jnp.bfloat16)
    met()
    begin()
    gathered[slot(0, place % CORES, column)] = own[...]

    matrices = turn_matrices((heads_dev * QK_ROPE, heads_dev * 128), QK_ROPE)
    straight, crossed = (
        jnp.dot(query_turn_ref[...], matrix, preferred_element_type=jnp.float32)
        for matrix in matrices
    )
    for head in range(heads_dev):
        span = slice(head * 128, (head + 1) * 128)
        queries[head, :, :128] = query_ref[:, span]
        queries[head, :, 128:] = (
            straight[:, span] * cosines[...] + crossed[:, span] * sines[...]
        ).astype(jnp.bfloat16)
    for load in loads:
        load.wait()

    scale = (PLAIN_HEAD_WIDTH + QK_ROPE) ** (-0.5)
    peaks = [None] * heads_dev
    sums = [None] * heads_dev
    totals = [None] * heads_dev
    for k in range(chips):
        step(k)
        first = slot(k, 0, 0)
        width = per_chip * rows_dev
        latents = gathered[pl.ds(first, per_chip), :, :latent_width].reshape(width, latent_width)
        rot = gathered[pl.ds(first, per_chip), :, latent_width:].reshape(width, 128)
        keys = jnp.dot(latents, keyw_ref[...], preferred_element_type=jnp.float32).astype(
            jnp.bfloat16
        )
        values = jnp.dot(latents, valuew_ref[...], preferred_element_type=jnp.float32).astype(
            jnp.bfloat16
        )
        for head in range(heads_dev):
            span = slice(head * 128, (head + 1) * 128)
            scores = scale * lax.dot_general(
                queries[head],
                jnp.concatenate([keys[:, span], rot], axis=1),
                (((1,), (1,)), ((), ())),
                preferred_element_type=jnp.float32,
            )
            peak = jnp.max(scores, axis=1, keepdims=True)
            if k:
                peak = jnp.maximum(peak, peaks[head])
            weights = jnp.exp(scores - peak)
            total = jnp.sum(weights, axis=1, keepdims=True)
            summed = jnp.dot(
                weights.astype(jnp.bfloat16), values[:, span], preferred_element_type=jnp.float32
            )
            if k:
                fade = jnp.exp(peaks[head] - peak)
                total = total + fade * sums[head]
                summed = summed + fade * totals[head]
            peaks[head], sums[head], totals[head] = peak, total, summed
        lane = lax.broadcasted_iota(jnp.int32, (width, 128), 1) - QK_ROPE
        named = (lane == place) | (lane == place + count)
        share_ref[pl.ds(first, per_chip)] = jnp.sum(
            jnp.where(named, rot.astype(jnp.float32), 0.0), axis=1, keepdims=True
        ).reshape(per_chip, rows_dev, 1)
    for head in range(heads_dev):
        out_ref[:, head * 128 : (head + 1) * 128] = (totals[head] / sums[head]).astype(jnp.bfloat16)
    for copy in sends:
        copy.wait_send()


def gather_sems(chips, group):
    dma = pltpu.SemaphoreType.DMA
    return [dma((chips,))] * 2 + [dma((chips, group))] * 4


def run_attention(query, query_turn, latent, key_turn, gain, routes, route_weights, key_w, value_w):
    group = lax.axis_size("tp")
    chips = lax.axis_size("sp") // CORES
    blocks = chips * CORES * group
    tokens, latent_width = latent.shape
    rows_dev = routes.shape[0]
    heads_dev = query.shape[1] // PLAIN_HEAD_WIDTH
    quarter = QK_ROPE // 4
    freqs = theta ** (-np.arange(quarter, dtype=np.float32) / np.float32(quarter))
    freqs = np.tile(freqs.astype(np.float32), 128 // quarter).reshape(1, 128)
    dma = pltpu.SemaphoreType.DMA
    whole = pl.BlockSpec(memory_space=pltpu.VMEM)
    sent = latent_width + 128
    return pl.pallas_call(
        functools.partial(attention_kernel, chips, group),
        out_shape=[
            jax.ShapeDtypeStruct((tokens, heads_dev * VALUE_WIDTH), jnp.bfloat16),
            jax.ShapeDtypeStruct((blocks, rows_dev, 1), jnp.float32),
        ],
        in_specs=[whole] * 8 + [pl.BlockSpec(memory_space=pl.ANY)] * 2,
        out_specs=[whole, whole],
        scratch_shapes=[
            pltpu.VMEM((rows_dev, sent), jnp.bfloat16),
            pltpu.VMEM((blocks, rows_dev, sent), jnp.bfloat16),
            pltpu.VMEM((heads_dev, tokens, 256), jnp.bfloat16),
            pltpu.VMEM((tokens, 128), jnp.float32),
            pltpu.VMEM((tokens, 128), jnp.float32),
            pltpu.VMEM(key_w.shape, jnp.bfloat16),
            pltpu.VMEM(value_w.shape, jnp.bfloat16),
            dma((2,)),
        ]
        + gather_sems(chips, group),
        compiler_params=pltpu.CompilerParams(
            collective_id=1, has_side_effects=True, vmem_limit_bytes=VMEM_BYTES // 2
        ),
    )(
        query,
        query_turn,
        latent,
        key_turn,
        gain.reshape(1, latent_width),
        jnp.asarray(freqs),
        routes,
        route_weights,
        key_w,
        value_w,
    )


def neighbour_order(chips):
    table = []
    for z in range(chips):
        table.append(sorted(range(chips), key=lambda o: (abs(o - z), o if z < chips // 2 else -o)))
    return table


def pick(z, values):
    out = values[0]
    for at in range(1, len(values)):
        out = jnp.where(z == at, values[at], out)
    return out


def experts_kernel(
    chips,
    early,
    attended_ref,
    residual_ref,
    gain_ref,
    share_ref,
    out_hbm,
    gate_hbm,
    up_hbm,
    down_hbm,
    out_ref,
    heads,
    hidden,
    gathered,
    partial,
    from_core,
    from_x,
    from_x_early,
    from_z,
    from_z_early,
    outw_ref,
    gate_ref,
    up_ref,
    down_ref,
    load_sem,
    h_send,
    h_recv,
    gz_send,
    gz_recv,
    gx_send,
    gx_recv,
    gc_send,
    gc_recv,
    rc_send,
    rc_recv,
    rx_send,
    rx_recv,
    rz_send,
    rz_recv,
):
    place = lax.axis_index("sp")
    column = lax.axis_index("tp")
    chip, core = place // CORES, place % CORES
    across = 1 - column
    rows_dev, model_width = hidden.shape
    late = rows_dev - early
    table = neighbour_order(chips)
    order = [chip] + [pick(chip, [table[z][j] for z in range(chips)]) for j in range(1, chips)]
    far = [0] + [
        pick(chip, [abs(table[z][j] - z) for z in range(chips)]) for j in range(1, chips)
    ]
    sends = []
    first_rows = pl.ds(0, early)
    last_rows = pl.ds(early, late)

    def launch(copy, when=None):
        if when is None:
            copy.start()
        else:
            pl.when(when)(copy.start)
        sends.append((copy, when))

    def remote(src, dst, send_sem, recv_sem, device):
        return pltpu.make_async_remote_copy(
            src_ref=src, dst_ref=dst, send_sem=send_sem, recv_sem=recv_sem, device_id=device
        )

    def on_chip(at):
        return {"sp": at * CORES + core}

    partner = {"sp": chip * CORES + 1 - core}
    beside = {"tp": across}

    barrier = pltpu.get_barrier_semaphore()
    pl.semaphore_signal(barrier, inc=1, device_id=partner)
    pl.semaphore_signal(barrier, inc=1, device_id=beside)
    for j in range(1, chips):
        pl.semaphore_signal(barrier, inc=1, device_id=on_chip((chip + j) % chips))
    loads = [
        pltpu.make_async_copy(src, dst, load_sem.at[i])
        for i, (src, dst) in enumerate(
            (
                (out_hbm, outw_ref),
                (gate_hbm, gate_ref),
                (up_hbm, up_ref),
                (down_hbm, down_ref),
            )
        )
    ]
    for load in loads:
        load.start()
    pl.semaphore_wait(barrier, chips + 1)

    swap = remote(attended_ref.at[across], heads.at[column], h_send, h_recv, beside)
    launch(swap)
    heads[column] = attended_ref[column]
    loads[0].wait()
    landed = heads.at[across]
    remote(landed, landed, h_send, h_recv, beside).wait_recv()
    joined = jnp.concatenate([heads[0], heads[1]], axis=1)
    projected = jnp.dot(joined, outw_ref[...], preferred_element_type=jnp.float32)
    mixed = (residual_ref[...].astype(jnp.float32) + projected).astype(jnp.bfloat16)
    gathered[place, column] = norm_scale(mixed, gain_ref[...]).astype(jnp.bfloat16)
    hidden[...] = mixed

    kinds = ((0, last_rows), (0, first_rows), (1, first_rows), (1, last_rows))
    use = [k for k in range(4) if (late if k in (0, 3) else early)]

    def piece(at, core_at, kind):
        flip, rows = kinds[kind]
        return gathered.at[at * CORES + core_at, across if flip else column, rows]

    def gz_copy(at, kind, to, lane):
        ref = piece(at, core, kind)
        return remote(ref, ref, gz_send.at[at, kind, lane], gz_recv.at[at, kind], on_chip(to))

    def gz_wait(at, kind):
        ref = piece(at, core, kind)
        remote(
            ref, ref, gz_send.at[at, kind, 0], gz_recv.at[at, kind], on_chip(at)
        ).wait_recv()

    def gx_copy(at, kind):
        ref = piece(at, core, kind)
        return remote(ref, ref, gx_send.at[at, kind], gx_recv.at[at, kind], beside)

    def gx_wait(at, kind):
        ref = piece(at, core, 3 - kind)
        remote(ref, ref, gx_send.at[at, kind], gx_recv.at[at, kind], beside).wait_recv()

    def gc_copy(at, kind):
        ref = piece(at, core, kind)
        return remote(ref, ref, gc_send.at[at, kind], gc_recv.at[at, kind], partner)

    def gc_wait(at, kind):
        ref = piece(at, 1 - core, kind)
        remote(ref, ref, gc_send.at[at, kind], gc_recv.at[at, kind], partner).wait_recv()

    def both_ways(kind):
        launch(gz_copy(chip, kind, chip - 1, 0), chip > 0)
        launch(gz_copy(chip, kind, chip + 1, 1), chip < chips - 1)

    def begin():
        if early:
            launch(gx_copy(chip, 1))
        if late:
            both_ways(0)
            launch(gx_copy(chip, 0))
        if early:
            both_ways(1)
        for kind in use:
            if kind < 2:
                launch(gc_copy(chip, kind))
        if early:
            gx_wait(chip, 1)
            both_ways(2)
            launch(gc_copy(chip, 2))

    def forward(at, now=None):
        step = jnp.where(at < chip, 1, -1)
        more = jnp.where(at < chip, chip < chips - 1, chip > 0)
        for kind in use:
            if kind == 3:
                continue
            if now is None:
                gz_wait(at, kind)
            else:
                pl.when(now)(functools.partial(gz_wait, at, kind))
            launch(gz_copy(at, kind, chip + step, 0), more if now is None else now & more)
            if kind == 0:
                launch(gx_copy(at, 0), now)
            launch(gc_copy(at, kind), now)

    def crossed(at):
        if late:
            gx_wait(at, 0)
            launch(gc_copy(at, 3))

    def apply(load_from, count, store_to):
        active = expert_active(load_from(gathered).reshape(count, model_width), gate_ref[...], up_ref[...])
        product = jnp.dot(active, down_ref[...], preferred_element_type=jnp.float32)
        store_to((product * load_from(share_ref).reshape(count, 1)).astype(jnp.bfloat16))

    def pair(at):
        return pl.ds(at * CORES, CORES)

    def compute_early(at):
        if not early:
            return
        gc_wait(at, 1)
        gc_wait(at, 2)

        def store(value):
            partial[pair(at), :, first_rows] = value.reshape(CORES, 2, early, model_width)

        apply(lambda ref: ref[pair(at), :, first_rows], 2 * CORES * early, store)
        launch(core_sum_early(at))

    def compute_late(at, kind):
        if not late:
            return
        gc_wait(at, kind)
        side = across if kind else column

        def store(value):
            partial[pair(at), side, last_rows] = value.reshape(CORES, late, model_width)

        apply(lambda ref: ref[pair(at), side, last_rows], CORES * late, store)
        launch(core_sum_late(at, kind))

    def core_sum_early(at):
        return remote(
            partial.at[at * CORES + 1 - core, :, first_rows],
            from_core.at[at, :, first_rows],
            rc_send.at[at, 1],
            rc_recv.at[at, 1],
            partner,
        )

    def core_sum_late(at, kind):
        side = across if kind else column
        return remote(
            partial.at[at * CORES + 1 - core, side, last_rows],
            from_core.at[at, side, last_rows],
            rc_send.at[at, kind],
            rc_recv.at[at, kind],
            partner,
        )

    def x_sum(at):
        return remote(
            partial.at[at * CORES + core, across, last_rows],
            from_x.at[at],
            rx_send.at[at],
            rx_recv.at[at],
            beside,
        )

    def z_sum_early(at, sender):
        return remote(
            partial.at[at * CORES + core, :, first_rows],
            from_z_early.at[sender],
            rz_send.at[at, 0],
            rz_recv.at[sender, 0],
            on_chip(at),
        )

    def z_sum_late(at, sender):
        return remote(
            partial.at[at * CORES + core, column, last_rows],
            from_z.at[sender],
            rz_send.at[at, 1],
            rz_recv.at[sender, 1],
            on_chip(at),
        )

    def wide(value):
        return value.astype(jnp.float32)

    def sum_early(j):
        at = order[j]
        if not early:
            return
        core_sum_early(at).wait_recv()
        mine = at * CORES + core
        partial[mine, :, first_rows] = (
            wide(partial[mine, :, first_rows]) + wide(from_core[at, :, first_rows])
        ).astype(jnp.bfloat16)
        if j:
            launch(z_sum_early(at, chip))

    def sum_late(j, kind):
        at = order[j]
        if not late:
            return
        core_sum_late(at, kind).wait_recv()
        mine = at * CORES + core
        side = across if kind else column
        partial[mine, side, last_rows] = (
            wide(partial[mine, side, last_rows]) + wide(from_core[at, side, last_rows])
        ).astype(jnp.bfloat16)
        if kind:
            launch(x_sum(at))

    def sum_across(j):
        at = order[j]
        if not late:
            return
        x_sum(at).wait_recv()
        mine = at * CORES + core
        partial[mine, column, last_rows] = (
            wide(partial[mine, column, last_rows]) + wide(from_x[at])
        ).astype(jnp.bfloat16)
        if j:
            launch(z_sum_late(at, chip))

    def arrive(distance):
        for j in range(distance, min(2 * distance, chips - 1) + 1):
            if all(abs(table[z][j] - z) == distance for z in range(chips)):
                forward(order[j])
            else:
                forward(order[j], far[j] == distance)

    begin()
    for load in loads[1:]:
        load.wait()
    compute_early(chip)
    compute_late(chip, 0)
    for j in range(chips):
        at = order[j]
        if j == 0:
            arrive(1)
        crossed(at)
        if j:
            compute_early(at)
            compute_late(at, 0)
        compute_late(at, 3)
        sum_early(j)
        sum_late(j, 3)
        sum_late(j, 0)
        if j:
            sum_across(j - 1)
            arrive(j + 1)
    sum_across(chips - 1)
    mine = chip * CORES + core
    if early:
        total = wide(partial[mine, :, first_rows])
        for j in range(1, chips):
            z_sum_early(chip, order[j]).wait_recv()
            total = total + wide(from_z_early[order[j]])
        partial[mine, :, first_rows] = total.astype(jnp.bfloat16)
        last = remote(
            partial.at[mine, across, first_rows],
            from_x_early,
            rx_send.at[chips],
            rx_recv.at[chips],
            beside,
        )
        launch(last)
    if late:
        total = wide(hidden[last_rows]) + wide(partial[mine, column, last_rows])
        for j in range(1, chips):
            z_sum_late(chip, order[j]).wait_recv()
            total = total + wide(from_z[order[j]])
        out_ref[last_rows] = total.astype(jnp.bfloat16)
    if early:
        last.wait_recv()
        out_ref[first_rows] = (
            wide(hidden[first_rows]) + wide(partial[mine, column, first_rows]) + wide(from_x_early[...])
        ).astype(jnp.bfloat16)
    for copy, when in sends:
        if when is None:
            copy.wait_send()
        else:
            pl.when(when)(copy.wait_send)


def run_experts(attended, residual, gain, shares, out_w, gate_w, up_w, down_w):
    chips = lax.axis_size("sp") // CORES
    rows_dev, model_width = residual.shape
    pairs = chips * CORES
    early = EARLY_ROWS if rows_dev > EARLY_ROWS else 0
    late = rows_dev - early
    dma = pltpu.SemaphoreType.DMA
    block = (rows_dev, model_width)
    heads = (2, rows_dev, attended.shape[1])
    whole = pl.BlockSpec(memory_space=pltpu.VMEM)

    def vmem(*shape):
        return pltpu.VMEM(shape, jnp.bfloat16)

    return pl.pallas_call(
        functools.partial(experts_kernel, chips, early),
        out_shape=jax.ShapeDtypeStruct(block, jnp.bfloat16),
        in_specs=[whole] * 4 + [pl.BlockSpec(memory_space=pl.ANY)] * 4,
        out_specs=whole,
        scratch_shapes=[
            vmem(*heads),
            vmem(*block),
            vmem(pairs, 2, *block),
            vmem(pairs, 2, *block),
            vmem(chips, 2, *block),
            vmem(chips, late, model_width),
            vmem(max(early, 16), model_width),
            vmem(chips, late, model_width),
            vmem(chips, 2, max(early, 16), model_width),
            vmem(*out_w.shape),
            vmem(*gate_w.shape),
            vmem(*up_w.shape),
            vmem(*down_w.shape),
            dma((4,)),
            dma,
            dma,
            dma((chips, 3, 2)),
            dma((chips, 3)),
            dma((chips, 2)),
            dma((chips, 2)),
            dma((chips, 4)),
            dma((chips, 4)),
            dma((chips, 4)),
            dma((chips, 4)),
            dma((chips + 1,)),
            dma((chips + 1,)),
            dma((chips, 2)),
            dma((chips, 2)),
        ],
        compiler_params=pltpu.CompilerParams(
            collective_id=0, has_side_effects=True, vmem_limit_bytes=VMEM_BYTES
        ),
    )(
        attended.reshape(heads),
        residual,
        gain.reshape(1, model_width),
        shares.reshape(pairs, 2, rows_dev, 1),
        out_w,
        gate_w,
        up_w,
        down_w,
    )


def experts_fit(tokens, rows_dev, model_width):
    group, places = lax.axis_size("tp"), lax.axis_size("sp")
    chips = places // CORES
    if group != 2 or places % CORES or chips & (chips - 1) or rows_dev % 16:
        return False
    if tokens != group * rows_dev or QK_ROPE + 2 * places > 128:
        return False
    return 3 * places * group * rows_dev * model_width * 2 < VMEM_BYTES // 2


def on_device(
    query_plain,
    query_turn,
    latent,
    key_turn,
    latent_norm_scale,
    plain_key_matrix,
    value_matrix,
    residual,
    out_weight,
    ffn_gain,
    gate_weight,
    up_weight,
    down_weight,
    routes,
    route_weights,
):
    if experts_fit(latent.shape[0], *residual.shape):
        attended, own_share = run_attention(
            query_plain,
            query_turn,
            latent,
            key_turn,
            latent_norm_scale,
            routes,
            route_weights,
            plain_key_matrix,
            value_matrix,
        )
        return run_experts(
            attended,
            residual,
            ffn_gain,
            own_share,
            out_weight,
            gate_weight[0],
            up_weight[0],
            down_weight[0],
        )
    tok_dev = latent.shape[0]
    heads_dev = query_plain.shape[1] // PLAIN_HEAD_WIDTH
    model_width = residual.shape[1]
    place = lax.axis_index("sp") * tok_dev + jnp.arange(tok_dev, dtype=jnp.int32)
    grid_row = place // GRID_W
    grid_col = place % GRID_W
    rows_dev, model_width = residual.shape
    group = lax.axis_size("tp")
    count = lax.axis_size("sp")
    expert_ids = jnp.arange(count, dtype=jnp.int32)
    share = jnp.sum(
        route_weights[..., None] * (routes[..., None] == expert_ids).astype(jnp.float32), axis=1
    )
    latent_width = latent.shape[1]
    wide = latent_width + QK_ROPE

    def key_side(latents, turns, at_row, at_col):
        normed_latent = norm_scale(latents, latent_norm_scale).astype(jnp.bfloat16)
        key_rot = turn(turns.astype(jnp.float32), at_row, at_col).astype(jnp.bfloat16)
        return [normed_latent, key_rot]

    sent = jnp.concatenate(key_side(latent, key_turn, grid_row, grid_col), axis=1)
    everyone = lax.all_gather(sent, "sp", axis=0, tiled=True)
    shares = lax.all_gather(share, ("sp", "tp"), axis=0, tiled=True)
    own_share = jnp.sum(
        jnp.where(expert_ids[None, :] == lax.axis_index("sp"), shares, 0.0), axis=1, keepdims=True
    )
    all_latent = everyone[:, :latent_width]
    all_rot = everyone[:, latent_width:wide]
    keys = jnp.dot(all_latent, plain_key_matrix, preferred_element_type=jnp.float32).astype(
        jnp.bfloat16
    )
    values = jnp.dot(all_latent, value_matrix, preferred_element_type=jnp.float32).astype(
        jnp.bfloat16
    )
    query_rot = turn(
        query_turn.astype(jnp.float32).reshape(tok_dev, heads_dev, QK_ROPE), grid_row, grid_col
    ).astype(jnp.bfloat16)
    scale = (PLAIN_HEAD_WIDTH + QK_ROPE) ** (-0.5)
    attended = []
    for head in range(heads_dev):
        span = slice(head * PLAIN_HEAD_WIDTH, (head + 1) * PLAIN_HEAD_WIDTH)
        scores = (
            jnp.einsum(
                "qd,kd->qk", query_plain[:, span], keys[:, span], preferred_element_type=jnp.float32
            )
            + jnp.einsum(
                "qd,kd->qk", query_rot[:, head], all_rot, preferred_element_type=jnp.float32
            )
        ) * scale
        weights = jnp.exp(scores - jnp.max(scores, axis=1, keepdims=True))
        summed = jnp.dot(
            weights.astype(jnp.bfloat16),
            values[:, head * VALUE_WIDTH : (head + 1) * VALUE_WIDTH],
            preferred_element_type=jnp.float32,
        )
        attended.append(
            (summed / jnp.sum(weights, axis=1, keepdims=True)).astype(jnp.bfloat16)
        )
    attended = jnp.concatenate(attended, axis=1)
    swapped = lax.all_to_all(
        attended.reshape(group, rows_dev, heads_dev * VALUE_WIDTH),
        "tp",
        split_axis=0,
        concat_axis=0,
        tiled=True,
    )
    own_rows = jnp.transpose(swapped, (1, 0, 2)).reshape(rows_dev, group * heads_dev * VALUE_WIDTH)
    projected = jnp.dot(own_rows, out_weight, preferred_element_type=jnp.float32)
    hidden = (residual.astype(jnp.float32) + projected).astype(jnp.bfloat16)
    normed = norm_scale(hidden, ffn_gain).astype(jnp.bfloat16)
    rows = lax.all_gather(normed, ("sp", "tp"), axis=0, tiled=True)
    active = expert_active(rows, gate_weight[0], up_weight[0])
    product = jnp.dot(active, down_weight[0], preferred_element_type=jnp.float32)
    mixture = lax.psum_scatter(
        (own_share * product).astype(jnp.bfloat16),
        ("sp", "tp"),
        scatter_dimension=0,
        tiled=True,
    )
    return (hidden.astype(jnp.float32) + mixture.astype(jnp.float32)).astype(jnp.bfloat16)


def solution(mesh):
    placed = (
        P(("grp", "sp"), "tp"),
        P(("grp", "sp"), "tp"),
        P(("grp", "sp"), None),
        P(("grp", "sp"), None),
        P(),
        P(None, "tp"),
        P(None, "tp"),
        P(("grp", "sp", "tp"), None),
        P(),
        P(),
        P("sp", None, "tp"),
        P("sp", None, "tp"),
        P("sp", "tp", None),
        P(("grp", "sp", "tp"), None),
        P(("grp", "sp", "tp"), None),
    )
    return jax.shard_map(
        on_device,
        mesh=mesh,
        in_specs=placed,
        out_specs=P(("grp", "sp", "tp"), None),
        check_vma=False,
    )
```

```python
import functools

import jax
import jax.numpy as jnp
import numpy as np
from jax import lax
from jax.experimental import pallas as pl
from jax.experimental.pallas import tpu as pltpu
from jax.sharding import PartitionSpec as P

PLAIN_HEAD_WIDTH = 128
QK_ROPE = 64
VALUE_WIDTH = 128
GRID_W = 64


theta = 10000.0
eps = 1e-06
limit = 7.0
slope = 1.702
CORES = 2
EARLY_ROWS = 32
VMEM_BYTES = 60 * 2**20


def turn(vector, row_shift, col_shift):
    width = vector.shape[-1]
    count = width // 4
    half = width // 2
    freqs = theta ** (-jnp.arange(count, dtype=jnp.float32) / count)
    extra = (1,) * (vector.ndim - 2)
    pieces = []
    for portion, shift in ((vector[..., :half], row_shift), (vector[..., half:], col_shift)):
        angle = (shift.astype(jnp.float32)[:, None] * freqs[None, :]).reshape(
            (shift.shape[0],) + extra + (count,)
        )
        lower = portion[..., :count]
        upper = portion[..., count:]
        pieces.append(
            jnp.concatenate(
                [
                    lower * jnp.cos(angle) - upper * jnp.sin(angle),
                    lower * jnp.sin(angle) + upper * jnp.cos(angle),
                ],
                axis=-1,
            )
        )
    return jnp.concatenate(pieces, axis=-1)


def norm_scale(values, gain):
    wide = values.astype(jnp.float32)
    return (
        wide
        * lax.rsqrt(jnp.mean(wide * wide, axis=-1, keepdims=True) + eps)
        * gain.astype(jnp.float32)
    )


def expert_active(rows, gate_w, up_w):
    gate_pre = jnp.minimum(jnp.dot(rows, gate_w, preferred_element_type=jnp.float32), limit)
    up_pre = jnp.clip(jnp.dot(rows, up_w, preferred_element_type=jnp.float32), -limit, limit)
    return ((up_pre + 1.0) * gate_pre * jax.nn.sigmoid(slope * gate_pre)).astype(jnp.bfloat16)


def flipped(index, mask):
    out = index
    bit = 1
    while bit <= mask:
        if mask & bit:
            out = out + bit - 2 * bit * ((index // bit) % 2)
        bit *= 2
    return out


def gatherer(chips, group, own, gathered, sems, launch):
    z_send, z_recv, x_send, x_recv, c_send, c_recv = sems
    place = lax.axis_index("sp")
    column = lax.axis_index("tp")
    chip, core = place // CORES, place % CORES
    per_chip = CORES * group
    partner = {"sp": chip * CORES + 1 - core}

    def other(shift):
        return (column + shift) % group

    def slot(k, core_at, column_at):
        return flipped(chip, k) * per_chip + core_at * group + column_at

    def chip_peer(k):
        return {"sp": flipped(chip, k) * CORES + core}

    def remote(src, dst, send_sem, recv_sem, device):
        return pltpu.make_async_remote_copy(
            src_ref=src, dst_ref=dst, send_sem=send_sem, recv_sem=recv_sem, device_id=device
        )

    def greet():
        barrier = pltpu.get_barrier_semaphore()
        pl.semaphore_signal(barrier, inc=1, device_id=partner)
        for k in range(1, chips):
            pl.semaphore_signal(barrier, inc=1, device_id=chip_peer(k))
        for shift in range(1, group):
            pl.semaphore_signal(barrier, inc=1, device_id={"tp": other(shift)})

    def met():
        pl.semaphore_wait(pltpu.get_barrier_semaphore(), chips + group - 1)

    def source(k, back):
        if k == 0 and back == 0:
            return own
        return gathered.at[slot(k, core, other(group - back))]

    def chip_wait(k):
        landed = gathered.at[slot(k, core, column)]
        remote(landed, landed, z_send.at[k], z_recv.at[k], chip_peer(k)).wait_recv()

    def core_copy(k, back):
        return remote(
            source(k, back),
            gathered.at[slot(k, core, other(group - back))],
            c_send.at[k, back],
            c_recv.at[k, back],
            partner,
        )

    def core_wait(k, back):
        landed = gathered.at[slot(k, 1 - core, other(group - back))]
        remote(landed, landed, c_send.at[k, back], c_recv.at[k, back], partner).wait_recv()

    def tp_copy(k, shift):
        return remote(
            source(k, 0),
            gathered.at[slot(k, core, column)],
            x_send.at[k, shift],
            x_recv.at[k, shift],
            {"tp": other(shift)},
        )

    def tp_wait(k, shift):
        landed = gathered.at[slot(k, core, other(group - shift))]
        remote(
            landed, landed, x_send.at[k, shift], x_recv.at[k, shift], {"tp": other(shift)}
        ).wait_recv()

    def spread(k):
        for shift in range(1, group):
            launch(tp_copy(k, shift))
        launch(core_copy(k, 0))

    def begin():
        for k in range(1, chips):
            launch(
                remote(
                    own,
                    gathered.at[slot(0, core, column)],
                    z_send.at[k],
                    z_recv.at[k],
                    chip_peer(k),
                )
            )
        spread(0)

    def step(k):
        if k + 1 < chips:
            chip_wait(k + 1)
            spread(k + 1)
        for shift in range(1, group):
            tp_wait(k, shift)
            launch(core_copy(k, shift))
        for back in range(group):
            core_wait(k, back)

    return greet, met, begin, step, slot, chip_peer, partner, other, remote


def turn_matrices(shape, width):
    row = lax.broadcasted_iota(jnp.int32, shape, 0)
    col = lax.broadcasted_iota(jnp.int32, shape, 1)
    count = width // 4
    lane = col % 128
    source = (col // 128) * width + lane
    inside = lane < width
    lower = lane % (2 * count) < count
    straight = jnp.where(inside & (row == source), 1.0, 0.0)
    moved = jnp.where(lower, source + count, source - count)
    sign = jnp.where(lower, -1.0, 1.0)
    crossed = jnp.where(inside & (row == moved), sign, 0.0)
    return straight.astype(jnp.bfloat16), crossed.astype(jnp.bfloat16)


def attention_kernel(
    chips,
    group,
    *refs,
):
    inputs, refs = refs[:10], refs[10:]
    out_ref, share_ref, own, gathered, queries, cosines, sines, key_turns = refs[:8]
    held, load_sem, sems = refs[8:18], refs[18], refs[19:]
    (
        latent_ref,
        gain_ref,
        freqs_ref,
        key_turn_ref,
        routes_ref,
        route_weights_ref,
        query_turn_ref,
        query_ref,
        keyw_ref,
        valuew_ref,
    ) = held
    place = lax.axis_index("sp")
    column = lax.axis_index("tp")
    tokens, latent_width = inputs[0].shape
    rows_dev = own.shape[0]
    heads_dev = inputs[7].shape[1] // PLAIN_HEAD_WIDTH
    count = lax.axis_size("sp")
    per_chip = CORES * group
    sends = []

    def launch(copy):
        copy.start()
        sends.append(copy)

    greet, met, begin, step, slot = gatherer(chips, group, own, gathered, sems, launch)[:5]
    greet()
    loads = [
        pltpu.make_async_copy(src, dst, load_sem.at[i])
        for i, (src, dst) in enumerate(zip(inputs, held))
    ]
    for load in loads:
        load.start()
    loads[2].wait()

    at = place * tokens + lax.broadcasted_iota(jnp.int32, (tokens, 128), 0)
    lane = lax.broadcasted_iota(jnp.int32, (tokens, 128), 1)
    shift = jnp.where(lane < QK_ROPE // 2, at // GRID_W, at % GRID_W).astype(jnp.float32)
    angle = shift * freqs_ref[...]
    cosines[...] = jnp.cos(angle)
    sines[...] = jnp.sin(angle)

    def turned(vector, matrices, cos, sin):
        straight, crossed = (
            jnp.dot(vector, matrix, preferred_element_type=jnp.float32) for matrix in matrices
        )
        return straight * cos + crossed * sin

    mine = pl.ds(pl.multiple_of(column * rows_dev, 16), rows_dev)
    for load in loads[:2] + loads[3:6]:
        load.wait()
    key_turns[...] = key_turn_ref[...].T
    named = routes_ref[...].T
    weighing = route_weights_ref[...].T
    key_rot = turned(
        key_turns[mine, :],
        turn_matrices((QK_ROPE, 128), QK_ROPE),
        cosines[mine, :],
        sines[mine, :],
    )
    lane = lax.broadcasted_iota(jnp.int32, (rows_dev, 128), 1) - QK_ROPE
    expert = jnp.where(lane < count, lane, lane - count)
    share = jnp.zeros((rows_dev, 128), jnp.float32)
    for k in range(named.shape[1]):
        share = share + jnp.where(named[:, k : k + 1] == expert, weighing[:, k : k + 1], 0.0)
    high = share.astype(jnp.bfloat16).astype(jnp.float32)
    packed = jnp.where(lane < count, high, share - high)
    packed = jnp.where(lane < 2 * count, packed, 0.0)
    own[:, :latent_width] = norm_scale(latent_ref[mine, :], gain_ref[...].reshape(1, latent_width)).astype(jnp.bfloat16)
    own[:, latent_width:] = jnp.where(lane < 0, key_rot, packed).astype(jnp.bfloat16)
    met()
    begin()
    gathered[slot(0, place % CORES, column)] = own[...]

    for load in loads[6:]:
        load.wait()
    matrices = turn_matrices((heads_dev * QK_ROPE, heads_dev * 128), QK_ROPE)
    straight, crossed = (
        jnp.dot(query_turn_ref[...], matrix, preferred_element_type=jnp.float32)
        for matrix in matrices
    )
    for head in range(heads_dev):
        span = slice(head * 128, (head + 1) * 128)
        queries[head, :, :128] = query_ref[:, span]
        queries[head, :, 128:] = (
            straight[:, span] * cosines[...] + crossed[:, span] * sines[...]
        ).astype(jnp.bfloat16)

    scale = (PLAIN_HEAD_WIDTH + QK_ROPE) ** (-0.5)
    peaks = [None] * heads_dev
    sums = [None] * heads_dev
    totals = [None] * heads_dev
    for k in range(chips):
        step(k)
        first = slot(k, 0, 0)
        width = per_chip * rows_dev
        latents = gathered[pl.ds(first, per_chip), :, :latent_width].reshape(width, latent_width)
        rot = gathered[pl.ds(first, per_chip), :, latent_width:].reshape(width, 128)
        keys = jnp.dot(latents, keyw_ref[...], preferred_element_type=jnp.float32).astype(
            jnp.bfloat16
        )
        values = jnp.dot(latents, valuew_ref[...], preferred_element_type=jnp.float32).astype(
            jnp.bfloat16
        )
        for head in range(heads_dev):
            span = slice(head * 128, (head + 1) * 128)
            scores = scale * lax.dot_general(
                queries[head],
                jnp.concatenate([keys[:, span], rot], axis=1),
                (((1,), (1,)), ((), ())),
                preferred_element_type=jnp.float32,
            )
            peak = jnp.max(scores, axis=1, keepdims=True)
            if k:
                peak = jnp.maximum(peak, peaks[head])
            weights = jnp.exp(scores - peak)
            total = jnp.sum(weights, axis=1, keepdims=True)
            summed = jnp.dot(
                weights.astype(jnp.bfloat16), values[:, span], preferred_element_type=jnp.float32
            )
            if k:
                fade = jnp.exp(peaks[head] - peak)
                total = total + fade * sums[head]
                summed = summed + fade * totals[head]
            peaks[head], sums[head], totals[head] = peak, total, summed
        lane = lax.broadcasted_iota(jnp.int32, (width, 128), 1) - QK_ROPE
        named = (lane == place) | (lane == place + count)
        share_ref[pl.ds(first, per_chip)] = jnp.sum(
            jnp.where(named, rot.astype(jnp.float32), 0.0), axis=1, keepdims=True
        ).reshape(per_chip, rows_dev, 1)
    for head in range(heads_dev):
        out_ref[:, head * 128 : (head + 1) * 128] = (totals[head] / sums[head]).astype(jnp.bfloat16)
    for copy in sends:
        copy.wait_send()


def gather_sems(chips, group):
    dma = pltpu.SemaphoreType.DMA
    return [dma((chips,))] * 2 + [dma((chips, group))] * 4


def run_attention(query, query_turn, latent, key_turn, gain, routes, route_weights, key_w, value_w):
    group = lax.axis_size("tp")
    chips = lax.axis_size("sp") // CORES
    blocks = chips * CORES * group
    tokens, latent_width = latent.shape
    rows_dev = routes.shape[0]
    heads_dev = query.shape[1] // PLAIN_HEAD_WIDTH
    quarter = QK_ROPE // 4
    freqs = theta ** (-np.arange(quarter, dtype=np.float32) / np.float32(quarter))
    freqs = np.tile(freqs.astype(np.float32), 128 // quarter).reshape(1, 128)
    dma = pltpu.SemaphoreType.DMA
    whole = pl.BlockSpec(memory_space=pltpu.VMEM)
    sent = latent_width + 128
    arrays = (
        latent,
        gain,
        jnp.asarray(freqs),
        key_turn.T,
        routes.T,
        route_weights.T,
        query_turn,
        query,
        key_w,
        value_w,
    )
    return pl.pallas_call(
        functools.partial(attention_kernel, chips, group),
        out_shape=[
            jax.ShapeDtypeStruct((tokens, heads_dev * VALUE_WIDTH), jnp.bfloat16),
            jax.ShapeDtypeStruct((blocks, rows_dev, 1), jnp.float32),
        ],
        in_specs=[pl.BlockSpec(memory_space=pltpu.HBM)] * len(arrays),
        out_specs=[whole, whole],
        scratch_shapes=[
            pltpu.VMEM((rows_dev, sent), jnp.bfloat16),
            pltpu.VMEM((blocks, rows_dev, sent), jnp.bfloat16),
            pltpu.VMEM((heads_dev, tokens, 256), jnp.bfloat16),
            pltpu.VMEM((tokens, 128), jnp.float32),
            pltpu.VMEM((tokens, 128), jnp.float32),
            pltpu.VMEM((tokens, QK_ROPE), jnp.bfloat16),
        ]
        + [pltpu.VMEM(array.shape, array.dtype) for array in arrays]
        + [dma((len(arrays),))]
        + gather_sems(chips, group),
        compiler_params=pltpu.CompilerParams(
            collective_id=1, has_side_effects=True, vmem_limit_bytes=VMEM_BYTES
        ),
    )(*arrays)


def neighbour_order(chips):
    table = []
    for z in range(chips):
        table.append(sorted(range(chips), key=lambda o: (abs(o - z), o if z < chips // 2 else -o)))
    return table


def pick(z, values):
    out = values[0]
    for at in range(1, len(values)):
        out = jnp.where(z == at, values[at], out)
    return out


def experts_kernel(
    chips,
    early,
    attended_ref,
    share_ref,
    residual_hbm,
    gain_hbm,
    out_hbm,
    gate_hbm,
    up_hbm,
    down_hbm,
    out_ref,
    heads,
    hidden,
    gathered,
    partial,
    from_core,
    from_x,
    from_x_early,
    from_z,
    from_z_early,
    residual_ref,
    gain_ref,
    outw_ref,
    gate_ref,
    up_ref,
    down_ref,
    load_sem,
    h_send,
    h_recv,
    gz_send,
    gz_recv,
    gx_send,
    gx_recv,
    gc_send,
    gc_recv,
    rc_send,
    rc_recv,
    rx_send,
    rx_recv,
    rz_send,
    rz_recv,
):
    place = lax.axis_index("sp")
    column = lax.axis_index("tp")
    chip, core = place // CORES, place % CORES
    across = 1 - column
    rows_dev, model_width = hidden.shape
    late = rows_dev - early
    table = neighbour_order(chips)
    order = [chip] + [pick(chip, [table[z][j] for z in range(chips)]) for j in range(1, chips)]
    far = [0] + [
        pick(chip, [abs(table[z][j] - z) for z in range(chips)]) for j in range(1, chips)
    ]
    sends = []
    first_rows = pl.ds(0, early)
    last_rows = pl.ds(early, late)

    def launch(copy, when=None):
        if when is None:
            copy.start()
        else:
            pl.when(when)(copy.start)
        sends.append((copy, when))

    def remote(src, dst, send_sem, recv_sem, device):
        return pltpu.make_async_remote_copy(
            src_ref=src, dst_ref=dst, send_sem=send_sem, recv_sem=recv_sem, device_id=device
        )

    def on_chip(at):
        return {"sp": at * CORES + core}

    partner = {"sp": chip * CORES + 1 - core}
    beside = {"tp": across}

    barrier = pltpu.get_barrier_semaphore()
    pl.semaphore_signal(barrier, inc=1, device_id=partner)
    pl.semaphore_signal(barrier, inc=1, device_id=beside)
    for j in range(1, chips):
        pl.semaphore_signal(barrier, inc=1, device_id=on_chip((chip + j) % chips))
    loads = [
        pltpu.make_async_copy(src, dst, load_sem.at[i])
        for i, (src, dst) in enumerate(
            (
                (residual_hbm, residual_ref),
                (gain_hbm, gain_ref),
                (out_hbm, outw_ref),
                (gate_hbm, gate_ref),
                (up_hbm, up_ref),
                (down_hbm, down_ref),
            )
        )
    ]
    for load in loads:
        load.start()
    pl.semaphore_wait(barrier, chips + 1)

    swap = remote(attended_ref.at[across], heads.at[column], h_send, h_recv, beside)
    launch(swap)
    heads[column] = attended_ref[column]
    for load in loads[:3]:
        load.wait()
    landed = heads.at[across]
    remote(landed, landed, h_send, h_recv, beside).wait_recv()
    joined = jnp.concatenate([heads[0], heads[1]], axis=1)
    projected = jnp.dot(joined, outw_ref[...], preferred_element_type=jnp.float32)
    mixed = (residual_ref[...].astype(jnp.float32) + projected).astype(jnp.bfloat16)
    gathered[place, column] = norm_scale(mixed, gain_ref[...].reshape(1, model_width)).astype(jnp.bfloat16)
    hidden[...] = mixed

    kinds = ((0, last_rows), (0, first_rows), (1, first_rows), (1, last_rows))
    use = [k for k in range(4) if (late if k in (0, 3) else early)]

    def piece(at, core_at, kind):
        flip, rows = kinds[kind]
        return gathered.at[at * CORES + core_at, across if flip else column, rows]

    def gz_copy(at, kind, to, lane):
        ref = piece(at, core, kind)
        return remote(ref, ref, gz_send.at[at, kind, lane], gz_recv.at[at, kind], on_chip(to))

    def gz_wait(at, kind):
        ref = piece(at, core, kind)
        remote(
            ref, ref, gz_send.at[at, kind, 0], gz_recv.at[at, kind], on_chip(at)
        ).wait_recv()

    def gx_copy(at, kind):
        ref = piece(at, core, kind)
        return remote(ref, ref, gx_send.at[at, kind], gx_recv.at[at, kind], beside)

    def gx_wait(at, kind):
        ref = piece(at, core, 3 - kind)
        remote(ref, ref, gx_send.at[at, kind], gx_recv.at[at, kind], beside).wait_recv()

    def gc_copy(at, kind):
        ref = piece(at, core, kind)
        return remote(ref, ref, gc_send.at[at, kind], gc_recv.at[at, kind], partner)

    def gc_wait(at, kind):
        ref = piece(at, 1 - core, kind)
        remote(ref, ref, gc_send.at[at, kind], gc_recv.at[at, kind], partner).wait_recv()

    def both_ways(kind):
        launch(gz_copy(chip, kind, chip - 1, 0), chip > 0)
        launch(gz_copy(chip, kind, chip + 1, 1), chip < chips - 1)

    def begin():
        if early:
            launch(gx_copy(chip, 1))
        if late:
            both_ways(0)
            launch(gx_copy(chip, 0))
        if early:
            both_ways(1)
        for kind in use:
            if kind < 2:
                launch(gc_copy(chip, kind))
        if early:
            gx_wait(chip, 1)
            both_ways(2)
            launch(gc_copy(chip, 2))

    def forward(at, now=None):
        step = jnp.where(at < chip, 1, -1)
        more = jnp.where(at < chip, chip < chips - 1, chip > 0)
        for kind in use:
            if kind == 3:
                continue
            if now is None:
                gz_wait(at, kind)
            else:
                pl.when(now)(functools.partial(gz_wait, at, kind))
            launch(gz_copy(at, kind, chip + step, 0), more if now is None else now & more)
            if kind == 0:
                launch(gx_copy(at, 0), now)
            launch(gc_copy(at, kind), now)

    def crossed(at):
        if late:
            gx_wait(at, 0)
            launch(gc_copy(at, 3))

    def apply(load_from, count, store_to):
        active = expert_active(load_from(gathered).reshape(count, model_width), gate_ref[...], up_ref[...])
        product = jnp.dot(active, down_ref[...], preferred_element_type=jnp.float32)
        store_to((product * load_from(share_ref).reshape(count, 1)).astype(jnp.bfloat16))

    def pair(at):
        return pl.ds(at * CORES, CORES)

    def compute_early(at):
        if not early:
            return
        gc_wait(at, 1)
        gc_wait(at, 2)

        def store(value):
            partial[pair(at), :, first_rows] = value.reshape(CORES, 2, early, model_width)

        apply(lambda ref: ref[pair(at), :, first_rows], 2 * CORES * early, store)
        launch(core_sum_early(at))

    def compute_late(at, kind):
        if not late:
            return
        gc_wait(at, kind)
        side = across if kind else column

        def store(value):
            partial[pair(at), side, last_rows] = value.reshape(CORES, late, model_width)

        apply(lambda ref: ref[pair(at), side, last_rows], CORES * late, store)
        launch(core_sum_late(at, kind))

    def core_sum_early(at):
        return remote(
            partial.at[at * CORES + 1 - core, :, first_rows],
            from_core.at[at, :, first_rows],
            rc_send.at[at, 1],
            rc_recv.at[at, 1],
            partner,
        )

    def core_sum_late(at, kind):
        side = across if kind else column
        return remote(
            partial.at[at * CORES + 1 - core, side, last_rows],
            from_core.at[at, side, last_rows],
            rc_send.at[at, kind],
            rc_recv.at[at, kind],
            partner,
        )

    def x_sum(at):
        return remote(
            partial.at[at * CORES + core, across, last_rows],
            from_x.at[at],
            rx_send.at[at],
            rx_recv.at[at],
            beside,
        )

    def z_sum_early(at, sender):
        return remote(
            partial.at[at * CORES + core, :, first_rows],
            from_z_early.at[sender],
            rz_send.at[at, 0],
            rz_recv.at[sender, 0],
            on_chip(at),
        )

    def z_sum_late(at, sender):
        return remote(
            partial.at[at * CORES + core, column, last_rows],
            from_z.at[sender],
            rz_send.at[at, 1],
            rz_recv.at[sender, 1],
            on_chip(at),
        )

    def wide(value):
        return value.astype(jnp.float32)

    def sum_early(j):
        at = order[j]
        if not early:
            return
        core_sum_early(at).wait_recv()
        mine = at * CORES + core
        partial[mine, :, first_rows] = (
            wide(partial[mine, :, first_rows]) + wide(from_core[at, :, first_rows])
        ).astype(jnp.bfloat16)
        if j:
            launch(z_sum_early(at, chip))

    def sum_late(j, kind):
        at = order[j]
        if not late:
            return
        core_sum_late(at, kind).wait_recv()
        mine = at * CORES + core
        side = across if kind else column
        partial[mine, side, last_rows] = (
            wide(partial[mine, side, last_rows]) + wide(from_core[at, side, last_rows])
        ).astype(jnp.bfloat16)
        if kind:
            launch(x_sum(at))

    def sum_across(j):
        at = order[j]
        if not late:
            return
        x_sum(at).wait_recv()
        mine = at * CORES + core
        partial[mine, column, last_rows] = (
            wide(partial[mine, column, last_rows]) + wide(from_x[at])
        ).astype(jnp.bfloat16)
        if j:
            launch(z_sum_late(at, chip))

    def arrive(distance):
        for j in range(distance, min(2 * distance, chips - 1) + 1):
            if all(abs(table[z][j] - z) == distance for z in range(chips)):
                forward(order[j])
            else:
                forward(order[j], far[j] == distance)

    begin()
    for load in loads[3:]:
        load.wait()
    compute_early(chip)
    compute_late(chip, 0)
    for j in range(chips):
        at = order[j]
        if j == 0:
            arrive(1)
        crossed(at)
        if j:
            compute_early(at)
            compute_late(at, 0)
        compute_late(at, 3)
        sum_early(j)
        sum_late(j, 3)
        sum_late(j, 0)
        if j:
            sum_across(j - 1)
            arrive(j + 1)
    sum_across(chips - 1)
    mine = chip * CORES + core
    if early:
        total = wide(partial[mine, :, first_rows])
        for j in range(1, chips):
            z_sum_early(chip, order[j]).wait_recv()
            total = total + wide(from_z_early[order[j]])
        partial[mine, :, first_rows] = total.astype(jnp.bfloat16)
        last = remote(
            partial.at[mine, across, first_rows],
            from_x_early,
            rx_send.at[chips],
            rx_recv.at[chips],
            beside,
        )
        launch(last)
    if late:
        total = wide(hidden[last_rows]) + wide(partial[mine, column, last_rows])
        for j in range(1, chips):
            z_sum_late(chip, order[j]).wait_recv()
            total = total + wide(from_z[order[j]])
        out_ref[last_rows] = total.astype(jnp.bfloat16)
    if early:
        last.wait_recv()
        out_ref[first_rows] = (
            wide(hidden[first_rows]) + wide(partial[mine, column, first_rows]) + wide(from_x_early[...])
        ).astype(jnp.bfloat16)
    for copy, when in sends:
        if when is None:
            copy.wait_send()
        else:
            pl.when(when)(copy.wait_send)


def run_experts(attended, residual, gain, shares, out_w, gate_w, up_w, down_w):
    chips = lax.axis_size("sp") // CORES
    rows_dev, model_width = residual.shape
    pairs = chips * CORES
    early = EARLY_ROWS if rows_dev > EARLY_ROWS else 0
    late = rows_dev - early
    dma = pltpu.SemaphoreType.DMA
    block = (rows_dev, model_width)
    heads = (2, rows_dev, attended.shape[1])
    whole = pl.BlockSpec(memory_space=pltpu.VMEM)

    def vmem(*shape):
        return pltpu.VMEM(shape, jnp.bfloat16)

    return pl.pallas_call(
        functools.partial(experts_kernel, chips, early),
        out_shape=jax.ShapeDtypeStruct(block, jnp.bfloat16),
        in_specs=[whole] * 2 + [pl.BlockSpec(memory_space=pltpu.HBM)] * 6,
        out_specs=whole,
        scratch_shapes=[
            vmem(*heads),
            vmem(*block),
            vmem(pairs, 2, *block),
            vmem(pairs, 2, *block),
            vmem(chips, 2, *block),
            vmem(chips, late, model_width),
            vmem(max(early, 16), model_width),
            vmem(chips, late, model_width),
            vmem(chips, 2, max(early, 16), model_width),
            vmem(*block),
            vmem(*gain.shape),
            vmem(*out_w.shape),
            vmem(*gate_w.shape),
            vmem(*up_w.shape),
            vmem(*down_w.shape),
            dma((6,)),
            dma,
            dma,
            dma((chips, 3, 2)),
            dma((chips, 3)),
            dma((chips, 2)),
            dma((chips, 2)),
            dma((chips, 4)),
            dma((chips, 4)),
            dma((chips, 4)),
            dma((chips, 4)),
            dma((chips + 1,)),
            dma((chips + 1,)),
            dma((chips, 2)),
            dma((chips, 2)),
        ],
        compiler_params=pltpu.CompilerParams(
            collective_id=0, has_side_effects=True, vmem_limit_bytes=VMEM_BYTES
        ),
    )(
        attended.reshape(heads),
        shares.reshape(pairs, 2, rows_dev, 1),
        residual,
        gain,
        out_w,
        gate_w,
        up_w,
        down_w,
    )


def experts_fit(tokens, rows_dev, model_width):
    group, places = lax.axis_size("tp"), lax.axis_size("sp")
    chips = places // CORES
    if group != 2 or places % CORES or chips & (chips - 1) or rows_dev % 16:
        return False
    if tokens != group * rows_dev or QK_ROPE + 2 * places > 128:
        return False
    return 3 * places * group * rows_dev * model_width * 2 < VMEM_BYTES // 2


def on_device(
    query_plain,
    query_turn,
    latent,
    key_turn,
    latent_norm_scale,
    plain_key_matrix,
    value_matrix,
    residual,
    out_weight,
    ffn_gain,
    gate_weight,
    up_weight,
    down_weight,
    routes,
    route_weights,
):
    if experts_fit(latent.shape[0], *residual.shape):
        attended, own_share = run_attention(
            query_plain,
            query_turn,
            latent,
            key_turn,
            latent_norm_scale,
            routes,
            route_weights,
            plain_key_matrix,
            value_matrix,
        )
        return run_experts(
            attended,
            residual,
            ffn_gain,
            own_share,
            out_weight,
            gate_weight[0],
            up_weight[0],
            down_weight[0],
        )
    tok_dev = latent.shape[0]
    heads_dev = query_plain.shape[1] // PLAIN_HEAD_WIDTH
    model_width = residual.shape[1]
    place = lax.axis_index("sp") * tok_dev + jnp.arange(tok_dev, dtype=jnp.int32)
    grid_row = place // GRID_W
    grid_col = place % GRID_W
    rows_dev, model_width = residual.shape
    group = lax.axis_size("tp")
    count = lax.axis_size("sp")
    expert_ids = jnp.arange(count, dtype=jnp.int32)
    share = jnp.sum(
        route_weights[..., None] * (routes[..., None] == expert_ids).astype(jnp.float32), axis=1
    )
    latent_width = latent.shape[1]
    wide = latent_width + QK_ROPE

    def key_side(latents, turns, at_row, at_col):
        normed_latent = norm_scale(latents, latent_norm_scale).astype(jnp.bfloat16)
        key_rot = turn(turns.astype(jnp.float32), at_row, at_col).astype(jnp.bfloat16)
        return [normed_latent, key_rot]

    sent = jnp.concatenate(key_side(latent, key_turn, grid_row, grid_col), axis=1)
    everyone = lax.all_gather(sent, "sp", axis=0, tiled=True)
    shares = lax.all_gather(share, ("sp", "tp"), axis=0, tiled=True)
    own_share = jnp.sum(
        jnp.where(expert_ids[None, :] == lax.axis_index("sp"), shares, 0.0), axis=1, keepdims=True
    )
    all_latent = everyone[:, :latent_width]
    all_rot = everyone[:, latent_width:wide]
    keys = jnp.dot(all_latent, plain_key_matrix, preferred_element_type=jnp.float32).astype(
        jnp.bfloat16
    )
    values = jnp.dot(all_latent, value_matrix, preferred_element_type=jnp.float32).astype(
        jnp.bfloat16
    )
    query_rot = turn(
        query_turn.astype(jnp.float32).reshape(tok_dev, heads_dev, QK_ROPE), grid_row, grid_col
    ).astype(jnp.bfloat16)
    scale = (PLAIN_HEAD_WIDTH + QK_ROPE) ** (-0.5)
    attended = []
    for head in range(heads_dev):
        span = slice(head * PLAIN_HEAD_WIDTH, (head + 1) * PLAIN_HEAD_WIDTH)
        scores = (
            jnp.einsum(
                "qd,kd->qk", query_plain[:, span], keys[:, span], preferred_element_type=jnp.float32
            )
            + jnp.einsum(
                "qd,kd->qk", query_rot[:, head], all_rot, preferred_element_type=jnp.float32
            )
        ) * scale
        weights = jnp.exp(scores - jnp.max(scores, axis=1, keepdims=True))
        summed = jnp.dot(
            weights.astype(jnp.bfloat16),
            values[:, head * VALUE_WIDTH : (head + 1) * VALUE_WIDTH],
            preferred_element_type=jnp.float32,
        )
        attended.append(
            (summed / jnp.sum(weights, axis=1, keepdims=True)).astype(jnp.bfloat16)
        )
    attended = jnp.concatenate(attended, axis=1)
    swapped = lax.all_to_all(
        attended.reshape(group, rows_dev, heads_dev * VALUE_WIDTH),
        "tp",
        split_axis=0,
        concat_axis=0,
        tiled=True,
    )
    own_rows = jnp.transpose(swapped, (1, 0, 2)).reshape(rows_dev, group * heads_dev * VALUE_WIDTH)
    projected = jnp.dot(own_rows, out_weight, preferred_element_type=jnp.float32)
    hidden = (residual.astype(jnp.float32) + projected).astype(jnp.bfloat16)
    normed = norm_scale(hidden, ffn_gain).astype(jnp.bfloat16)
    rows = lax.all_gather(normed, ("sp", "tp"), axis=0, tiled=True)
    active = expert_active(rows, gate_weight[0], up_weight[0])
    product = jnp.dot(active, down_weight[0], preferred_element_type=jnp.float32)
    mixture = lax.psum_scatter(
        (own_share * product).astype(jnp.bfloat16),
        ("sp", "tp"),
        scatter_dimension=0,
        tiled=True,
    )
    return (hidden.astype(jnp.float32) + mixture.astype(jnp.float32)).astype(jnp.bfloat16)


def solution(mesh):
    placed = (
        P(("grp", "sp"), "tp"),
        P(("grp", "sp"), "tp"),
        P(("grp", "sp"), None),
        P(("grp", "sp"), None),
        P(),
        P(None, "tp"),
        P(None, "tp"),
        P(("grp", "sp", "tp"), None),
        P(),
        P(),
        P("sp", None, "tp"),
        P("sp", None, "tp"),
        P("sp", "tp", None),
        P(("grp", "sp", "tp"), None),
        P(("grp", "sp", "tp"), None),
    )
    return jax.shard_map(
        on_device,
        mesh=mesh,
        in_specs=placed,
        out_specs=P(("grp", "sp", "tp"), None),
        check_vma=False,
    )
```

```python
import functools

import jax
import jax.numpy as jnp
import numpy as np
from jax import lax
from jax.experimental import pallas as pl
from jax.experimental.pallas import tpu as pltpu
from jax.sharding import PartitionSpec as P

PLAIN_HEAD_WIDTH = 128
QK_ROPE = 64
VALUE_WIDTH = 128
GRID_W = 64


theta = 10000.0
eps = 1e-06
limit = 7.0
slope = 1.702
CORES = 2
EARLY_ROWS = 32
VMEM_BYTES = 60 * 2**20


def turn(vector, row_shift, col_shift):
    width = vector.shape[-1]
    count = width // 4
    half = width // 2
    freqs = theta ** (-jnp.arange(count, dtype=jnp.float32) / count)
    extra = (1,) * (vector.ndim - 2)
    pieces = []
    for portion, shift in ((vector[..., :half], row_shift), (vector[..., half:], col_shift)):
        angle = (shift.astype(jnp.float32)[:, None] * freqs[None, :]).reshape(
            (shift.shape[0],) + extra + (count,)
        )
        lower = portion[..., :count]
        upper = portion[..., count:]
        pieces.append(
            jnp.concatenate(
                [
                    lower * jnp.cos(angle) - upper * jnp.sin(angle),
                    lower * jnp.sin(angle) + upper * jnp.cos(angle),
                ],
                axis=-1,
            )
        )
    return jnp.concatenate(pieces, axis=-1)


def norm_scale(values, gain):
    wide = values.astype(jnp.float32)
    return (
        wide
        * lax.rsqrt(jnp.mean(wide * wide, axis=-1, keepdims=True) + eps)
        * gain.astype(jnp.float32)
    )


def expert_active(rows, gate_w, up_w):
    gate_pre = jnp.minimum(jnp.dot(rows, gate_w, preferred_element_type=jnp.float32), limit)
    up_pre = jnp.clip(jnp.dot(rows, up_w, preferred_element_type=jnp.float32), -limit, limit)
    return ((up_pre + 1.0) * gate_pre * jax.nn.sigmoid(slope * gate_pre)).astype(jnp.bfloat16)


def flipped(index, mask):
    out = index
    bit = 1
    while bit <= mask:
        if mask & bit:
            out = out + bit - 2 * bit * ((index // bit) % 2)
        bit *= 2
    return out


def gatherer(chips, group, own, gathered, sems, launch):
    z_send, z_recv, x_send, x_recv, c_send, c_recv = sems
    place = lax.axis_index("sp")
    column = lax.axis_index("tp")
    chip, core = place // CORES, place % CORES
    per_chip = CORES * group
    partner = {"sp": chip * CORES + 1 - core}

    def other(shift):
        return (column + shift) % group

    def slot(k, core_at, column_at):
        return flipped(chip, k) * per_chip + core_at * group + column_at

    def chip_peer(k):
        return {"sp": flipped(chip, k) * CORES + core}

    def remote(src, dst, send_sem, recv_sem, device):
        return pltpu.make_async_remote_copy(
            src_ref=src, dst_ref=dst, send_sem=send_sem, recv_sem=recv_sem, device_id=device
        )

    def greet():
        barrier = pltpu.get_barrier_semaphore()
        pl.semaphore_signal(barrier, inc=1, device_id=partner)
        for k in range(1, chips):
            pl.semaphore_signal(barrier, inc=1, device_id=chip_peer(k))
        for shift in range(1, group):
            pl.semaphore_signal(barrier, inc=1, device_id={"tp": other(shift)})

    def met():
        pl.semaphore_wait(pltpu.get_barrier_semaphore(), chips + group - 1)

    def source(k, back):
        if k == 0 and back == 0:
            return own
        return gathered.at[slot(k, core, other(group - back))]

    def chip_wait(k):
        landed = gathered.at[slot(k, core, column)]
        remote(landed, landed, z_send.at[k], z_recv.at[k], chip_peer(k)).wait_recv()

    def core_copy(k, back):
        return remote(
            source(k, back),
            gathered.at[slot(k, core, other(group - back))],
            c_send.at[k, back],
            c_recv.at[k, back],
            partner,
        )

    def core_wait(k, back):
        landed = gathered.at[slot(k, 1 - core, other(group - back))]
        remote(landed, landed, c_send.at[k, back], c_recv.at[k, back], partner).wait_recv()

    def tp_copy(k, shift):
        return remote(
            source(k, 0),
            gathered.at[slot(k, core, column)],
            x_send.at[k, shift],
            x_recv.at[k, shift],
            {"tp": other(shift)},
        )

    def tp_wait(k, shift):
        landed = gathered.at[slot(k, core, other(group - shift))]
        remote(
            landed, landed, x_send.at[k, shift], x_recv.at[k, shift], {"tp": other(shift)}
        ).wait_recv()

    def spread(k):
        for shift in range(1, group):
            launch(tp_copy(k, shift))
        launch(core_copy(k, 0))

    def begin():
        for k in range(1, chips):
            launch(
                remote(
                    own,
                    gathered.at[slot(0, core, column)],
                    z_send.at[k],
                    z_recv.at[k],
                    chip_peer(k),
                )
            )
        spread(0)

    def step(k):
        if k + 1 < chips:
            chip_wait(k + 1)
            spread(k + 1)
        for shift in range(1, group):
            tp_wait(k, shift)
            launch(core_copy(k, shift))
        for back in range(group):
            core_wait(k, back)

    return greet, met, begin, step, slot, chip_peer, partner, other, remote


def turn_matrices(shape, width):
    row = lax.broadcasted_iota(jnp.int32, shape, 0)
    col = lax.broadcasted_iota(jnp.int32, shape, 1)
    count = width // 4
    lane = col % 128
    source = (col // 128) * width + lane
    inside = lane < width
    lower = lane % (2 * count) < count
    straight = jnp.where(inside & (row == source), 1.0, 0.0)
    moved = jnp.where(lower, source + count, source - count)
    sign = jnp.where(lower, -1.0, 1.0)
    crossed = jnp.where(inside & (row == moved), sign, 0.0)
    return straight.astype(jnp.bfloat16), crossed.astype(jnp.bfloat16)


def attention_kernel(
    chips,
    group,
    *refs,
):
    inputs, refs = refs[:10], refs[10:]
    out_ref, share_ref, own, gathered, queries, cosines, sines, key_turns = refs[:8]
    held, load_sem, sems = refs[8:18], refs[18], refs[19:]
    (
        latent_ref,
        gain_ref,
        freqs_ref,
        key_turn_ref,
        routes_ref,
        route_weights_ref,
        query_turn_ref,
        query_ref,
        keyw_ref,
        valuew_ref,
    ) = held
    place = lax.axis_index("sp")
    column = lax.axis_index("tp")
    tokens, latent_width = inputs[0].shape
    rows_dev = own.shape[0]
    heads_dev = inputs[7].shape[1] // PLAIN_HEAD_WIDTH
    count = lax.axis_size("sp")
    per_chip = CORES * group
    sends = []

    def launch(copy):
        copy.start()
        sends.append(copy)

    greet, met, begin, step, slot = gatherer(chips, group, own, gathered, sems, launch)[:5]
    greet()
    loads = [
        pltpu.make_async_copy(src, dst, load_sem.at[i])
        for i, (src, dst) in enumerate(zip(inputs, held))
    ]
    for load in loads:
        load.start()
    loads[2].wait()

    at = place * tokens + lax.broadcasted_iota(jnp.int32, (tokens, 128), 0)
    lane = lax.broadcasted_iota(jnp.int32, (tokens, 128), 1)
    shift = jnp.where(lane < QK_ROPE // 2, at // GRID_W, at % GRID_W).astype(jnp.float32)
    angle = shift * freqs_ref[...]
    cosines[...] = jnp.cos(angle)
    sines[...] = jnp.sin(angle)

    def turned(vector, matrices, cos, sin):
        straight, crossed = (
            jnp.dot(vector, matrix, preferred_element_type=jnp.float32) for matrix in matrices
        )
        return straight * cos + crossed * sin

    mine = pl.ds(pl.multiple_of(column * rows_dev, 16), rows_dev)
    for load in loads[:2] + loads[3:6]:
        load.wait()
    key_turns[...] = key_turn_ref[...].T
    named = routes_ref[...].T
    weighing = route_weights_ref[...].T
    key_rot = turned(
        key_turns[mine, :],
        turn_matrices((QK_ROPE, 128), QK_ROPE),
        cosines[mine, :],
        sines[mine, :],
    )
    lane = lax.broadcasted_iota(jnp.int32, (rows_dev, 128), 1) - QK_ROPE
    expert = jnp.where(lane < count, lane, lane - count)
    share = jnp.zeros((rows_dev, 128), jnp.float32)
    for k in range(named.shape[1]):
        share = share + jnp.where(named[:, k : k + 1] == expert, weighing[:, k : k + 1], 0.0)
    high = share.astype(jnp.bfloat16).astype(jnp.float32)
    packed = jnp.where(lane < count, high, share - high)
    packed = jnp.where(lane < 2 * count, packed, 0.0)
    own[:, :latent_width] = norm_scale(latent_ref[mine, :], gain_ref[...].reshape(1, latent_width)).astype(jnp.bfloat16)
    own[:, latent_width:] = jnp.where(lane < 0, key_rot, packed).astype(jnp.bfloat16)
    met()
    begin()
    gathered[slot(0, place % CORES, column)] = own[...]

    for load in loads[6:]:
        load.wait()
    matrices = turn_matrices((heads_dev * QK_ROPE, heads_dev * 128), QK_ROPE)
    straight, crossed = (
        jnp.dot(query_turn_ref[...], matrix, preferred_element_type=jnp.float32)
        for matrix in matrices
    )
    for head in range(heads_dev):
        span = slice(head * 128, (head + 1) * 128)
        queries[head, :, :128] = query_ref[:, span]
        queries[head, :, 128:] = (
            straight[:, span] * cosines[...] + crossed[:, span] * sines[...]
        ).astype(jnp.bfloat16)

    scale = (PLAIN_HEAD_WIDTH + QK_ROPE) ** (-0.5)
    peaks = [None] * heads_dev
    sums = [None] * heads_dev
    totals = [None] * heads_dev
    for k in range(chips):
        step(k)
        first = slot(k, 0, 0)
        width = per_chip * rows_dev
        latents = gathered[pl.ds(first, per_chip), :, :latent_width].reshape(width, latent_width)
        rot = gathered[pl.ds(first, per_chip), :, latent_width:].reshape(width, 128)
        keys = jnp.dot(latents, keyw_ref[...], preferred_element_type=jnp.float32).astype(
            jnp.bfloat16
        )
        values = jnp.dot(latents, valuew_ref[...], preferred_element_type=jnp.float32).astype(
            jnp.bfloat16
        )
        for head in range(heads_dev):
            span = slice(head * 128, (head + 1) * 128)
            scores = scale * lax.dot_general(
                queries[head],
                jnp.concatenate([keys[:, span], rot], axis=1),
                (((1,), (1,)), ((), ())),
                preferred_element_type=jnp.float32,
            )
            peak = jnp.max(scores, axis=1, keepdims=True)
            if k:
                peak = jnp.maximum(peak, peaks[head])
            weights = jnp.exp(scores - peak)
            total = jnp.sum(weights, axis=1, keepdims=True)
            summed = jnp.dot(
                weights.astype(jnp.bfloat16), values[:, span], preferred_element_type=jnp.float32
            )
            if k:
                fade = jnp.exp(peaks[head] - peak)
                total = total + fade * sums[head]
                summed = summed + fade * totals[head]
            peaks[head], sums[head], totals[head] = peak, total, summed
        lane = lax.broadcasted_iota(jnp.int32, (width, 128), 1) - QK_ROPE
        named = (lane == place) | (lane == place + count)
        share_ref[pl.ds(first, per_chip)] = jnp.sum(
            jnp.where(named, rot.astype(jnp.float32), 0.0), axis=1, keepdims=True
        ).reshape(per_chip, rows_dev, 1)
    for head in range(heads_dev):
        out_ref[:, head * 128 : (head + 1) * 128] = (totals[head] / sums[head]).astype(jnp.bfloat16)
    for copy in sends:
        copy.wait_send()


def gather_sems(chips, group):
    dma = pltpu.SemaphoreType.DMA
    return [dma((chips,))] * 2 + [dma((chips, group))] * 4


def run_attention(query, query_turn, latent, key_turn, gain, routes, route_weights, key_w, value_w):
    group = lax.axis_size("tp")
    chips = lax.axis_size("sp") // CORES
    blocks = chips * CORES * group
    tokens, latent_width = latent.shape
    rows_dev = routes.shape[0]
    heads_dev = query.shape[1] // PLAIN_HEAD_WIDTH
    quarter = QK_ROPE // 4
    freqs = theta ** (-np.arange(quarter, dtype=np.float32) / np.float32(quarter))
    freqs = np.tile(freqs.astype(np.float32), 128 // quarter).reshape(1, 128)
    dma = pltpu.SemaphoreType.DMA
    whole = pl.BlockSpec(memory_space=pltpu.VMEM)
    sent = latent_width + 128
    arrays = (
        latent,
        gain,
        jnp.asarray(freqs),
        key_turn.T,
        routes.T,
        route_weights.T,
        query_turn,
        query,
        key_w,
        value_w,
    )
    return pl.pallas_call(
        functools.partial(attention_kernel, chips, group),
        out_shape=[
            jax.ShapeDtypeStruct((tokens, heads_dev * VALUE_WIDTH), jnp.bfloat16),
            jax.ShapeDtypeStruct((blocks, rows_dev, 1), jnp.float32),
        ],
        in_specs=[pl.BlockSpec(memory_space=pltpu.HBM)] * len(arrays),
        out_specs=[whole, whole],
        scratch_shapes=[
            pltpu.VMEM((rows_dev, sent), jnp.bfloat16),
            pltpu.VMEM((blocks, rows_dev, sent), jnp.bfloat16),
            pltpu.VMEM((heads_dev, tokens, 256), jnp.bfloat16),
            pltpu.VMEM((tokens, 128), jnp.float32),
            pltpu.VMEM((tokens, 128), jnp.float32),
            pltpu.VMEM((tokens, QK_ROPE), jnp.bfloat16),
        ]
        + [pltpu.VMEM(array.shape, array.dtype) for array in arrays]
        + [dma((len(arrays),))]
        + gather_sems(chips, group),
        compiler_params=pltpu.CompilerParams(
            collective_id=1, has_side_effects=True, vmem_limit_bytes=VMEM_BYTES
        ),
    )(*arrays)


def neighbour_order(chips):
    table = []
    for z in range(chips):
        table.append(sorted(range(chips), key=lambda o: (abs(o - z), o if z < chips // 2 else -o)))
    return table


def pick(z, values):
    out = values[0]
    for at in range(1, len(values)):
        out = jnp.where(z == at, values[at], out)
    return out


def experts_kernel(
    chips,
    early,
    attended_ref,
    share_ref,
    residual_hbm,
    gain_hbm,
    out_hbm,
    gate_hbm,
    up_hbm,
    down_hbm,
    out_ref,
    heads,
    hidden,
    gathered,
    partial,
    from_core,
    from_x,
    from_x_early,
    from_z,
    from_z_early,
    residual_ref,
    gain_ref,
    outw_ref,
    gate_ref,
    up_ref,
    down_ref,
    load_sem,
    h_send,
    h_recv,
    gz_send,
    gz_recv,
    gx_send,
    gx_recv,
    gc_send,
    gc_recv,
    rc_send,
    rc_recv,
    rx_send,
    rx_recv,
    rz_send,
    rz_recv,
):
    place = lax.axis_index("sp")
    column = lax.axis_index("tp")
    chip, core = place // CORES, place % CORES
    across = 1 - column
    rows_dev, model_width = hidden.shape
    late = rows_dev - early
    table = neighbour_order(chips)
    order = [chip] + [pick(chip, [table[z][j] for z in range(chips)]) for j in range(1, chips)]
    sends = []
    first_rows = pl.ds(0, early)
    last_rows = pl.ds(early, late)

    def launch(copy, when=None):
        if when is None:
            copy.start()
        else:
            pl.when(when)(copy.start)
        sends.append((copy, when))

    def remote(src, dst, send_sem, recv_sem, device):
        return pltpu.make_async_remote_copy(
            src_ref=src, dst_ref=dst, send_sem=send_sem, recv_sem=recv_sem, device_id=device
        )

    def on_chip(at):
        return {"sp": at * CORES + core}

    partner = {"sp": chip * CORES + 1 - core}
    beside = {"tp": across}

    barrier = pltpu.get_barrier_semaphore()
    pl.semaphore_signal(barrier, inc=1, device_id=partner)
    pl.semaphore_signal(barrier, inc=1, device_id=beside)
    for j in range(1, chips):
        pl.semaphore_signal(barrier, inc=1, device_id=on_chip((chip + j) % chips))
    loads = [
        pltpu.make_async_copy(src, dst, load_sem.at[i])
        for i, (src, dst) in enumerate(
            (
                (residual_hbm, residual_ref),
                (gain_hbm, gain_ref),
                (out_hbm, outw_ref),
                (gate_hbm, gate_ref),
                (up_hbm, up_ref),
                (down_hbm, down_ref),
            )
        )
    ]
    for load in loads:
        load.start()
    pl.semaphore_wait(barrier, chips + 1)

    swap = remote(attended_ref.at[across], heads.at[column], h_send, h_recv, beside)
    launch(swap)
    heads[column] = attended_ref[column]
    for load in loads[:3]:
        load.wait()
    landed = heads.at[across]
    remote(landed, landed, h_send, h_recv, beside).wait_recv()
    joined = jnp.concatenate([heads[0], heads[1]], axis=1)
    projected = jnp.dot(joined, outw_ref[...], preferred_element_type=jnp.float32)
    mixed = (residual_ref[...].astype(jnp.float32) + projected).astype(jnp.bfloat16)
    gathered[place, column] = norm_scale(mixed, gain_ref[...].reshape(1, model_width)).astype(jnp.bfloat16)
    hidden[...] = mixed

    kinds = ((0, last_rows), (0, first_rows), (1, first_rows), (1, last_rows))
    use = [k for k in range(4) if (late if k in (0, 3) else early)]

    def piece(at, core_at, kind):
        flip, rows = kinds[kind]
        return gathered.at[at * CORES + core_at, across if flip else column, rows]

    def gz_copy(at, kind, to, lane):
        ref = piece(at, core, kind)
        return remote(ref, ref, gz_send.at[at, kind, lane], gz_recv.at[at, kind], on_chip(to))

    def gz_wait(at, kind):
        ref = piece(at, core, kind)
        remote(
            ref, ref, gz_send.at[at, kind, 0], gz_recv.at[at, kind], on_chip(at)
        ).wait_recv()

    def gx_copy(at, kind):
        ref = piece(at, core, kind)
        return remote(ref, ref, gx_send.at[at, kind], gx_recv.at[at, kind], beside)

    def gx_wait(at, kind):
        ref = piece(at, core, 3 - kind)
        remote(ref, ref, gx_send.at[at, kind], gx_recv.at[at, kind], beside).wait_recv()

    def gc_copy(at, kind):
        ref = piece(at, core, kind)
        return remote(ref, ref, gc_send.at[at, kind], gc_recv.at[at, kind], partner)

    def gc_wait(at, kind):
        ref = piece(at, 1 - core, kind)
        remote(ref, ref, gc_send.at[at, kind], gc_recv.at[at, kind], partner).wait_recv()

    def both_ways(kind):
        launch(gz_copy(chip, kind, chip - 1, 0), chip > 0)
        launch(gz_copy(chip, kind, chip + 1, 1), chip < chips - 1)

    def begin():
        if early:
            launch(gx_copy(chip, 1))
        if late:
            both_ways(0)
            launch(gx_copy(chip, 0))
        if early:
            both_ways(1)
        for kind in use:
            if kind < 2:
                launch(gc_copy(chip, kind))
        if early:
            gx_wait(chip, 1)
            both_ways(2)
            launch(gc_copy(chip, 2))

    def forward(at, kinds, now=None):
        step = jnp.where(at < chip, 1, -1)
        more = jnp.where(at < chip, chip < chips - 1, chip > 0)
        for kind in kinds:
            if kind not in use:
                continue
            if now is None:
                gz_wait(at, kind)
            else:
                pl.when(now)(functools.partial(gz_wait, at, kind))
            launch(gz_copy(at, kind, chip + step, 0), more if now is None else now & more)
            if kind == 0:
                launch(gx_copy(at, 0), now)
            launch(gc_copy(at, kind), now)

    def crossed(at):
        if late:
            gx_wait(at, 0)
            launch(gc_copy(at, 3))

    def apply(load_from, count, store_to):
        active = expert_active(load_from(gathered).reshape(count, model_width), gate_ref[...], up_ref[...])
        product = jnp.dot(active, down_ref[...], preferred_element_type=jnp.float32)
        store_to((product * load_from(share_ref).reshape(count, 1)).astype(jnp.bfloat16))

    def pair(at):
        return pl.ds(at * CORES, CORES)

    def compute_early(at):
        if not early:
            return
        gc_wait(at, 1)
        gc_wait(at, 2)

        def store(value):
            partial[pair(at), :, first_rows] = value.reshape(CORES, 2, early, model_width)

        apply(lambda ref: ref[pair(at), :, first_rows], 2 * CORES * early, store)
        launch(core_sum_early(at))

    def compute_late(at, kind):
        if not late:
            return
        gc_wait(at, kind)
        side = across if kind else column

        def store(value):
            partial[pair(at), side, last_rows] = value.reshape(CORES, late, model_width)

        apply(lambda ref: ref[pair(at), side, last_rows], CORES * late, store)
        launch(core_sum_late(at, kind))

    def core_sum_early(at):
        return remote(
            partial.at[at * CORES + 1 - core, :, first_rows],
            from_core.at[at, :, first_rows],
            rc_send.at[at, 1],
            rc_recv.at[at, 1],
            partner,
        )

    def core_sum_late(at, kind):
        side = across if kind else column
        return remote(
            partial.at[at * CORES + 1 - core, side, last_rows],
            from_core.at[at, side, last_rows],
            rc_send.at[at, kind],
            rc_recv.at[at, kind],
            partner,
        )

    def x_sum(at):
        return remote(
            partial.at[at * CORES + core, across, last_rows],
            from_x.at[at],
            rx_send.at[at],
            rx_recv.at[at],
            beside,
        )

    inner = (chip > 0) & (chip < chips - 1)
    outer = (chip == 0) | (chip == chips - 1)

    def z_sum(j, part):
        at = order[j]
        step = jnp.where(at > chip, 1, -1)
        to = chip + step
        slot = at
        if chips > 2:
            ends = outer if j == chips - 1 else False
            if j == chips - 1:
                to = jnp.where(outer, at, to)
            inward = (at > 0) & (at < chips - 1) & (step < 0)
            slot = jnp.where((to == at) & (inward | ends), chips, at)
        mine = at * CORES + core
        if part:
            src, dst = partial.at[mine, column, last_rows], from_z.at[slot]
        else:
            src, dst = partial.at[mine, :, first_rows], from_z_early.at[slot]
        return remote(src, dst, rz_send.at[at, part], rz_recv.at[slot, part], on_chip(to))

    def z_landed(slot, part):
        ref = (from_z if part else from_z_early).at[slot]
        remote(
            ref, ref, rz_send.at[chip, part], rz_recv.at[slot, part], on_chip(chip)
        ).wait_recv()

    def pass_on(j, part):
        at = order[j]
        mine = at * CORES + core

        @pl.when(inner)
        def _():
            z_landed(at, part)
            if part:
                partial[mine, column, last_rows] = (
                    wide(partial[mine, column, last_rows]) + wide(from_z[at])
                ).astype(jnp.bfloat16)
            else:
                partial[mine, :, first_rows] = (
                    wide(partial[mine, :, first_rows]) + wide(from_z_early[at])
                ).astype(jnp.bfloat16)

        launch(z_sum(j, part), inner)

    def send_sum(j, part):
        if j:
            launch(z_sum(j, part), None if j == chips - 1 else outer)

    def wide(value):
        return value.astype(jnp.float32)

    def sum_early(j):
        at = order[j]
        if not early:
            return
        core_sum_early(at).wait_recv()
        mine = at * CORES + core
        partial[mine, :, first_rows] = (
            wide(partial[mine, :, first_rows]) + wide(from_core[at, :, first_rows])
        ).astype(jnp.bfloat16)
        send_sum(j, 0)

    def sum_late(j, kind):
        at = order[j]
        if not late:
            return
        core_sum_late(at, kind).wait_recv()
        mine = at * CORES + core
        side = across if kind else column
        partial[mine, side, last_rows] = (
            wide(partial[mine, side, last_rows]) + wide(from_core[at, side, last_rows])
        ).astype(jnp.bfloat16)
        if kind:
            launch(x_sum(at))

    def sum_across(j, now=None):
        at = order[j]
        if not late:
            return
        mine = at * CORES + core

        def add():
            x_sum(at).wait_recv()
            partial[mine, column, last_rows] = (
                wide(partial[mine, column, last_rows]) + wide(from_x[at])
            ).astype(jnp.bfloat16)

        if now is None:
            add()
        else:
            pl.when(now)(add)
        if now is None or now is outer:
            send_sum(j, 1)

    begin()
    for load in loads[3:]:
        load.wait()
    def work(j):
        at = order[j]
        compute_early(at)
        compute_late(at, 0)
        crossed(at)
        compute_late(at, 3)

    def gather_sums(j):
        sum_early(j)
        sum_late(j, 3)
        sum_late(j, 0)

    compute_early(chip)
    compute_late(chip, 0)
    forward(order[1], (0,))
    if chips > 2:
        forward(order[2], (0,), inner)
    crossed(chip)
    compute_late(chip, 3)
    forward(order[1], (1, 2))
    if chips > 2:
        forward(order[2], (1, 2), inner)
    gather_sums(0)
    work(1)
    if chips > 2:
        forward(order[2], (0,), outer)
        forward(order[3], (0,), inner)
        gather_sums(1)
        sum_across(0, outer)
        forward(order[2], (1, 2), outer)
        forward(order[3], (1, 2), inner)
        work(2)
        gather_sums(2)
        sum_across(0, inner)
        forward(order[3], (0,), outer)
        sum_across(1, outer)
        forward(order[3], (1, 2), outer)
        sum_across(2, outer)
        work(3)
        gather_sums(3)
        sum_across(1, inner)
        sum_across(2, inner)
    else:
        gather_sums(1)
        sum_across(0)
    if early:
        for j in range(chips - 2, 0, -1):
            pass_on(j, 0)
    sum_across(chips - 1)
    if late:
        for j in range(chips - 2, 0, -1):
            pass_on(j, 1)
    mine = chip * CORES + core
    ends = (chip, chips) if chips > 2 else (chip,)
    if early:
        total = wide(partial[mine, :, first_rows])
        for slot in ends:
            z_landed(slot, 0)
            total = total + wide(from_z_early[slot])
        partial[mine, :, first_rows] = total.astype(jnp.bfloat16)
        last = remote(
            partial.at[mine, across, first_rows],
            from_x_early,
            rx_send.at[chips],
            rx_recv.at[chips],
            beside,
        )
        launch(last)
    if late:
        total = wide(hidden[last_rows]) + wide(partial[mine, column, last_rows])
        for slot in ends:
            z_landed(slot, 1)
            total = total + wide(from_z[slot])
        out_ref[last_rows] = total.astype(jnp.bfloat16)
    if early:
        last.wait_recv()
        out_ref[first_rows] = (
            wide(hidden[first_rows]) + wide(partial[mine, column, first_rows]) + wide(from_x_early[...])
        ).astype(jnp.bfloat16)
    for copy, when in sends:
        if when is None:
            copy.wait_send()
        else:
            pl.when(when)(copy.wait_send)


def run_experts(attended, residual, gain, shares, out_w, gate_w, up_w, down_w):
    chips = lax.axis_size("sp") // CORES
    rows_dev, model_width = residual.shape
    pairs = chips * CORES
    early = EARLY_ROWS if rows_dev > EARLY_ROWS else 0
    late = rows_dev - early
    dma = pltpu.SemaphoreType.DMA
    block = (rows_dev, model_width)
    heads = (2, rows_dev, attended.shape[1])
    whole = pl.BlockSpec(memory_space=pltpu.VMEM)

    def vmem(*shape):
        return pltpu.VMEM(shape, jnp.bfloat16)

    return pl.pallas_call(
        functools.partial(experts_kernel, chips, early),
        out_shape=jax.ShapeDtypeStruct(block, jnp.bfloat16),
        in_specs=[whole] * 2 + [pl.BlockSpec(memory_space=pltpu.HBM)] * 6,
        out_specs=whole,
        scratch_shapes=[
            vmem(*heads),
            vmem(*block),
            vmem(pairs, 2, *block),
            vmem(pairs, 2, *block),
            vmem(chips, 2, *block),
            vmem(chips, late, model_width),
            vmem(max(early, 16), model_width),
            vmem(chips + 1, late, model_width),
            vmem(chips + 1, 2, max(early, 16), model_width),
            vmem(*block),
            vmem(*gain.shape),
            vmem(*out_w.shape),
            vmem(*gate_w.shape),
            vmem(*up_w.shape),
            vmem(*down_w.shape),
            dma((6,)),
            dma,
            dma,
            dma((chips, 3, 2)),
            dma((chips, 3)),
            dma((chips, 2)),
            dma((chips, 2)),
            dma((chips, 4)),
            dma((chips, 4)),
            dma((chips, 4)),
            dma((chips, 4)),
            dma((chips + 1,)),
            dma((chips + 1,)),
            dma((chips, 2)),
            dma((chips + 1, 2)),
        ],
        compiler_params=pltpu.CompilerParams(
            collective_id=0, has_side_effects=True, vmem_limit_bytes=VMEM_BYTES
        ),
    )(
        attended.reshape(heads),
        shares.reshape(pairs, 2, rows_dev, 1),
        residual,
        gain,
        out_w,
        gate_w,
        up_w,
        down_w,
    )


def experts_fit(tokens, rows_dev, model_width):
    group, places = lax.axis_size("tp"), lax.axis_size("sp")
    chips = places // CORES
    if group != 2 or places % CORES or chips not in (2, 4) or rows_dev % 16:
        return False
    if tokens != group * rows_dev or QK_ROPE + 2 * places > 128:
        return False
    return 3 * places * group * rows_dev * model_width * 2 < VMEM_BYTES // 2


def on_device(
    query_plain,
    query_turn,
    latent,
    key_turn,
    latent_norm_scale,
    plain_key_matrix,
    value_matrix,
    residual,
    out_weight,
    ffn_gain,
    gate_weight,
    up_weight,
    down_weight,
    routes,
    route_weights,
):
    if experts_fit(latent.shape[0], *residual.shape):
        attended, own_share = run_attention(
            query_plain,
            query_turn,
            latent,
            key_turn,
            latent_norm_scale,
            routes,
            route_weights,
            plain_key_matrix,
            value_matrix,
        )
        return run_experts(
            attended,
            residual,
            ffn_gain,
            own_share,
            out_weight,
            gate_weight[0],
            up_weight[0],
            down_weight[0],
        )
    tok_dev = latent.shape[0]
    heads_dev = query_plain.shape[1] // PLAIN_HEAD_WIDTH
    model_width = residual.shape[1]
    place = lax.axis_index("sp") * tok_dev + jnp.arange(tok_dev, dtype=jnp.int32)
    grid_row = place // GRID_W
    grid_col = place % GRID_W
    rows_dev, model_width = residual.shape
    group = lax.axis_size("tp")
    count = lax.axis_size("sp")
    expert_ids = jnp.arange(count, dtype=jnp.int32)
    share = jnp.sum(
        route_weights[..., None] * (routes[..., None] == expert_ids).astype(jnp.float32), axis=1
    )
    latent_width = latent.shape[1]
    wide = latent_width + QK_ROPE

    def key_side(latents, turns, at_row, at_col):
        normed_latent = norm_scale(latents, latent_norm_scale).astype(jnp.bfloat16)
        key_rot = turn(turns.astype(jnp.float32), at_row, at_col).astype(jnp.bfloat16)
        return [normed_latent, key_rot]

    sent = jnp.concatenate(key_side(latent, key_turn, grid_row, grid_col), axis=1)
    everyone = lax.all_gather(sent, "sp", axis=0, tiled=True)
    shares = lax.all_gather(share, ("sp", "tp"), axis=0, tiled=True)
    own_share = jnp.sum(
        jnp.where(expert_ids[None, :] == lax.axis_index("sp"), shares, 0.0), axis=1, keepdims=True
    )
    all_latent = everyone[:, :latent_width]
    all_rot = everyone[:, latent_width:wide]
    keys = jnp.dot(all_latent, plain_key_matrix, preferred_element_type=jnp.float32).astype(
        jnp.bfloat16
    )
    values = jnp.dot(all_latent, value_matrix, preferred_element_type=jnp.float32).astype(
        jnp.bfloat16
    )
    query_rot = turn(
        query_turn.astype(jnp.float32).reshape(tok_dev, heads_dev, QK_ROPE), grid_row, grid_col
    ).astype(jnp.bfloat16)
    scale = (PLAIN_HEAD_WIDTH + QK_ROPE) ** (-0.5)
    attended = []
    for head in range(heads_dev):
        span = slice(head * PLAIN_HEAD_WIDTH, (head + 1) * PLAIN_HEAD_WIDTH)
        scores = (
            jnp.einsum(
                "qd,kd->qk", query_plain[:, span], keys[:, span], preferred_element_type=jnp.float32
            )
            + jnp.einsum(
                "qd,kd->qk", query_rot[:, head], all_rot, preferred_element_type=jnp.float32
            )
        ) * scale
        weights = jnp.exp(scores - jnp.max(scores, axis=1, keepdims=True))
        summed = jnp.dot(
            weights.astype(jnp.bfloat16),
            values[:, head * VALUE_WIDTH : (head + 1) * VALUE_WIDTH],
            preferred_element_type=jnp.float32,
        )
        attended.append(
            (summed / jnp.sum(weights, axis=1, keepdims=True)).astype(jnp.bfloat16)
        )
    attended = jnp.concatenate(attended, axis=1)
    swapped = lax.all_to_all(
        attended.reshape(group, rows_dev, heads_dev * VALUE_WIDTH),
        "tp",
        split_axis=0,
        concat_axis=0,
        tiled=True,
    )
    own_rows = jnp.transpose(swapped, (1, 0, 2)).reshape(rows_dev, group * heads_dev * VALUE_WIDTH)
    projected = jnp.dot(own_rows, out_weight, preferred_element_type=jnp.float32)
    hidden = (residual.astype(jnp.float32) + projected).astype(jnp.bfloat16)
    normed = norm_scale(hidden, ffn_gain).astype(jnp.bfloat16)
    rows = lax.all_gather(normed, ("sp", "tp"), axis=0, tiled=True)
    active = expert_active(rows, gate_weight[0], up_weight[0])
    product = jnp.dot(active, down_weight[0], preferred_element_type=jnp.float32)
    mixture = lax.psum_scatter(
        (own_share * product).astype(jnp.bfloat16),
        ("sp", "tp"),
        scatter_dimension=0,
        tiled=True,
    )
    return (hidden.astype(jnp.float32) + mixture.astype(jnp.float32)).astype(jnp.bfloat16)


def solution(mesh):
    placed = (
        P(("grp", "sp"), "tp"),
        P(("grp", "sp"), "tp"),
        P(("grp", "sp"), None),
        P(("grp", "sp"), None),
        P(),
        P(None, "tp"),
        P(None, "tp"),
        P(("grp", "sp", "tp"), None),
        P(),
        P(),
        P("sp", None, "tp"),
        P("sp", None, "tp"),
        P("sp", "tp", None),
        P(("grp", "sp", "tp"), None),
        P(("grp", "sp", "tp"), None),
    )
    return jax.shard_map(
        on_device,
        mesh=mesh,
        in_specs=placed,
        out_specs=P(("grp", "sp", "tp"), None),
        check_vma=False,
    )
```

```python
import functools

import jax
import jax.numpy as jnp
import numpy as np
from jax import lax
from jax.experimental import pallas as pl
from jax.experimental.pallas import tpu as pltpu
from jax.sharding import PartitionSpec as P

PLAIN_HEAD_WIDTH = 128
QK_ROPE = 64
VALUE_WIDTH = 128
GRID_W = 64


theta = 10000.0
eps = 1e-06
limit = 7.0
slope = 1.702
CORES = 2
EARLY_ROWS = 32
VMEM_BYTES = 60 * 2**20


def turn(vector, row_shift, col_shift):
    width = vector.shape[-1]
    count = width // 4
    half = width // 2
    freqs = theta ** (-jnp.arange(count, dtype=jnp.float32) / count)
    extra = (1,) * (vector.ndim - 2)
    pieces = []
    for portion, shift in ((vector[..., :half], row_shift), (vector[..., half:], col_shift)):
        angle = (shift.astype(jnp.float32)[:, None] * freqs[None, :]).reshape(
            (shift.shape[0],) + extra + (count,)
        )
        lower = portion[..., :count]
        upper = portion[..., count:]
        pieces.append(
            jnp.concatenate(
                [
                    lower * jnp.cos(angle) - upper * jnp.sin(angle),
                    lower * jnp.sin(angle) + upper * jnp.cos(angle),
                ],
                axis=-1,
            )
        )
    return jnp.concatenate(pieces, axis=-1)


def norm_scale(values, gain):
    wide = values.astype(jnp.float32)
    return (
        wide
        * lax.rsqrt(jnp.mean(wide * wide, axis=-1, keepdims=True) + eps)
        * gain.astype(jnp.float32)
    )


def expert_active(rows, gate_w, up_w):
    gate_pre = jnp.minimum(jnp.dot(rows, gate_w, preferred_element_type=jnp.float32), limit)
    up_pre = jnp.clip(jnp.dot(rows, up_w, preferred_element_type=jnp.float32), -limit, limit)
    return ((up_pre + 1.0) * gate_pre * jax.nn.sigmoid(slope * gate_pre)).astype(jnp.bfloat16)


def flipped(index, mask):
    out = index
    bit = 1
    while bit <= mask:
        if mask & bit:
            out = out + bit - 2 * bit * ((index // bit) % 2)
        bit *= 2
    return out


def gatherer(chips, group, own, gathered, sems, launch):
    z_send, z_recv, x_send, x_recv, c_send, c_recv = sems
    place = lax.axis_index("sp")
    column = lax.axis_index("tp")
    chip, core = place // CORES, place % CORES
    per_chip = CORES * group
    partner = {"sp": chip * CORES + 1 - core}

    def other(shift):
        return (column + shift) % group

    def slot(k, core_at, column_at):
        return flipped(chip, k) * per_chip + core_at * group + column_at

    def chip_peer(k):
        return {"sp": flipped(chip, k) * CORES + core}

    def remote(src, dst, send_sem, recv_sem, device):
        return pltpu.make_async_remote_copy(
            src_ref=src, dst_ref=dst, send_sem=send_sem, recv_sem=recv_sem, device_id=device
        )

    def greet():
        barrier = pltpu.get_barrier_semaphore()
        pl.semaphore_signal(barrier, inc=1, device_id=partner)
        for k in range(1, chips):
            pl.semaphore_signal(barrier, inc=1, device_id=chip_peer(k))
        for shift in range(1, group):
            pl.semaphore_signal(barrier, inc=1, device_id={"tp": other(shift)})

    def met():
        pl.semaphore_wait(pltpu.get_barrier_semaphore(), chips + group - 1)

    def source(k, back):
        if k == 0 and back == 0:
            return own
        return gathered.at[slot(k, core, other(group - back))]

    def chip_wait(k):
        landed = gathered.at[slot(k, core, column)]
        remote(landed, landed, z_send.at[k], z_recv.at[k], chip_peer(k)).wait_recv()

    def core_copy(k, back):
        return remote(
            source(k, back),
            gathered.at[slot(k, core, other(group - back))],
            c_send.at[k, back],
            c_recv.at[k, back],
            partner,
        )

    def core_wait(k, back):
        landed = gathered.at[slot(k, 1 - core, other(group - back))]
        remote(landed, landed, c_send.at[k, back], c_recv.at[k, back], partner).wait_recv()

    def tp_copy(k, shift):
        return remote(
            source(k, 0),
            gathered.at[slot(k, core, column)],
            x_send.at[k, shift],
            x_recv.at[k, shift],
            {"tp": other(shift)},
        )

    def tp_wait(k, shift):
        landed = gathered.at[slot(k, core, other(group - shift))]
        remote(
            landed, landed, x_send.at[k, shift], x_recv.at[k, shift], {"tp": other(shift)}
        ).wait_recv()

    def spread(k):
        for shift in range(1, group):
            launch(tp_copy(k, shift))
        launch(core_copy(k, 0))

    def begin():
        for k in range(1, chips):
            launch(
                remote(
                    own,
                    gathered.at[slot(0, core, column)],
                    z_send.at[k],
                    z_recv.at[k],
                    chip_peer(k),
                )
            )
        spread(0)

    def step(k):
        if k + 1 < chips:
            chip_wait(k + 1)
            spread(k + 1)
        for shift in range(1, group):
            tp_wait(k, shift)
            launch(core_copy(k, shift))
        for back in range(group):
            core_wait(k, back)

    return greet, met, begin, step, slot, chip_peer, partner, other, remote


def turn_matrices(shape, width):
    row = lax.broadcasted_iota(jnp.int32, shape, 0)
    col = lax.broadcasted_iota(jnp.int32, shape, 1)
    count = width // 4
    lane = col % 128
    source = (col // 128) * width + lane
    inside = lane < width
    lower = lane % (2 * count) < count
    straight = jnp.where(inside & (row == source), 1.0, 0.0)
    moved = jnp.where(lower, source + count, source - count)
    sign = jnp.where(lower, -1.0, 1.0)
    crossed = jnp.where(inside & (row == moved), sign, 0.0)
    return straight.astype(jnp.bfloat16), crossed.astype(jnp.bfloat16)


def attention_stage(chips, group, inputs, out_ref, share_ref, refs, prefetch):
    own, gathered, queries, cosines, sines, key_turns = refs[:6]
    held, load_sem, sems = refs[6:16], refs[16], refs[17:]
    (
        latent_ref,
        gain_ref,
        freqs_ref,
        key_turn_ref,
        routes_ref,
        route_weights_ref,
        query_turn_ref,
        query_ref,
        keyw_ref,
        valuew_ref,
    ) = held
    place = lax.axis_index("sp")
    column = lax.axis_index("tp")
    tokens, latent_width = inputs[0].shape
    rows_dev = own.shape[0]
    heads_dev = inputs[7].shape[1] // PLAIN_HEAD_WIDTH
    count = lax.axis_size("sp")
    per_chip = CORES * group
    sends = []

    def launch(copy):
        copy.start()
        sends.append(copy)

    greet, met, begin, step, slot = gatherer(chips, group, own, gathered, sems, launch)[:5]
    greet()
    loads = [
        pltpu.make_async_copy(src, dst, load_sem.at[i])
        for i, (src, dst) in enumerate(zip(inputs, held))
    ]
    for load in loads:
        load.start()
    loads[2].wait()

    at = place * tokens + lax.broadcasted_iota(jnp.int32, (tokens, 128), 0)
    lane = lax.broadcasted_iota(jnp.int32, (tokens, 128), 1)
    shift = jnp.where(lane < QK_ROPE // 2, at // GRID_W, at % GRID_W).astype(jnp.float32)
    angle = shift * freqs_ref[...]
    cosines[...] = jnp.cos(angle)
    sines[...] = jnp.sin(angle)

    def turned(vector, matrices, cos, sin):
        straight, crossed = (
            jnp.dot(vector, matrix, preferred_element_type=jnp.float32) for matrix in matrices
        )
        return straight * cos + crossed * sin

    mine = pl.ds(pl.multiple_of(column * rows_dev, 16), rows_dev)
    for load in loads[:2] + loads[3:6]:
        load.wait()
    key_turns[...] = key_turn_ref[...].T
    named = routes_ref[...].T
    weighing = route_weights_ref[...].T
    key_rot = turned(
        key_turns[mine, :],
        turn_matrices((QK_ROPE, 128), QK_ROPE),
        cosines[mine, :],
        sines[mine, :],
    )
    lane = lax.broadcasted_iota(jnp.int32, (rows_dev, 128), 1) - QK_ROPE
    expert = jnp.where(lane < count, lane, lane - count)
    share = jnp.zeros((rows_dev, 128), jnp.float32)
    for k in range(named.shape[1]):
        share = share + jnp.where(named[:, k : k + 1] == expert, weighing[:, k : k + 1], 0.0)
    high = share.astype(jnp.bfloat16).astype(jnp.float32)
    packed = jnp.where(lane < count, high, share - high)
    packed = jnp.where(lane < 2 * count, packed, 0.0)
    own[:, :latent_width] = norm_scale(latent_ref[mine, :], gain_ref[...].reshape(1, latent_width)).astype(jnp.bfloat16)
    own[:, latent_width:] = jnp.where(lane < 0, key_rot, packed).astype(jnp.bfloat16)
    met()
    begin()
    gathered[slot(0, place % CORES, column)] = own[...]

    for load in loads[6:]:
        load.wait()
    prefetch()
    matrices = turn_matrices((heads_dev * QK_ROPE, heads_dev * 128), QK_ROPE)
    straight, crossed = (
        jnp.dot(query_turn_ref[...], matrix, preferred_element_type=jnp.float32)
        for matrix in matrices
    )
    for head in range(heads_dev):
        span = slice(head * 128, (head + 1) * 128)
        queries[head, :, :128] = query_ref[:, span]
        queries[head, :, 128:] = (
            straight[:, span] * cosines[...] + crossed[:, span] * sines[...]
        ).astype(jnp.bfloat16)

    scale = (PLAIN_HEAD_WIDTH + QK_ROPE) ** (-0.5)
    peaks = [None] * heads_dev
    sums = [None] * heads_dev
    totals = [None] * heads_dev
    for k in range(chips):
        step(k)
        first = slot(k, 0, 0)
        width = per_chip * rows_dev
        latents = gathered[pl.ds(first, per_chip), :, :latent_width].reshape(width, latent_width)
        rot = gathered[pl.ds(first, per_chip), :, latent_width:].reshape(width, 128)
        keys = jnp.dot(latents, keyw_ref[...], preferred_element_type=jnp.float32).astype(
            jnp.bfloat16
        )
        values = jnp.dot(latents, valuew_ref[...], preferred_element_type=jnp.float32).astype(
            jnp.bfloat16
        )
        for head in range(heads_dev):
            span = slice(head * 128, (head + 1) * 128)
            scores = scale * lax.dot_general(
                queries[head],
                jnp.concatenate([keys[:, span], rot], axis=1),
                (((1,), (1,)), ((), ())),
                preferred_element_type=jnp.float32,
            )
            peak = jnp.max(scores, axis=1, keepdims=True)
            if k:
                peak = jnp.maximum(peak, peaks[head])
            weights = jnp.exp(scores - peak)
            total = jnp.sum(weights, axis=1, keepdims=True)
            summed = jnp.dot(
                weights.astype(jnp.bfloat16), values[:, span], preferred_element_type=jnp.float32
            )
            if k:
                fade = jnp.exp(peaks[head] - peak)
                total = total + fade * sums[head]
                summed = summed + fade * totals[head]
            peaks[head], sums[head], totals[head] = peak, total, summed
        lane = lax.broadcasted_iota(jnp.int32, (width, 128), 1) - QK_ROPE
        named = (lane == place) | (lane == place + count)
        share_ref[pl.ds(first // group, CORES)] = jnp.sum(
            jnp.where(named, rot.astype(jnp.float32), 0.0), axis=1, keepdims=True
        ).reshape(CORES, group, rows_dev, 1)
    for head in range(heads_dev):
        value = (totals[head] / sums[head]).astype(jnp.bfloat16)
        out_ref[:, :, head * 128 : (head + 1) * 128] = value.reshape(group, rows_dev, 128)
    for copy in sends:
        copy.wait_send()


def gather_sems(chips, group):
    dma = pltpu.SemaphoreType.DMA
    return [dma((chips,))] * 2 + [dma((chips, group))] * 4


def neighbour_order(chips):
    table = []
    for z in range(chips):
        table.append(sorted(range(chips), key=lambda o: (abs(o - z), o if z < chips // 2 else -o)))
    return table


def pick(z, values):
    out = values[0]
    for at in range(1, len(values)):
        out = jnp.where(z == at, values[at], out)
    return out


def experts_stage(chips, early, attended_ref, share_ref, out_ref, loads, refs):
    (
        heads,
        hidden,
        gathered,
        partial,
        from_core,
        from_x,
        from_x_early,
        from_z,
        from_z_early,
        residual_ref,
        gain_ref,
        outw_ref,
        gate_ref,
        up_ref,
        down_ref,
        h_send,
        h_recv,
        gz_send,
        gz_recv,
        gx_send,
        gx_recv,
        gc_send,
        gc_recv,
        rc_send,
        rc_recv,
        rx_send,
        rx_recv,
        rz_send,
        rz_recv,
    ) = refs
    place = lax.axis_index("sp")
    column = lax.axis_index("tp")
    chip, core = place // CORES, place % CORES
    across = 1 - column
    rows_dev, model_width = hidden.shape
    late = rows_dev - early
    table = neighbour_order(chips)
    order = [chip] + [pick(chip, [table[z][j] for z in range(chips)]) for j in range(1, chips)]
    sends = []
    first_rows = pl.ds(0, early)
    last_rows = pl.ds(early, late)

    def launch(copy, when=None):
        if when is None:
            copy.start()
        else:
            pl.when(when)(copy.start)
        sends.append((copy, when))

    def remote(src, dst, send_sem, recv_sem, device):
        return pltpu.make_async_remote_copy(
            src_ref=src, dst_ref=dst, send_sem=send_sem, recv_sem=recv_sem, device_id=device
        )

    def on_chip(at):
        return {"sp": at * CORES + core}

    partner = {"sp": chip * CORES + 1 - core}
    beside = {"tp": across}

    swap = remote(attended_ref.at[across], heads.at[column], h_send, h_recv, beside)
    launch(swap)
    heads[column] = attended_ref[column]
    for load in loads[:3]:
        load.wait()
    landed = heads.at[across]
    remote(landed, landed, h_send, h_recv, beside).wait_recv()
    joined = jnp.concatenate([heads[0], heads[1]], axis=1)
    projected = jnp.dot(joined, outw_ref[...], preferred_element_type=jnp.float32)
    mixed = (residual_ref[...].astype(jnp.float32) + projected).astype(jnp.bfloat16)
    gathered[place, column] = norm_scale(mixed, gain_ref[...].reshape(1, model_width)).astype(jnp.bfloat16)
    hidden[...] = mixed

    kinds = ((0, last_rows), (0, first_rows), (1, first_rows), (1, last_rows))
    use = [k for k in range(4) if (late if k in (0, 3) else early)]

    def piece(at, core_at, kind):
        flip, rows = kinds[kind]
        return gathered.at[at * CORES + core_at, across if flip else column, rows]

    def gz_copy(at, kind, to, lane):
        ref = piece(at, core, kind)
        return remote(ref, ref, gz_send.at[at, kind, lane], gz_recv.at[at, kind], on_chip(to))

    def gz_wait(at, kind):
        ref = piece(at, core, kind)
        remote(
            ref, ref, gz_send.at[at, kind, 0], gz_recv.at[at, kind], on_chip(at)
        ).wait_recv()

    def gx_copy(at, kind):
        ref = piece(at, core, kind)
        return remote(ref, ref, gx_send.at[at, kind], gx_recv.at[at, kind], beside)

    def gx_wait(at, kind):
        ref = piece(at, core, 3 - kind)
        remote(ref, ref, gx_send.at[at, kind], gx_recv.at[at, kind], beside).wait_recv()

    def gc_copy(at, kind):
        ref = piece(at, core, kind)
        return remote(ref, ref, gc_send.at[at, kind], gc_recv.at[at, kind], partner)

    def gc_wait(at, kind):
        ref = piece(at, 1 - core, kind)
        remote(ref, ref, gc_send.at[at, kind], gc_recv.at[at, kind], partner).wait_recv()

    def both_ways(kind):
        launch(gz_copy(chip, kind, chip - 1, 0), chip > 0)
        launch(gz_copy(chip, kind, chip + 1, 1), chip < chips - 1)

    def begin():
        if early:
            launch(gx_copy(chip, 1))
        if late:
            both_ways(0)
            launch(gx_copy(chip, 0))
        if early:
            both_ways(1)
        for kind in use:
            if kind < 2:
                launch(gc_copy(chip, kind))
        if early:
            gx_wait(chip, 1)
            both_ways(2)
            launch(gc_copy(chip, 2))

    def forward(at, kinds, now=None):
        step = jnp.where(at < chip, 1, -1)
        more = jnp.where(at < chip, chip < chips - 1, chip > 0)
        for kind in kinds:
            if kind not in use:
                continue
            if now is None:
                gz_wait(at, kind)
            else:
                pl.when(now)(functools.partial(gz_wait, at, kind))
            launch(gz_copy(at, kind, chip + step, 0), more if now is None else now & more)
            if kind == 0:
                launch(gx_copy(at, 0), now)
            launch(gc_copy(at, kind), now)

    def crossed(at):
        if late:
            gx_wait(at, 0)
            launch(gc_copy(at, 3))

    def apply(load_from, count, store_to):
        active = expert_active(load_from(gathered).reshape(count, model_width), gate_ref[...], up_ref[...])
        product = jnp.dot(active, down_ref[...], preferred_element_type=jnp.float32)
        store_to((product * load_from(share_ref).reshape(count, 1)).astype(jnp.bfloat16))

    def pair(at):
        return pl.ds(at * CORES, CORES)

    def compute_early(at):
        if not early:
            return
        gc_wait(at, 1)
        gc_wait(at, 2)

        def store(value):
            partial[pair(at), :, first_rows] = value.reshape(CORES, 2, early, model_width)

        apply(lambda ref: ref[pair(at), :, first_rows], 2 * CORES * early, store)
        launch(core_sum_early(at))

    def compute_late(at, kind):
        if not late:
            return
        gc_wait(at, kind)
        side = across if kind else column

        def store(value):
            partial[pair(at), side, last_rows] = value.reshape(CORES, late, model_width)

        apply(lambda ref: ref[pair(at), side, last_rows], CORES * late, store)
        launch(core_sum_late(at, kind))

    def core_sum_early(at):
        return remote(
            partial.at[at * CORES + 1 - core, :, first_rows],
            from_core.at[at, :, first_rows],
            rc_send.at[at, 1],
            rc_recv.at[at, 1],
            partner,
        )

    def core_sum_late(at, kind):
        side = across if kind else column
        return remote(
            partial.at[at * CORES + 1 - core, side, last_rows],
            from_core.at[at, side, last_rows],
            rc_send.at[at, kind],
            rc_recv.at[at, kind],
            partner,
        )

    def x_sum(at):
        return remote(
            partial.at[at * CORES + core, across, last_rows],
            from_x.at[at],
            rx_send.at[at],
            rx_recv.at[at],
            beside,
        )

    inner = (chip > 0) & (chip < chips - 1)
    outer = (chip == 0) | (chip == chips - 1)

    def z_sum(j, part):
        at = order[j]
        step = jnp.where(at > chip, 1, -1)
        to = chip + step
        slot = at
        if chips > 2:
            ends = outer if j == chips - 1 else False
            if j == chips - 1:
                to = jnp.where(outer, at, to)
            inward = (at > 0) & (at < chips - 1) & (step < 0)
            slot = jnp.where((to == at) & (inward | ends), chips, at)
        mine = at * CORES + core
        if part:
            src, dst = partial.at[mine, column, last_rows], from_z.at[slot]
        else:
            src, dst = partial.at[mine, :, first_rows], from_z_early.at[slot]
        return remote(src, dst, rz_send.at[at, part], rz_recv.at[slot, part], on_chip(to))

    def z_landed(slot, part):
        ref = (from_z if part else from_z_early).at[slot]
        remote(
            ref, ref, rz_send.at[chip, part], rz_recv.at[slot, part], on_chip(chip)
        ).wait_recv()

    def pass_on(j, part):
        at = order[j]
        mine = at * CORES + core

        @pl.when(inner)
        def _():
            z_landed(at, part)
            if part:
                partial[mine, column, last_rows] = (
                    wide(partial[mine, column, last_rows]) + wide(from_z[at])
                ).astype(jnp.bfloat16)
            else:
                partial[mine, :, first_rows] = (
                    wide(partial[mine, :, first_rows]) + wide(from_z_early[at])
                ).astype(jnp.bfloat16)

        launch(z_sum(j, part), inner)

    def send_sum(j, part):
        if j:
            launch(z_sum(j, part), None if j == chips - 1 else outer)

    def wide(value):
        return value.astype(jnp.float32)

    def sum_early(j):
        at = order[j]
        if not early:
            return
        core_sum_early(at).wait_recv()
        mine = at * CORES + core
        partial[mine, :, first_rows] = (
            wide(partial[mine, :, first_rows]) + wide(from_core[at, :, first_rows])
        ).astype(jnp.bfloat16)
        send_sum(j, 0)

    def sum_late(j, kind):
        at = order[j]
        if not late:
            return
        core_sum_late(at, kind).wait_recv()
        mine = at * CORES + core
        side = across if kind else column
        partial[mine, side, last_rows] = (
            wide(partial[mine, side, last_rows]) + wide(from_core[at, side, last_rows])
        ).astype(jnp.bfloat16)
        if kind:
            launch(x_sum(at))

    def sum_across(j, now=None):
        at = order[j]
        if not late:
            return
        mine = at * CORES + core

        def add():
            x_sum(at).wait_recv()
            partial[mine, column, last_rows] = (
                wide(partial[mine, column, last_rows]) + wide(from_x[at])
            ).astype(jnp.bfloat16)

        if now is None:
            add()
        else:
            pl.when(now)(add)
        if now is None or now is outer:
            send_sum(j, 1)

    begin()
    for load in loads[3:]:
        load.wait()
    def work(j):
        at = order[j]
        compute_early(at)
        compute_late(at, 0)
        crossed(at)
        compute_late(at, 3)

    def gather_sums(j):
        sum_early(j)
        sum_late(j, 3)
        sum_late(j, 0)

    compute_early(chip)
    compute_late(chip, 0)
    forward(order[1], (0,))
    if chips > 2:
        forward(order[2], (0,), inner)
    crossed(chip)
    compute_late(chip, 3)
    forward(order[1], (1, 2))
    if chips > 2:
        forward(order[2], (1, 2), inner)
    gather_sums(0)
    work(1)
    if chips > 2:
        forward(order[2], (0,), outer)
        forward(order[3], (0,), inner)
        gather_sums(1)
        sum_across(0, outer)
        forward(order[2], (1, 2), outer)
        forward(order[3], (1, 2), inner)
        work(2)
        gather_sums(2)
        sum_across(0, inner)
        forward(order[3], (0,), outer)
        sum_across(1, outer)
        forward(order[3], (1, 2), outer)
        sum_across(2, outer)
        work(3)
        gather_sums(3)
        sum_across(1, inner)
        sum_across(2, inner)
    else:
        gather_sums(1)
        sum_across(0)
    if early:
        for j in range(chips - 2, 0, -1):
            pass_on(j, 0)
    sum_across(chips - 1)
    if late:
        for j in range(chips - 2, 0, -1):
            pass_on(j, 1)
    mine = chip * CORES + core
    ends = (chip, chips) if chips > 2 else (chip,)
    if early:
        total = wide(partial[mine, :, first_rows])
        for slot in ends:
            z_landed(slot, 0)
            total = total + wide(from_z_early[slot])
        partial[mine, :, first_rows] = total.astype(jnp.bfloat16)
        last = remote(
            partial.at[mine, across, first_rows],
            from_x_early,
            rx_send.at[chips],
            rx_recv.at[chips],
            beside,
        )
        launch(last)
    if late:
        total = wide(hidden[last_rows]) + wide(partial[mine, column, last_rows])
        for slot in ends:
            z_landed(slot, 1)
            total = total + wide(from_z[slot])
        out_ref[last_rows] = total.astype(jnp.bfloat16)
    if early:
        last.wait_recv()
        out_ref[first_rows] = (
            wide(hidden[first_rows]) + wide(partial[mine, column, first_rows]) + wide(from_x_early[...])
        ).astype(jnp.bfloat16)
    for copy, when in sends:
        if when is None:
            copy.wait_send()
        else:
            pl.when(when)(copy.wait_send)


def whole_kernel(chips, group, early, *refs):
    inputs, refs = refs[:16], refs[16:]
    out_ref, attended_ref, share_ref, load_sem = refs[:4]
    first, second = refs[4:27], refs[27:]
    loads = [
        pltpu.make_async_copy(src, dst, load_sem.at[i])
        for i, (src, dst) in enumerate(zip(inputs[10:], second[9:15]))
    ]

    def prefetch():
        for load in loads:
            load.start()

    attention_stage(chips, group, inputs[:10], attended_ref, share_ref, first, prefetch)
    experts_stage(chips, early, attended_ref, share_ref, out_ref, loads, second)


def run_whole(
    query,
    query_turn,
    latent,
    key_turn,
    latent_gain,
    key_w,
    value_w,
    residual,
    out_w,
    gain,
    gate_w,
    up_w,
    down_w,
    routes,
    route_weights,
):
    group = lax.axis_size("tp")
    chips = lax.axis_size("sp") // CORES
    pairs = chips * CORES
    tokens, latent_width = latent.shape
    rows_dev, model_width = residual.shape
    heads_dev = query.shape[1] // PLAIN_HEAD_WIDTH
    early = EARLY_ROWS if rows_dev > EARLY_ROWS else 0
    late = rows_dev - early
    quarter = QK_ROPE // 4
    freqs = theta ** (-np.arange(quarter, dtype=np.float32) / np.float32(quarter))
    freqs = np.tile(freqs.astype(np.float32), 128 // quarter).reshape(1, 128)
    dma = pltpu.SemaphoreType.DMA
    block = (rows_dev, model_width)
    heads = (group, rows_dev, heads_dev * VALUE_WIDTH)
    sent = latent_width + 128

    def vmem(*shape):
        return pltpu.VMEM(shape, jnp.bfloat16)

    first = (
        latent,
        latent_gain,
        jnp.asarray(freqs),
        key_turn.T,
        routes.T,
        route_weights.T,
        query_turn,
        query,
        key_w,
        value_w,
    )
    second = (residual, gain, out_w, gate_w, up_w, down_w)
    return pl.pallas_call(
        functools.partial(whole_kernel, chips, group, early),
        out_shape=jax.ShapeDtypeStruct(block, jnp.bfloat16),
        in_specs=[pl.BlockSpec(memory_space=pltpu.HBM)] * 16,
        out_specs=pl.BlockSpec(memory_space=pltpu.VMEM),
        scratch_shapes=[
            vmem(*heads),
            pltpu.VMEM((pairs, group, rows_dev, 1), jnp.float32),
            dma((6,)),
            vmem(rows_dev, sent),
            vmem(pairs * group, rows_dev, sent),
            vmem(heads_dev, tokens, 256),
            pltpu.VMEM((tokens, 128), jnp.float32),
            pltpu.VMEM((tokens, 128), jnp.float32),
            vmem(tokens, QK_ROPE),
        ]
        + [pltpu.VMEM(array.shape, array.dtype) for array in first]
        + [dma((len(first),))]
        + gather_sems(chips, group)
        + [
            vmem(*heads),
            vmem(*block),
            vmem(pairs, 2, *block),
            vmem(pairs, 2, *block),
            vmem(chips, 2, *block),
            vmem(chips, late, model_width),
            vmem(max(early, 16), model_width),
            vmem(chips + 1, late, model_width),
            vmem(chips + 1, 2, max(early, 16), model_width),
        ]
        + [pltpu.VMEM(array.shape, array.dtype) for array in second]
        + [
            dma,
            dma,
            dma((chips, 3, 2)),
            dma((chips, 3)),
            dma((chips, 2)),
            dma((chips, 2)),
            dma((chips, 4)),
            dma((chips, 4)),
            dma((chips, 4)),
            dma((chips, 4)),
            dma((chips + 1,)),
            dma((chips + 1,)),
            dma((chips, 2)),
            dma((chips + 1, 2)),
        ],
        compiler_params=pltpu.CompilerParams(
            collective_id=0, has_side_effects=True, vmem_limit_bytes=VMEM_BYTES
        ),
    )(*first, *second)


def experts_fit(tokens, rows_dev, model_width):
    group, places = lax.axis_size("tp"), lax.axis_size("sp")
    chips = places // CORES
    if group != 2 or places % CORES or chips not in (2, 4) or rows_dev % 16:
        return False
    if tokens != group * rows_dev or QK_ROPE + 2 * places > 128:
        return False
    return 3 * places * group * rows_dev * model_width * 2 < VMEM_BYTES // 2


def on_device(
    query_plain,
    query_turn,
    latent,
    key_turn,
    latent_norm_scale,
    plain_key_matrix,
    value_matrix,
    residual,
    out_weight,
    ffn_gain,
    gate_weight,
    up_weight,
    down_weight,
    routes,
    route_weights,
):
    if experts_fit(latent.shape[0], *residual.shape):
        return run_whole(
            query_plain,
            query_turn,
            latent,
            key_turn,
            latent_norm_scale,
            plain_key_matrix,
            value_matrix,
            residual,
            out_weight,
            ffn_gain,
            gate_weight[0],
            up_weight[0],
            down_weight[0],
            routes,
            route_weights,
        )
    tok_dev = latent.shape[0]
    heads_dev = query_plain.shape[1] // PLAIN_HEAD_WIDTH
    model_width = residual.shape[1]
    place = lax.axis_index("sp") * tok_dev + jnp.arange(tok_dev, dtype=jnp.int32)
    grid_row = place // GRID_W
    grid_col = place % GRID_W
    rows_dev, model_width = residual.shape
    group = lax.axis_size("tp")
    count = lax.axis_size("sp")
    expert_ids = jnp.arange(count, dtype=jnp.int32)
    share = jnp.sum(
        route_weights[..., None] * (routes[..., None] == expert_ids).astype(jnp.float32), axis=1
    )
    latent_width = latent.shape[1]
    wide = latent_width + QK_ROPE

    def key_side(latents, turns, at_row, at_col):
        normed_latent = norm_scale(latents, latent_norm_scale).astype(jnp.bfloat16)
        key_rot = turn(turns.astype(jnp.float32), at_row, at_col).astype(jnp.bfloat16)
        return [normed_latent, key_rot]

    sent = jnp.concatenate(key_side(latent, key_turn, grid_row, grid_col), axis=1)
    everyone = lax.all_gather(sent, "sp", axis=0, tiled=True)
    shares = lax.all_gather(share, ("sp", "tp"), axis=0, tiled=True)
    own_share = jnp.sum(
        jnp.where(expert_ids[None, :] == lax.axis_index("sp"), shares, 0.0), axis=1, keepdims=True
    )
    all_latent = everyone[:, :latent_width]
    all_rot = everyone[:, latent_width:wide]
    keys = jnp.dot(all_latent, plain_key_matrix, preferred_element_type=jnp.float32).astype(
        jnp.bfloat16
    )
    values = jnp.dot(all_latent, value_matrix, preferred_element_type=jnp.float32).astype(
        jnp.bfloat16
    )
    query_rot = turn(
        query_turn.astype(jnp.float32).reshape(tok_dev, heads_dev, QK_ROPE), grid_row, grid_col
    ).astype(jnp.bfloat16)
    scale = (PLAIN_HEAD_WIDTH + QK_ROPE) ** (-0.5)
    attended = []
    for head in range(heads_dev):
        span = slice(head * PLAIN_HEAD_WIDTH, (head + 1) * PLAIN_HEAD_WIDTH)
        scores = (
            jnp.einsum(
                "qd,kd->qk", query_plain[:, span], keys[:, span], preferred_element_type=jnp.float32
            )
            + jnp.einsum(
                "qd,kd->qk", query_rot[:, head], all_rot, preferred_element_type=jnp.float32
            )
        ) * scale
        weights = jnp.exp(scores - jnp.max(scores, axis=1, keepdims=True))
        summed = jnp.dot(
            weights.astype(jnp.bfloat16),
            values[:, head * VALUE_WIDTH : (head + 1) * VALUE_WIDTH],
            preferred_element_type=jnp.float32,
        )
        attended.append(
            (summed / jnp.sum(weights, axis=1, keepdims=True)).astype(jnp.bfloat16)
        )
    attended = jnp.concatenate(attended, axis=1)
    swapped = lax.all_to_all(
        attended.reshape(group, rows_dev, heads_dev * VALUE_WIDTH),
        "tp",
        split_axis=0,
        concat_axis=0,
        tiled=True,
    )
    own_rows = jnp.transpose(swapped, (1, 0, 2)).reshape(rows_dev, group * heads_dev * VALUE_WIDTH)
    projected = jnp.dot(own_rows, out_weight, preferred_element_type=jnp.float32)
    hidden = (residual.astype(jnp.float32) + projected).astype(jnp.bfloat16)
    normed = norm_scale(hidden, ffn_gain).astype(jnp.bfloat16)
    rows = lax.all_gather(normed, ("sp", "tp"), axis=0, tiled=True)
    active = expert_active(rows, gate_weight[0], up_weight[0])
    product = jnp.dot(active, down_weight[0], preferred_element_type=jnp.float32)
    mixture = lax.psum_scatter(
        (own_share * product).astype(jnp.bfloat16),
        ("sp", "tp"),
        scatter_dimension=0,
        tiled=True,
    )
    return (hidden.astype(jnp.float32) + mixture.astype(jnp.float32)).astype(jnp.bfloat16)


def solution(mesh):
    placed = (
        P(("grp", "sp"), "tp"),
        P(("grp", "sp"), "tp"),
        P(("grp", "sp"), None),
        P(("grp", "sp"), None),
        P(),
        P(None, "tp"),
        P(None, "tp"),
        P(("grp", "sp", "tp"), None),
        P(),
        P(),
        P("sp", None, "tp"),
        P("sp", None, "tp"),
        P("sp", "tp", None),
        P(("grp", "sp", "tp"), None),
        P(("grp", "sp", "tp"), None),
    )
    return jax.shard_map(
        on_device,
        mesh=mesh,
        in_specs=placed,
        out_specs=P(("grp", "sp", "tp"), None),
        check_vma=False,
    )
```

```python
import functools

import jax
import jax.numpy as jnp
import numpy as np
from jax import lax
from jax.experimental import pallas as pl
from jax.experimental.pallas import tpu as pltpu
from jax.sharding import PartitionSpec as P

PLAIN_HEAD_WIDTH = 128
QK_ROPE = 64
VALUE_WIDTH = 128
GRID_W = 64


theta = 10000.0
eps = 1e-06
limit = 7.0
slope = 1.702
CORES = 2
EARLY_ROWS = 32
STRIPS = 2
VMEM_BYTES = 60 * 2**20


def turn(vector, row_shift, col_shift):
    width = vector.shape[-1]
    count = width // 4
    half = width // 2
    freqs = theta ** (-jnp.arange(count, dtype=jnp.float32) / count)
    extra = (1,) * (vector.ndim - 2)
    pieces = []
    for portion, shift in ((vector[..., :half], row_shift), (vector[..., half:], col_shift)):
        angle = (shift.astype(jnp.float32)[:, None] * freqs[None, :]).reshape(
            (shift.shape[0],) + extra + (count,)
        )
        lower = portion[..., :count]
        upper = portion[..., count:]
        pieces.append(
            jnp.concatenate(
                [
                    lower * jnp.cos(angle) - upper * jnp.sin(angle),
                    lower * jnp.sin(angle) + upper * jnp.cos(angle),
                ],
                axis=-1,
            )
        )
    return jnp.concatenate(pieces, axis=-1)


def norm_scale(values, gain):
    wide = values.astype(jnp.float32)
    return (
        wide
        * lax.rsqrt(jnp.mean(wide * wide, axis=-1, keepdims=True) + eps)
        * gain.astype(jnp.float32)
    )


def expert_active(rows, gate_w, up_w):
    gate_pre = jnp.minimum(jnp.dot(rows, gate_w, preferred_element_type=jnp.float32), limit)
    up_pre = jnp.clip(jnp.dot(rows, up_w, preferred_element_type=jnp.float32), -limit, limit)
    return ((up_pre + 1.0) * gate_pre * jax.nn.sigmoid(slope * gate_pre)).astype(jnp.bfloat16)


def flipped(index, mask):
    out = index
    bit = 1
    while bit <= mask:
        if mask & bit:
            out = out + bit - 2 * bit * ((index // bit) % 2)
        bit *= 2
    return out


def gatherer(chips, group, own, gathered, sems, launch):
    z_send, z_recv, x_send, x_recv, c_send, c_recv = sems
    place = lax.axis_index("sp")
    column = lax.axis_index("tp")
    chip, core = place // CORES, place % CORES
    per_chip = CORES * group
    partner = {"sp": chip * CORES + 1 - core}

    def other(shift):
        return (column + shift) % group

    def slot(k, core_at, column_at):
        return flipped(chip, k) * per_chip + core_at * group + column_at

    def chip_peer(k):
        return {"sp": flipped(chip, k) * CORES + core}

    def remote(src, dst, send_sem, recv_sem, device):
        return pltpu.make_async_remote_copy(
            src_ref=src, dst_ref=dst, send_sem=send_sem, recv_sem=recv_sem, device_id=device
        )

    def greet():
        barrier = pltpu.get_barrier_semaphore()
        pl.semaphore_signal(barrier, inc=1, device_id=partner)
        for k in range(1, chips):
            pl.semaphore_signal(barrier, inc=1, device_id=chip_peer(k))
        for shift in range(1, group):
            pl.semaphore_signal(barrier, inc=1, device_id={"tp": other(shift)})

    def met():
        pl.semaphore_wait(pltpu.get_barrier_semaphore(), chips + group - 1)

    def source(k, back):
        if k == 0 and back == 0:
            return own
        return gathered.at[slot(k, core, other(group - back))]

    def chip_wait(k):
        landed = gathered.at[slot(k, core, column)]
        remote(landed, landed, z_send.at[k], z_recv.at[k], chip_peer(k)).wait_recv()

    def core_copy(k, back):
        return remote(
            source(k, back),
            gathered.at[slot(k, core, other(group - back))],
            c_send.at[k, back],
            c_recv.at[k, back],
            partner,
        )

    def core_wait(k, back):
        landed = gathered.at[slot(k, 1 - core, other(group - back))]
        remote(landed, landed, c_send.at[k, back], c_recv.at[k, back], partner).wait_recv()

    def tp_copy(k, shift):
        return remote(
            source(k, 0),
            gathered.at[slot(k, core, column)],
            x_send.at[k, shift],
            x_recv.at[k, shift],
            {"tp": other(shift)},
        )

    def tp_wait(k, shift):
        landed = gathered.at[slot(k, core, other(group - shift))]
        remote(
            landed, landed, x_send.at[k, shift], x_recv.at[k, shift], {"tp": other(shift)}
        ).wait_recv()

    def spread(k):
        for shift in range(1, group):
            launch(tp_copy(k, shift))
        launch(core_copy(k, 0))

    def begin():
        for k in range(1, chips):
            launch(
                remote(
                    own,
                    gathered.at[slot(0, core, column)],
                    z_send.at[k],
                    z_recv.at[k],
                    chip_peer(k),
                )
            )
        spread(0)

    def step(k):
        if k + 1 < chips:
            chip_wait(k + 1)
            spread(k + 1)
        for shift in range(1, group):
            tp_wait(k, shift)
            launch(core_copy(k, shift))
        for back in range(group):
            core_wait(k, back)

    return greet, met, begin, step, slot, chip_peer, partner, other, remote


def turn_matrices(shape, width):
    row = lax.broadcasted_iota(jnp.int32, shape, 0)
    col = lax.broadcasted_iota(jnp.int32, shape, 1)
    count = width // 4
    lane = col % 128
    source = (col // 128) * width + lane
    inside = lane < width
    lower = lane % (2 * count) < count
    straight = jnp.where(inside & (row == source), 1.0, 0.0)
    moved = jnp.where(lower, source + count, source - count)
    sign = jnp.where(lower, -1.0, 1.0)
    crossed = jnp.where(inside & (row == moved), sign, 0.0)
    return straight.astype(jnp.bfloat16), crossed.astype(jnp.bfloat16)


def attention_stage(chips, group, inputs, out_ref, share_ref, refs, prefetch, swap):
    own, gathered, queries, cosines, sines, key_turns = refs[:6]
    held, load_sem, sems = refs[6:16], refs[16], refs[17:]
    (
        latent_ref,
        gain_ref,
        freqs_ref,
        key_turn_ref,
        routes_ref,
        route_weights_ref,
        query_turn_ref,
        query_ref,
        keyw_ref,
        valuew_ref,
    ) = held
    place = lax.axis_index("sp")
    column = lax.axis_index("tp")
    tokens, latent_width = inputs[0].shape
    rows_dev = own.shape[0]
    heads_dev = inputs[7].shape[1] // PLAIN_HEAD_WIDTH
    count = lax.axis_size("sp")
    per_chip = CORES * group
    sends = []

    def launch(copy):
        copy.start()
        sends.append(copy)

    greet, met, begin, step, slot = gatherer(chips, group, own, gathered, sems, launch)[:5]
    greet()
    loads = [
        pltpu.make_async_copy(src, dst, load_sem.at[i])
        for i, (src, dst) in enumerate(zip(inputs, held))
    ]
    for load in loads:
        load.start()
    loads[2].wait()

    at = place * tokens + lax.broadcasted_iota(jnp.int32, (tokens, 128), 0)
    lane = lax.broadcasted_iota(jnp.int32, (tokens, 128), 1)
    shift = jnp.where(lane < QK_ROPE // 2, at // GRID_W, at % GRID_W).astype(jnp.float32)
    angle = shift * freqs_ref[...]
    cosines[...] = jnp.cos(angle)
    sines[...] = jnp.sin(angle)

    def turned(vector, matrices, cos, sin):
        straight, crossed = (
            jnp.dot(vector, matrix, preferred_element_type=jnp.float32) for matrix in matrices
        )
        return straight * cos + crossed * sin

    mine = pl.ds(pl.multiple_of(column * rows_dev, 16), rows_dev)
    for load in loads[:2] + loads[3:6]:
        load.wait()
    key_turns[...] = key_turn_ref[...].T
    named = routes_ref[...].T
    weighing = route_weights_ref[...].T
    key_rot = turned(
        key_turns[mine, :],
        turn_matrices((QK_ROPE, 128), QK_ROPE),
        cosines[mine, :],
        sines[mine, :],
    )
    lane = lax.broadcasted_iota(jnp.int32, (rows_dev, 128), 1) - QK_ROPE
    expert = jnp.where(lane < count, lane, lane - count)
    share = jnp.zeros((rows_dev, 128), jnp.float32)
    for k in range(named.shape[1]):
        share = share + jnp.where(named[:, k : k + 1] == expert, weighing[:, k : k + 1], 0.0)
    high = share.astype(jnp.bfloat16).astype(jnp.float32)
    packed = jnp.where(lane < count, high, share - high)
    packed = jnp.where(lane < 2 * count, packed, 0.0)
    own[:, :latent_width] = norm_scale(latent_ref[mine, :], gain_ref[...].reshape(1, latent_width)).astype(jnp.bfloat16)
    own[:, latent_width:] = jnp.where(lane < 0, key_rot, packed).astype(jnp.bfloat16)
    met()
    begin()
    gathered[slot(0, place % CORES, column)] = own[...]

    for load in loads[6:]:
        load.wait()
    prefetch()
    matrices = turn_matrices((heads_dev * QK_ROPE, heads_dev * 128), QK_ROPE)
    straight, crossed = (
        jnp.dot(query_turn_ref[...], matrix, preferred_element_type=jnp.float32)
        for matrix in matrices
    )
    for head in range(heads_dev):
        span = slice(head * 128, (head + 1) * 128)
        queries[head, :, :128] = query_ref[:, span]
        queries[head, :, 128:] = (
            straight[:, span] * cosines[...] + crossed[:, span] * sines[...]
        ).astype(jnp.bfloat16)

    scale = (PLAIN_HEAD_WIDTH + QK_ROPE) ** (-0.5)
    peaks = [None] * heads_dev
    sums = [None] * heads_dev
    totals = [None] * heads_dev
    for k in range(chips):
        step(k)
        first = slot(k, 0, 0)
        width = per_chip * rows_dev
        latents = gathered[pl.ds(first, per_chip), :, :latent_width].reshape(width, latent_width)
        rot = gathered[pl.ds(first, per_chip), :, latent_width:].reshape(width, 128)
        keys = jnp.dot(latents, keyw_ref[...], preferred_element_type=jnp.float32).astype(
            jnp.bfloat16
        )
        values = jnp.dot(latents, valuew_ref[...], preferred_element_type=jnp.float32).astype(
            jnp.bfloat16
        )
        for head in range(heads_dev):
            span = slice(head * 128, (head + 1) * 128)
            scores = scale * lax.dot_general(
                queries[head],
                jnp.concatenate([keys[:, span], rot], axis=1),
                (((1,), (1,)), ((), ())),
                preferred_element_type=jnp.float32,
            )
            peak = jnp.max(scores, axis=1, keepdims=True)
            if k:
                peak = jnp.maximum(peak, peaks[head])
            weights = jnp.exp(scores - peak)
            total = jnp.sum(weights, axis=1, keepdims=True)
            summed = jnp.dot(
                weights.astype(jnp.bfloat16), values[:, span], preferred_element_type=jnp.float32
            )
            if k:
                fade = jnp.exp(peaks[head] - peak)
                total = total + fade * sums[head]
                summed = summed + fade * totals[head]
            peaks[head], sums[head], totals[head] = peak, total, summed
            if k == chips - 1:
                value = (summed / total).astype(jnp.bfloat16)
                out_ref[:, :, head * 128 : (head + 1) * 128] = value.reshape(group, rows_dev, 128)
                swap(head)
        lane = lax.broadcasted_iota(jnp.int32, (width, 128), 1) - QK_ROPE
        named = (lane == place) | (lane == place + count)
        share_ref[pl.ds(first // group, CORES)] = jnp.sum(
            jnp.where(named, rot.astype(jnp.float32), 0.0), axis=1, keepdims=True
        ).reshape(CORES, group, rows_dev, 1)
    for copy in sends:
        copy.wait_send()


def gather_sems(chips, group):
    dma = pltpu.SemaphoreType.DMA
    return [dma((chips,))] * 2 + [dma((chips, group))] * 4


def neighbour_order(chips):
    table = []
    for z in range(chips):
        table.append(sorted(range(chips), key=lambda o: (abs(o - z), o if z < chips // 2 else -o)))
    return table


def pick(z, values):
    out = values[0]
    for at in range(1, len(values)):
        out = jnp.where(z == at, values[at], out)
    return out


def experts_stage(chips, early, attended_ref, out_ref, share_ref, loads, swaps, refs):
    (
        heads,
        hidden,
        gathered,
        partial,
        from_core,
        from_x,
        from_x_early,
        from_z,
        from_z_early,
        residual_ref,
        gain_ref,
        outw_ref,
        gate_ref,
        up_ref,
        down_ref,
        gz_send,
        gz_recv,
        gx_send,
        gx_recv,
        gc_send,
        gc_recv,
        rc_send,
        rc_recv,
        rx_send,
        rx_recv,
        rz_send,
        rz_recv,
    ) = refs
    place = lax.axis_index("sp")
    column = lax.axis_index("tp")
    chip, core = place // CORES, place % CORES
    across = 1 - column
    rows_dev, model_width = hidden.shape
    late = rows_dev - early
    table = neighbour_order(chips)
    order = [chip] + [pick(chip, [table[z][j] for z in range(chips)]) for j in range(1, chips)]
    sends = []
    strips = STRIPS if model_width % (128 * STRIPS) == 0 else 1
    strip = model_width // strips
    parts = [pl.ds(at * strip, strip) for at in range(strips)]
    first_rows = pl.ds(0, early)
    last_rows = pl.ds(early, late)

    def launch(copy, when=None):
        if when is None:
            copy.start()
        else:
            pl.when(when)(copy.start)
        sends.append((copy, when))

    def remote(src, dst, send_sem, recv_sem, device):
        return pltpu.make_async_remote_copy(
            src_ref=src, dst_ref=dst, send_sem=send_sem, recv_sem=recv_sem, device_id=device
        )

    def on_chip(at):
        return {"sp": at * CORES + core}

    partner = {"sp": chip * CORES + 1 - core}
    beside = {"tp": across}

    for load in loads[:3]:
        load.wait()
    half = attended_ref.shape[2]

    def project(values, side):
        rows = pl.ds(pl.multiple_of(side * half, 128), half)
        return jnp.dot(values, outw_ref[rows, :], preferred_element_type=jnp.float32)

    projected = project(attended_ref[column], column)
    for copy in swaps:
        copy.wait_recv()
    projected = projected + project(heads[...], across)
    sends.extend((copy, None) for copy in swaps)
    mixed = (residual_ref[...].astype(jnp.float32) + projected).astype(jnp.bfloat16)
    gathered[place, column] = norm_scale(mixed, gain_ref[...].reshape(1, model_width)).astype(jnp.bfloat16)
    hidden[...] = mixed

    kinds = ((0, last_rows), (0, first_rows), (1, first_rows), (1, last_rows))
    use = [k for k in range(4) if (late if k in (0, 3) else early)]

    def piece(at, core_at, kind):
        flip, rows = kinds[kind]
        return gathered.at[at * CORES + core_at, across if flip else column, rows]

    def gz_copy(at, kind, to, lane):
        ref = piece(at, core, kind)
        return remote(ref, ref, gz_send.at[at, kind, lane], gz_recv.at[at, kind], on_chip(to))

    def gz_wait(at, kind):
        ref = piece(at, core, kind)
        remote(
            ref, ref, gz_send.at[at, kind, 0], gz_recv.at[at, kind], on_chip(at)
        ).wait_recv()

    def gx_copy(at, kind):
        ref = piece(at, core, kind)
        return remote(ref, ref, gx_send.at[at, kind], gx_recv.at[at, kind], beside)

    def gx_wait(at, kind):
        ref = piece(at, core, 3 - kind)
        remote(ref, ref, gx_send.at[at, kind], gx_recv.at[at, kind], beside).wait_recv()

    def gc_copy(at, kind):
        ref = piece(at, core, kind)
        return remote(ref, ref, gc_send.at[at, kind], gc_recv.at[at, kind], partner)

    def gc_wait(at, kind):
        ref = piece(at, 1 - core, kind)
        remote(ref, ref, gc_send.at[at, kind], gc_recv.at[at, kind], partner).wait_recv()

    def both_ways(kind):
        launch(gz_copy(chip, kind, chip - 1, 0), chip > 0)
        launch(gz_copy(chip, kind, chip + 1, 1), chip < chips - 1)

    def begin():
        if early:
            launch(gx_copy(chip, 1))
        if late:
            both_ways(0)
            launch(gx_copy(chip, 0))
        if early:
            both_ways(1)
        for kind in use:
            if kind < 2:
                launch(gc_copy(chip, kind))
        if early:
            gx_wait(chip, 1)
            both_ways(2)
            launch(gc_copy(chip, 2))

    def forward(at, kinds, now=None):
        step = jnp.where(at < chip, 1, -1)
        more = jnp.where(at < chip, chip < chips - 1, chip > 0)
        for kind in kinds:
            if kind not in use:
                continue
            if now is None:
                gz_wait(at, kind)
            else:
                pl.when(now)(functools.partial(gz_wait, at, kind))
            launch(gz_copy(at, kind, chip + step, 0), more if now is None else now & more)
            if kind == 0:
                launch(gx_copy(at, 0), now)
            launch(gc_copy(at, kind), now)

    def crossed(at):
        if late:
            gx_wait(at, 0)
            launch(gc_copy(at, 3))

    def apply(load_from, count, store_to):
        active = expert_active(load_from(gathered).reshape(count, model_width), gate_ref[...], up_ref[...])
        product = jnp.dot(active, down_ref[...], preferred_element_type=jnp.float32)
        store_to((product * load_from(share_ref).reshape(count, 1)).astype(jnp.bfloat16))

    def pair(at):
        return pl.ds(at * CORES, CORES)

    def compute_early(at):
        if not early:
            return
        gc_wait(at, 1)
        gc_wait(at, 2)

        def store(value):
            partial[pair(at), :, first_rows] = value.reshape(CORES, 2, early, model_width)

        apply(lambda ref: ref[pair(at), :, first_rows], 2 * CORES * early, store)
        launch(core_sum_early(at))

    def compute_late(at, kind):
        if not late:
            return
        gc_wait(at, kind)
        side = across if kind else column

        def store(value):
            partial[pair(at), side, last_rows] = value.reshape(CORES, late, model_width)

        apply(lambda ref: ref[pair(at), side, last_rows], CORES * late, store)
        launch(core_sum_late(at, kind))

    def core_sum_early(at):
        return remote(
            partial.at[at * CORES + 1 - core, :, first_rows],
            from_core.at[at, :, first_rows],
            rc_send.at[at, 1],
            rc_recv.at[at, 1],
            partner,
        )

    def core_sum_late(at, kind):
        side = across if kind else column
        return remote(
            partial.at[at * CORES + 1 - core, side, last_rows],
            from_core.at[at, side, last_rows],
            rc_send.at[at, kind],
            rc_recv.at[at, kind],
            partner,
        )

    def x_sum(at, n):
        return remote(
            partial.at[at * CORES + core, across, last_rows, parts[n]],
            from_x.at[at, :, parts[n]],
            rx_send.at[at, n],
            rx_recv.at[at, n],
            beside,
        )

    inner = (chip > 0) & (chip < chips - 1)
    outer = (chip == 0) | (chip == chips - 1)

    def z_sum(j, part, n):
        at = order[j]
        step = jnp.where(at > chip, 1, -1)
        to = chip + step
        slot = at
        if chips > 2:
            ends = outer if j == chips - 1 else False
            if j == chips - 1:
                to = jnp.where(outer, at, to)
            inward = (at > 0) & (at < chips - 1) & (step < 0)
            slot = jnp.where((to == at) & (inward | ends), chips, at)
        mine = at * CORES + core
        if part:
            src = partial.at[mine, column, last_rows, parts[n]]
            dst = from_z.at[slot, :, parts[n]]
        else:
            src = partial.at[mine, :, first_rows, parts[n]]
            dst = from_z_early.at[slot, :, :, parts[n]]
        return remote(src, dst, rz_send.at[at, part, n], rz_recv.at[slot, part, n], on_chip(to))

    def z_landed(slot, part, n):
        ref = from_z.at[slot, :, parts[n]] if part else from_z_early.at[slot, :, :, parts[n]]
        remote(
            ref, ref, rz_send.at[chip, part, n], rz_recv.at[slot, part, n], on_chip(chip)
        ).wait_recv()

    def pass_on(j, part):
        at = order[j]
        mine = at * CORES + core

        def add(n):
            z_landed(at, part, n)
            if part:
                partial[mine, column, last_rows, parts[n]] = (
                    wide(partial[mine, column, last_rows, parts[n]]) + wide(from_z[at, :, parts[n]])
                ).astype(jnp.bfloat16)
            else:
                partial[mine, :, first_rows, parts[n]] = (
                    wide(partial[mine, :, first_rows, parts[n]])
                    + wide(from_z_early[at, :, :, parts[n]])
                ).astype(jnp.bfloat16)

        for n in range(strips):
            pl.when(inner)(functools.partial(add, n))
            launch(z_sum(j, part, n), inner)

    def send_sum(j, part, n):
        if j:
            launch(z_sum(j, part, n), None if j == chips - 1 else outer)

    def wide(value):
        return value.astype(jnp.float32)

    def sum_early(j):
        at = order[j]
        if not early:
            return
        core_sum_early(at).wait_recv()
        mine = at * CORES + core
        partial[mine, :, first_rows] = (
            wide(partial[mine, :, first_rows]) + wide(from_core[at, :, first_rows])
        ).astype(jnp.bfloat16)
        for n in range(strips):
            send_sum(j, 0, n)

    def sum_late(j, kind):
        at = order[j]
        if not late:
            return
        core_sum_late(at, kind).wait_recv()
        mine = at * CORES + core
        side = across if kind else column
        partial[mine, side, last_rows] = (
            wide(partial[mine, side, last_rows]) + wide(from_core[at, side, last_rows])
        ).astype(jnp.bfloat16)
        if kind:
            for n in range(strips):
                launch(x_sum(at, n))

    def sum_across(j, now=None):
        at = order[j]
        if not late:
            return
        mine = at * CORES + core

        def add(n):
            x_sum(at, n).wait_recv()
            partial[mine, column, last_rows, parts[n]] = (
                wide(partial[mine, column, last_rows, parts[n]]) + wide(from_x[at, :, parts[n]])
            ).astype(jnp.bfloat16)

        for n in range(strips):
            if now is None:
                add(n)
            else:
                pl.when(now)(functools.partial(add, n))
            if now is None or now is outer:
                send_sum(j, 1, n)

    begin()
    for load in loads[3:]:
        load.wait()
    def work(j):
        at = order[j]
        compute_early(at)
        compute_late(at, 0)
        crossed(at)
        compute_late(at, 3)

    def gather_sums(j):
        sum_early(j)
        sum_late(j, 3)
        sum_late(j, 0)

    compute_early(chip)
    compute_late(chip, 0)
    forward(order[1], (0,))
    if chips > 2:
        forward(order[2], (0,), inner)
    crossed(chip)
    compute_late(chip, 3)
    forward(order[1], (1, 2))
    if chips > 2:
        forward(order[2], (1, 2), inner)
    gather_sums(0)
    work(1)
    if chips > 2:
        forward(order[2], (0,), outer)
        forward(order[3], (0,), inner)
        gather_sums(1)
        sum_across(0, outer)
        forward(order[2], (1, 2), outer)
        forward(order[3], (1, 2), inner)
        work(2)
        gather_sums(2)
        sum_across(0, inner)
        forward(order[3], (0,), outer)
        sum_across(1, outer)
        forward(order[3], (1, 2), outer)
        work(3)
        gather_sums(3)
        sum_across(1, inner)
        sum_across(2)
    else:
        gather_sums(1)
        sum_across(0)
    if early:
        for j in range(chips - 2, 0, -1):
            pass_on(j, 0)
    sum_across(chips - 1)
    mine = chip * CORES + core
    ends = (chip, chips) if chips > 2 else (chip,)

    def last(n):
        return remote(
            partial.at[mine, across, first_rows, parts[n]],
            from_x_early.at[:, parts[n]],
            rx_send.at[chips, n],
            rx_recv.at[chips, n],
            beside,
        )

    if early:
        for n in range(strips):
            total = wide(partial[mine, :, first_rows, parts[n]])
            for slot in ends:
                z_landed(slot, 0, n)
                total = total + wide(from_z_early[slot, :, :, parts[n]])
            partial[mine, :, first_rows, parts[n]] = total.astype(jnp.bfloat16)
            launch(last(n))
    if late:
        for j in range(chips - 2, 0, -1):
            pass_on(j, 1)
    for n in range(strips):
        if late:
            total = wide(hidden[last_rows, parts[n]]) + wide(
                partial[mine, column, last_rows, parts[n]]
            )
            for slot in ends:
                z_landed(slot, 1, n)
                total = total + wide(from_z[slot, :, parts[n]])
            out_ref[last_rows, parts[n]] = total.astype(jnp.bfloat16)
        if early:
            last(n).wait_recv()
            out_ref[first_rows, parts[n]] = (
                wide(hidden[first_rows, parts[n]])
                + wide(partial[mine, column, first_rows, parts[n]])
                + wide(from_x_early[:, parts[n]])
            ).astype(jnp.bfloat16)
    for copy, when in sends:
        if when is None:
            copy.wait_send()
        else:
            pl.when(when)(copy.wait_send)


def whole_kernel(chips, group, early, *refs):
    inputs, refs = refs[:16], refs[16:]
    out_ref, attended_ref, share_ref, load_sem, h_send, h_recv = refs[:6]
    first, second = refs[6:29], refs[29:]
    column = lax.axis_index("tp")
    swaps = []

    def swap(head):
        span = pl.ds(head * VALUE_WIDTH, VALUE_WIDTH)
        copy = pltpu.make_async_remote_copy(
            src_ref=attended_ref.at[1 - column, :, span],
            dst_ref=second[0].at[:, span],
            send_sem=h_send.at[head],
            recv_sem=h_recv.at[head],
            device_id={"tp": 1 - column},
        )
        copy.start()
        swaps.append(copy)

    loads = [
        pltpu.make_async_copy(src, dst, load_sem.at[i])
        for i, (src, dst) in enumerate(zip(inputs[10:], second[9:15]))
    ]

    def prefetch():
        for load in loads:
            load.start()

    attention_stage(chips, group, inputs[:10], attended_ref, share_ref, first, prefetch, swap)
    experts_stage(chips, early, attended_ref, out_ref, share_ref, loads, swaps, second)


def run_whole(
    query,
    query_turn,
    latent,
    key_turn,
    latent_gain,
    key_w,
    value_w,
    residual,
    out_w,
    gain,
    gate_w,
    up_w,
    down_w,
    routes,
    route_weights,
):
    group = lax.axis_size("tp")
    chips = lax.axis_size("sp") // CORES
    pairs = chips * CORES
    tokens, latent_width = latent.shape
    rows_dev, model_width = residual.shape
    heads_dev = query.shape[1] // PLAIN_HEAD_WIDTH
    early = EARLY_ROWS if rows_dev > EARLY_ROWS else 0
    late = rows_dev - early
    quarter = QK_ROPE // 4
    freqs = theta ** (-np.arange(quarter, dtype=np.float32) / np.float32(quarter))
    freqs = np.tile(freqs.astype(np.float32), 128 // quarter).reshape(1, 128)
    dma = pltpu.SemaphoreType.DMA
    block = (rows_dev, model_width)
    heads = (group, rows_dev, heads_dev * VALUE_WIDTH)
    sent = latent_width + 128

    def vmem(*shape):
        return pltpu.VMEM(shape, jnp.bfloat16)

    first = (
        latent,
        latent_gain,
        jnp.asarray(freqs),
        key_turn.T,
        routes.T,
        route_weights.T,
        query_turn,
        query,
        key_w,
        value_w,
    )
    second = (residual, gain, out_w, gate_w, up_w, down_w)
    return pl.pallas_call(
        functools.partial(whole_kernel, chips, group, early),
        out_shape=jax.ShapeDtypeStruct(block, jnp.bfloat16),
        in_specs=[pl.BlockSpec(memory_space=pltpu.HBM)] * 16,
        out_specs=pl.BlockSpec(memory_space=pltpu.VMEM),
        scratch_shapes=[
            vmem(*heads),
            pltpu.VMEM((pairs, group, rows_dev, 1), jnp.float32),
            dma((6,)),
            dma((heads_dev,)),
            dma((heads_dev,)),
            vmem(rows_dev, sent),
            vmem(pairs * group, rows_dev, sent),
            vmem(heads_dev, tokens, 256),
            pltpu.VMEM((tokens, 128), jnp.float32),
            pltpu.VMEM((tokens, 128), jnp.float32),
            vmem(tokens, QK_ROPE),
        ]
        + [pltpu.VMEM(array.shape, array.dtype) for array in first]
        + [dma((len(first),))]
        + gather_sems(chips, group)
        + [
            vmem(*heads[1:]),
            vmem(*block),
            vmem(pairs, 2, *block),
            vmem(pairs, 2, *block),
            vmem(chips, 2, *block),
            vmem(chips, late, model_width),
            vmem(max(early, 16), model_width),
            vmem(chips + 1, late, model_width),
            vmem(chips + 1, 2, max(early, 16), model_width),
        ]
        + [pltpu.VMEM(array.shape, array.dtype) for array in second]
        + [
            dma((chips, 3, 2)),
            dma((chips, 3)),
            dma((chips, 2)),
            dma((chips, 2)),
            dma((chips, 4)),
            dma((chips, 4)),
            dma((chips, 4)),
            dma((chips, 4)),
            dma((chips + 1, STRIPS)),
            dma((chips + 1, STRIPS)),
            dma((chips, 2, STRIPS)),
            dma((chips + 1, 2, STRIPS)),
        ],
        compiler_params=pltpu.CompilerParams(
            collective_id=0, has_side_effects=True, vmem_limit_bytes=VMEM_BYTES
        ),
    )(*first, *second)


def experts_fit(tokens, rows_dev, model_width):
    group, places = lax.axis_size("tp"), lax.axis_size("sp")
    chips = places // CORES
    if group != 2 or places % CORES or chips not in (2, 4) or rows_dev % 16:
        return False
    if tokens != group * rows_dev or QK_ROPE + 2 * places > 128:
        return False
    return 3 * places * group * rows_dev * model_width * 2 < VMEM_BYTES // 2


def on_device(
    query_plain,
    query_turn,
    latent,
    key_turn,
    latent_norm_scale,
    plain_key_matrix,
    value_matrix,
    residual,
    out_weight,
    ffn_gain,
    gate_weight,
    up_weight,
    down_weight,
    routes,
    route_weights,
):
    if experts_fit(latent.shape[0], *residual.shape):
        return run_whole(
            query_plain,
            query_turn,
            latent,
            key_turn,
            latent_norm_scale,
            plain_key_matrix,
            value_matrix,
            residual,
            out_weight,
            ffn_gain,
            gate_weight[0],
            up_weight[0],
            down_weight[0],
            routes,
            route_weights,
        )
    tok_dev = latent.shape[0]
    heads_dev = query_plain.shape[1] // PLAIN_HEAD_WIDTH
    model_width = residual.shape[1]
    place = lax.axis_index("sp") * tok_dev + jnp.arange(tok_dev, dtype=jnp.int32)
    grid_row = place // GRID_W
    grid_col = place % GRID_W
    rows_dev, model_width = residual.shape
    group = lax.axis_size("tp")
    count = lax.axis_size("sp")
    expert_ids = jnp.arange(count, dtype=jnp.int32)
    share = jnp.sum(
        route_weights[..., None] * (routes[..., None] == expert_ids).astype(jnp.float32), axis=1
    )
    latent_width = latent.shape[1]
    wide = latent_width + QK_ROPE

    def key_side(latents, turns, at_row, at_col):
        normed_latent = norm_scale(latents, latent_norm_scale).astype(jnp.bfloat16)
        key_rot = turn(turns.astype(jnp.float32), at_row, at_col).astype(jnp.bfloat16)
        return [normed_latent, key_rot]

    sent = jnp.concatenate(key_side(latent, key_turn, grid_row, grid_col), axis=1)
    everyone = lax.all_gather(sent, "sp", axis=0, tiled=True)
    shares = lax.all_gather(share, ("sp", "tp"), axis=0, tiled=True)
    own_share = jnp.sum(
        jnp.where(expert_ids[None, :] == lax.axis_index("sp"), shares, 0.0), axis=1, keepdims=True
    )
    all_latent = everyone[:, :latent_width]
    all_rot = everyone[:, latent_width:wide]
    keys = jnp.dot(all_latent, plain_key_matrix, preferred_element_type=jnp.float32).astype(
        jnp.bfloat16
    )
    values = jnp.dot(all_latent, value_matrix, preferred_element_type=jnp.float32).astype(
        jnp.bfloat16
    )
    query_rot = turn(
        query_turn.astype(jnp.float32).reshape(tok_dev, heads_dev, QK_ROPE), grid_row, grid_col
    ).astype(jnp.bfloat16)
    scale = (PLAIN_HEAD_WIDTH + QK_ROPE) ** (-0.5)
    attended = []
    for head in range(heads_dev):
        span = slice(head * PLAIN_HEAD_WIDTH, (head + 1) * PLAIN_HEAD_WIDTH)
        scores = (
            jnp.einsum(
                "qd,kd->qk", query_plain[:, span], keys[:, span], preferred_element_type=jnp.float32
            )
            + jnp.einsum(
                "qd,kd->qk", query_rot[:, head], all_rot, preferred_element_type=jnp.float32
            )
        ) * scale
        weights = jnp.exp(scores - jnp.max(scores, axis=1, keepdims=True))
        summed = jnp.dot(
            weights.astype(jnp.bfloat16),
            values[:, head * VALUE_WIDTH : (head + 1) * VALUE_WIDTH],
            preferred_element_type=jnp.float32,
        )
        attended.append(
            (summed / jnp.sum(weights, axis=1, keepdims=True)).astype(jnp.bfloat16)
        )
    attended = jnp.concatenate(attended, axis=1)
    swapped = lax.all_to_all(
        attended.reshape(group, rows_dev, heads_dev * VALUE_WIDTH),
        "tp",
        split_axis=0,
        concat_axis=0,
        tiled=True,
    )
    own_rows = jnp.transpose(swapped, (1, 0, 2)).reshape(rows_dev, group * heads_dev * VALUE_WIDTH)
    projected = jnp.dot(own_rows, out_weight, preferred_element_type=jnp.float32)
    hidden = (residual.astype(jnp.float32) + projected).astype(jnp.bfloat16)
    normed = norm_scale(hidden, ffn_gain).astype(jnp.bfloat16)
    rows = lax.all_gather(normed, ("sp", "tp"), axis=0, tiled=True)
    active = expert_active(rows, gate_weight[0], up_weight[0])
    product = jnp.dot(active, down_weight[0], preferred_element_type=jnp.float32)
    mixture = lax.psum_scatter(
        (own_share * product).astype(jnp.bfloat16),
        ("sp", "tp"),
        scatter_dimension=0,
        tiled=True,
    )
    return (hidden.astype(jnp.float32) + mixture.astype(jnp.float32)).astype(jnp.bfloat16)


def solution(mesh):
    placed = (
        P(("grp", "sp"), "tp"),
        P(("grp", "sp"), "tp"),
        P(("grp", "sp"), None),
        P(("grp", "sp"), None),
        P(),
        P(None, "tp"),
        P(None, "tp"),
        P(("grp", "sp", "tp"), None),
        P(),
        P(),
        P("sp", None, "tp"),
        P("sp", None, "tp"),
        P("sp", "tp", None),
        P(("grp", "sp", "tp"), None),
        P(("grp", "sp", "tp"), None),
    )
    return jax.shard_map(
        on_device,
        mesh=mesh,
        in_specs=placed,
        out_specs=P(("grp", "sp", "tp"), None),
        check_vma=False,
    )
```

```python
import functools

import jax
import jax.numpy as jnp
import numpy as np
from jax import lax
from jax.experimental import pallas as pl
from jax.experimental.pallas import tpu as pltpu
from jax.sharding import PartitionSpec as P

PLAIN_HEAD_WIDTH = 128
QK_ROPE = 64
VALUE_WIDTH = 128
GRID_W = 64


theta = 10000.0
eps = 1e-06
limit = 7.0
slope = 1.702
CORES = 2
EARLY_ROWS = 32
STRIPS = 2
VMEM_BYTES = 60 * 2**20


def turn(vector, row_shift, col_shift):
    width = vector.shape[-1]
    count = width // 4
    half = width // 2
    freqs = theta ** (-jnp.arange(count, dtype=jnp.float32) / count)
    extra = (1,) * (vector.ndim - 2)
    pieces = []
    for portion, shift in ((vector[..., :half], row_shift), (vector[..., half:], col_shift)):
        angle = (shift.astype(jnp.float32)[:, None] * freqs[None, :]).reshape(
            (shift.shape[0],) + extra + (count,)
        )
        lower = portion[..., :count]
        upper = portion[..., count:]
        pieces.append(
            jnp.concatenate(
                [
                    lower * jnp.cos(angle) - upper * jnp.sin(angle),
                    lower * jnp.sin(angle) + upper * jnp.cos(angle),
                ],
                axis=-1,
            )
        )
    return jnp.concatenate(pieces, axis=-1)


def norm_scale(values, gain):
    wide = values.astype(jnp.float32)
    return (
        wide
        * lax.rsqrt(jnp.mean(wide * wide, axis=-1, keepdims=True) + eps)
        * gain.astype(jnp.float32)
    )


def expert_active(rows, gate_w, up_w):
    gate_pre = jnp.minimum(jnp.dot(rows, gate_w, preferred_element_type=jnp.float32), limit)
    up_pre = jnp.clip(jnp.dot(rows, up_w, preferred_element_type=jnp.float32), -limit, limit)
    return ((up_pre + 1.0) * gate_pre * jax.nn.sigmoid(slope * gate_pre)).astype(jnp.bfloat16)


def flipped(index, mask):
    out = index
    bit = 1
    while bit <= mask:
        if mask & bit:
            out = out + bit - 2 * bit * ((index // bit) % 2)
        bit *= 2
    return out


def gatherer(chips, group, own, gathered, sems, launch):
    z_send, z_recv, x_send, x_recv, c_send, c_recv = sems
    place = lax.axis_index("sp")
    column = lax.axis_index("tp")
    chip, core = place // CORES, place % CORES
    per_chip = CORES * group
    partner = {"sp": chip * CORES + 1 - core}

    def other(shift):
        return (column + shift) % group

    def slot(k, core_at, column_at):
        return flipped(chip, k) * per_chip + core_at * group + column_at

    def chip_peer(k):
        return {"sp": flipped(chip, k) * CORES + core}

    def remote(src, dst, send_sem, recv_sem, device):
        return pltpu.make_async_remote_copy(
            src_ref=src, dst_ref=dst, send_sem=send_sem, recv_sem=recv_sem, device_id=device
        )

    def greet():
        barrier = pltpu.get_barrier_semaphore()
        pl.semaphore_signal(barrier, inc=1, device_id=partner)
        for k in range(1, chips):
            pl.semaphore_signal(barrier, inc=1, device_id=chip_peer(k))
        for shift in range(1, group):
            pl.semaphore_signal(barrier, inc=1, device_id={"tp": other(shift)})

    def met():
        pl.semaphore_wait(pltpu.get_barrier_semaphore(), chips + group - 1)

    def source(k, back):
        if k == 0 and back == 0:
            return own
        return gathered.at[slot(k, core, other(group - back))]

    def chip_wait(k):
        landed = gathered.at[slot(k, core, column)]
        remote(landed, landed, z_send.at[k], z_recv.at[k], chip_peer(k)).wait_recv()

    def core_copy(k, back):
        return remote(
            source(k, back),
            gathered.at[slot(k, core, other(group - back))],
            c_send.at[k, back],
            c_recv.at[k, back],
            partner,
        )

    def core_wait(k, back):
        landed = gathered.at[slot(k, 1 - core, other(group - back))]
        remote(landed, landed, c_send.at[k, back], c_recv.at[k, back], partner).wait_recv()

    def tp_copy(k, shift):
        return remote(
            source(k, 0),
            gathered.at[slot(k, core, column)],
            x_send.at[k, shift],
            x_recv.at[k, shift],
            {"tp": other(shift)},
        )

    def tp_wait(k, shift):
        landed = gathered.at[slot(k, core, other(group - shift))]
        remote(
            landed, landed, x_send.at[k, shift], x_recv.at[k, shift], {"tp": other(shift)}
        ).wait_recv()

    def spread(k):
        for shift in range(1, group):
            launch(tp_copy(k, shift))
        launch(core_copy(k, 0))

    def begin():
        for k in range(1, chips):
            launch(
                remote(
                    own,
                    gathered.at[slot(0, core, column)],
                    z_send.at[k],
                    z_recv.at[k],
                    chip_peer(k),
                )
            )
        spread(0)

    def step(k):
        if k + 1 < chips:
            chip_wait(k + 1)
            spread(k + 1)
        for shift in range(1, group):
            tp_wait(k, shift)
            launch(core_copy(k, shift))
        for back in range(group):
            core_wait(k, back)

    return greet, met, begin, step, slot, chip_peer, partner, other, remote


def turn_matrices(shape, width):
    row = lax.broadcasted_iota(jnp.int32, shape, 0)
    col = lax.broadcasted_iota(jnp.int32, shape, 1)
    count = width // 4
    lane = col % 128
    source = (col // 128) * width + lane
    inside = lane < width
    lower = lane % (2 * count) < count
    straight = jnp.where(inside & (row == source), 1.0, 0.0)
    moved = jnp.where(lower, source + count, source - count)
    sign = jnp.where(lower, -1.0, 1.0)
    crossed = jnp.where(inside & (row == moved), sign, 0.0)
    return straight.astype(jnp.bfloat16), crossed.astype(jnp.bfloat16)


def attention_stage(chips, group, inputs, out_ref, share_ref, refs, prefetch, swap):
    own, gathered, queries, cosines, sines, key_turns = refs[:6]
    held, load_sem, sems = refs[6:16], refs[16], refs[17:]
    (
        latent_ref,
        gain_ref,
        freqs_ref,
        key_turn_ref,
        routes_ref,
        route_weights_ref,
        query_turn_ref,
        query_ref,
        keyw_ref,
        valuew_ref,
    ) = held
    place = lax.axis_index("sp")
    column = lax.axis_index("tp")
    tokens, latent_width = inputs[0].shape
    rows_dev = own.shape[0]
    heads_dev = inputs[7].shape[1] // PLAIN_HEAD_WIDTH
    count = lax.axis_size("sp")
    per_chip = CORES * group
    sends = []

    def launch(copy):
        copy.start()
        sends.append(copy)

    greet, met, begin, step, slot = gatherer(chips, group, own, gathered, sems, launch)[:5]
    greet()
    loads = [
        pltpu.make_async_copy(src, dst, load_sem.at[i])
        for i, (src, dst) in enumerate(zip(inputs, held))
    ]
    for load in loads:
        load.start()
    loads[2].wait()

    at = place * tokens + lax.broadcasted_iota(jnp.int32, (tokens, 128), 0)
    lane = lax.broadcasted_iota(jnp.int32, (tokens, 128), 1)
    shift = jnp.where(lane < QK_ROPE // 2, at // GRID_W, at % GRID_W).astype(jnp.float32)
    angle = shift * freqs_ref[...]
    cosines[...] = jnp.cos(angle)
    sines[...] = jnp.sin(angle)

    def turned(vector, matrices, cos, sin):
        straight, crossed = (
            jnp.dot(vector, matrix, preferred_element_type=jnp.float32) for matrix in matrices
        )
        return straight * cos + crossed * sin

    mine = pl.ds(pl.multiple_of(column * rows_dev, 16), rows_dev)
    for load in loads[:2] + loads[3:6]:
        load.wait()
    key_turns[...] = key_turn_ref[...].T
    named = routes_ref[...].T
    weighing = route_weights_ref[...].T
    key_rot = turned(
        key_turns[mine, :],
        turn_matrices((QK_ROPE, 128), QK_ROPE),
        cosines[mine, :],
        sines[mine, :],
    )
    lane = lax.broadcasted_iota(jnp.int32, (rows_dev, 128), 1) - QK_ROPE
    expert = jnp.where(lane < count, lane, lane - count)
    share = jnp.zeros((rows_dev, 128), jnp.float32)
    for k in range(named.shape[1]):
        share = share + jnp.where(named[:, k : k + 1] == expert, weighing[:, k : k + 1], 0.0)
    high = share.astype(jnp.bfloat16).astype(jnp.float32)
    packed = jnp.where(lane < count, high, share - high)
    packed = jnp.where(lane < 2 * count, packed, 0.0)
    own[:, :latent_width] = norm_scale(latent_ref[mine, :], gain_ref[...].reshape(1, latent_width)).astype(jnp.bfloat16)
    own[:, latent_width:] = jnp.where(lane < 0, key_rot, packed).astype(jnp.bfloat16)
    met()
    begin()
    gathered[slot(0, place % CORES, column)] = own[...]

    for load in loads[6:]:
        load.wait()
    prefetch()
    matrices = turn_matrices((heads_dev * QK_ROPE, heads_dev * 128), QK_ROPE)
    straight, crossed = (
        jnp.dot(query_turn_ref[...], matrix, preferred_element_type=jnp.float32)
        for matrix in matrices
    )
    for head in range(heads_dev):
        span = slice(head * 128, (head + 1) * 128)
        queries[head, :, :128] = query_ref[:, span]
        queries[head, :, 128:] = (
            straight[:, span] * cosines[...] + crossed[:, span] * sines[...]
        ).astype(jnp.bfloat16)

    scale = (PLAIN_HEAD_WIDTH + QK_ROPE) ** (-0.5)
    peaks = [None] * heads_dev
    sums = [None] * heads_dev
    totals = [None] * heads_dev
    for k in range(chips):
        step(k)
        first = slot(k, 0, 0)
        width = per_chip * rows_dev
        latents = gathered[pl.ds(first, per_chip), :, :latent_width].reshape(width, latent_width)
        rot = gathered[pl.ds(first, per_chip), :, latent_width:].reshape(width, 128)
        keys = jnp.dot(latents, keyw_ref[...], preferred_element_type=jnp.float32).astype(
            jnp.bfloat16
        )
        values = jnp.dot(latents, valuew_ref[...], preferred_element_type=jnp.float32).astype(
            jnp.bfloat16
        )
        for head in range(heads_dev):
            span = slice(head * 128, (head + 1) * 128)
            scores = scale * lax.dot_general(
                queries[head],
                jnp.concatenate([keys[:, span], rot], axis=1),
                (((1,), (1,)), ((), ())),
                preferred_element_type=jnp.float32,
            )
            peak = jnp.max(scores, axis=1, keepdims=True)
            if k:
                peak = jnp.maximum(peak, peaks[head])
            weights = jnp.exp(scores - peak)
            total = jnp.sum(weights, axis=1, keepdims=True)
            summed = jnp.dot(
                weights.astype(jnp.bfloat16), values[:, span], preferred_element_type=jnp.float32
            )
            if k:
                fade = jnp.exp(peaks[head] - peak)
                total = total + fade * sums[head]
                summed = summed + fade * totals[head]
            peaks[head], sums[head], totals[head] = peak, total, summed
            if k == chips - 1:
                value = (summed / total).astype(jnp.bfloat16)
                out_ref[:, :, head * 128 : (head + 1) * 128] = value.reshape(group, rows_dev, 128)
                swap(head)
        lane = lax.broadcasted_iota(jnp.int32, (width, 128), 1) - QK_ROPE
        named = (lane == place) | (lane == place + count)
        share_ref[pl.ds(first // group, CORES)] = jnp.sum(
            jnp.where(named, rot.astype(jnp.float32), 0.0), axis=1, keepdims=True
        ).reshape(CORES, group, rows_dev, 1)
    for copy in sends:
        copy.wait_send()


def gather_sems(chips, group):
    dma = pltpu.SemaphoreType.DMA
    return [dma((chips,))] * 2 + [dma((chips, group))] * 4


def neighbour_order(chips):
    table = []
    for z in range(chips):
        table.append(sorted(range(chips), key=lambda o: (abs(o - z), o if z < chips // 2 else -o)))
    return table


def pick(z, values):
    out = values[0]
    for at in range(1, len(values)):
        out = jnp.where(z == at, values[at], out)
    return out


def experts_stage(chips, early, attended_ref, out_ref, share_ref, loads, swaps, refs):
    (
        heads,
        hidden,
        gathered,
        partial,
        from_core,
        from_x,
        from_x_early,
        from_z,
        from_z_early,
        residual_ref,
        gain_ref,
        outw_ref,
        gate_ref,
        up_ref,
        down_ref,
        gz_send,
        gz_recv,
        gx_send,
        gx_recv,
        gc_send,
        gc_recv,
        rc_send,
        rc_recv,
        rx_send,
        rx_recv,
        rz_send,
        rz_recv,
    ) = refs
    place = lax.axis_index("sp")
    column = lax.axis_index("tp")
    chip, core = place // CORES, place % CORES
    across = 1 - column
    rows_dev, model_width = hidden.shape
    late = rows_dev - early
    table = neighbour_order(chips)
    order = [chip] + [pick(chip, [table[z][j] for z in range(chips)]) for j in range(1, chips)]
    sends = []
    strips = STRIPS if model_width % (128 * STRIPS) == 0 else 1
    strip = model_width // strips
    parts = [pl.ds(at * strip, strip) for at in range(strips)]
    first_rows = pl.ds(0, early)
    last_rows = pl.ds(early, late)

    def launch(copy, when=None):
        if when is None:
            copy.start()
        else:
            pl.when(when)(copy.start)
        sends.append((copy, when))

    def remote(src, dst, send_sem, recv_sem, device):
        return pltpu.make_async_remote_copy(
            src_ref=src, dst_ref=dst, send_sem=send_sem, recv_sem=recv_sem, device_id=device
        )

    def on_chip(at):
        return {"sp": at * CORES + core}

    partner = {"sp": chip * CORES + 1 - core}
    beside = {"tp": across}

    for load in loads[:3]:
        load.wait()
    half = attended_ref.shape[2]

    def project(values, side):
        rows = pl.ds(pl.multiple_of(side * half, 128), half)
        return jnp.dot(values, outw_ref[rows, :], preferred_element_type=jnp.float32)

    projected = project(attended_ref[column], column)
    for copy in swaps:
        copy.wait_recv()
    projected = projected + project(heads[...], across)
    sends.extend((copy, None) for copy in swaps)
    mixed = (residual_ref[...].astype(jnp.float32) + projected).astype(jnp.bfloat16)
    gathered[place, column] = norm_scale(mixed, gain_ref[...].reshape(1, model_width)).astype(jnp.bfloat16)
    hidden[...] = mixed

    kinds = ((0, last_rows), (0, first_rows), (1, first_rows), (1, last_rows))
    use = [k for k in range(4) if (late if k in (0, 3) else early)]

    def piece(at, core_at, kind):
        flip, rows = kinds[kind]
        return gathered.at[at * CORES + core_at, across if flip else column, rows]

    def gz_copy(at, kind, to, lane):
        ref = piece(at, core, kind)
        return remote(ref, ref, gz_send.at[at, kind, lane], gz_recv.at[at, kind], on_chip(to))

    def gz_wait(at, kind):
        ref = piece(at, core, kind)
        remote(
            ref, ref, gz_send.at[at, kind, 0], gz_recv.at[at, kind], on_chip(at)
        ).wait_recv()

    def gx_copy(at, kind):
        ref = piece(at, core, kind)
        return remote(ref, ref, gx_send.at[at, kind], gx_recv.at[at, kind], beside)

    def gx_wait(at, kind):
        ref = piece(at, core, 3 - kind)
        remote(ref, ref, gx_send.at[at, kind], gx_recv.at[at, kind], beside).wait_recv()

    def gc_copy(at, kind):
        ref = piece(at, core, kind)
        return remote(ref, ref, gc_send.at[at, kind], gc_recv.at[at, kind], partner)

    def gc_wait(at, kind):
        ref = piece(at, 1 - core, kind)
        remote(ref, ref, gc_send.at[at, kind], gc_recv.at[at, kind], partner).wait_recv()

    def both_ways(kind):
        launch(gz_copy(chip, kind, chip - 1, 0), chip > 0)
        launch(gz_copy(chip, kind, chip + 1, 1), chip < chips - 1)

    def begin():
        if early:
            launch(gx_copy(chip, 1))
        if late:
            both_ways(0)
            launch(gx_copy(chip, 0))
        if early:
            both_ways(1)
        for kind in use:
            if kind < 2:
                launch(gc_copy(chip, kind))
        if early:
            gx_wait(chip, 1)
            both_ways(2)
            launch(gc_copy(chip, 2))

    def forward(at, kinds, now=None):
        step = jnp.where(at < chip, 1, -1)
        more = jnp.where(at < chip, chip < chips - 1, chip > 0)
        for kind in kinds:
            if kind not in use:
                continue
            if now is None:
                gz_wait(at, kind)
            else:
                pl.when(now)(functools.partial(gz_wait, at, kind))
            launch(gz_copy(at, kind, chip + step, 0), more if now is None else now & more)
            if kind == 0:
                launch(gx_copy(at, 0), now)
            launch(gc_copy(at, kind), now)

    def crossed(at):
        if late:
            gx_wait(at, 0)
            launch(gc_copy(at, 3))

    def apply(load_from, count, store_to):
        active = expert_active(load_from(gathered).reshape(count, model_width), gate_ref[...], up_ref[...])
        product = jnp.dot(active, down_ref[...], preferred_element_type=jnp.float32)
        store_to((product * load_from(share_ref).reshape(count, 1)).astype(jnp.bfloat16))

    def pair(at):
        return pl.ds(at * CORES, CORES)

    def compute_early(at):
        if not early:
            return
        gc_wait(at, 1)
        gc_wait(at, 2)

        def store(value):
            partial[pair(at), :, first_rows] = value.reshape(CORES, 2, early, model_width)

        apply(lambda ref: ref[pair(at), :, first_rows], 2 * CORES * early, store)
        launch(core_sum_early(at))

    def compute_late(at, kind):
        if not late:
            return
        gc_wait(at, kind)
        side = across if kind else column

        def store(value):
            partial[pair(at), side, last_rows] = value.reshape(CORES, late, model_width)

        apply(lambda ref: ref[pair(at), side, last_rows], CORES * late, store)
        launch(core_sum_late(at, kind))

    def core_sum_early(at):
        return remote(
            partial.at[at * CORES + 1 - core, :, first_rows],
            from_core.at[at, :, first_rows],
            rc_send.at[at, 1],
            rc_recv.at[at, 1],
            partner,
        )

    def core_sum_late(at, kind):
        side = across if kind else column
        return remote(
            partial.at[at * CORES + 1 - core, side, last_rows],
            from_core.at[at, side, last_rows],
            rc_send.at[at, kind],
            rc_recv.at[at, kind],
            partner,
        )

    def x_sum(at, n):
        return remote(
            partial.at[at * CORES + core, across, last_rows, parts[n]],
            from_x.at[at, :, parts[n]],
            rx_send.at[at, n],
            rx_recv.at[at, n],
            beside,
        )

    inner = (chip > 0) & (chip < chips - 1)
    outer = (chip == 0) | (chip == chips - 1)

    def z_sum(j, part, n):
        at = order[j]
        step = jnp.where(at > chip, 1, -1)
        to = chip + step
        slot = at
        if chips > 2:
            ends = outer if j == chips - 1 else False
            if j == chips - 1:
                to = jnp.where(outer, at, to)
            inward = (at > 0) & (at < chips - 1) & (step < 0)
            slot = jnp.where((to == at) & (inward | ends), chips, at)
        mine = at * CORES + core
        if part:
            src = partial.at[mine, column, last_rows, parts[n]]
            dst = from_z.at[slot, :, parts[n]]
        else:
            src = partial.at[mine, :, first_rows, parts[n]]
            dst = from_z_early.at[slot, :, :, parts[n]]
        return remote(src, dst, rz_send.at[at, part, n], rz_recv.at[slot, part, n], on_chip(to))

    def z_landed(slot, part, n):
        ref = from_z.at[slot, :, parts[n]] if part else from_z_early.at[slot, :, :, parts[n]]
        remote(
            ref, ref, rz_send.at[chip, part, n], rz_recv.at[slot, part, n], on_chip(chip)
        ).wait_recv()

    def pass_on(j, part):
        at = order[j]
        mine = at * CORES + core

        def add(n):
            z_landed(at, part, n)
            if part:
                partial[mine, column, last_rows, parts[n]] = (
                    wide(partial[mine, column, last_rows, parts[n]]) + wide(from_z[at, :, parts[n]])
                ).astype(jnp.bfloat16)
            else:
                partial[mine, :, first_rows, parts[n]] = (
                    wide(partial[mine, :, first_rows, parts[n]])
                    + wide(from_z_early[at, :, :, parts[n]])
                ).astype(jnp.bfloat16)

        for n in range(strips):
            pl.when(inner)(functools.partial(add, n))
            launch(z_sum(j, part, n), inner)

    def send_sum(j, part, n):
        if j:
            launch(z_sum(j, part, n), None if j == chips - 1 else outer)

    def wide(value):
        return value.astype(jnp.float32)

    def sum_early(j):
        at = order[j]
        if not early:
            return
        core_sum_early(at).wait_recv()
        mine = at * CORES + core
        partial[mine, :, first_rows] = (
            wide(partial[mine, :, first_rows]) + wide(from_core[at, :, first_rows])
        ).astype(jnp.bfloat16)
        for n in range(strips):
            send_sum(j, 0, n)

    def sum_late(j, kind):
        at = order[j]
        if not late:
            return
        core_sum_late(at, kind).wait_recv()
        mine = at * CORES + core
        side = across if kind else column
        partial[mine, side, last_rows] = (
            wide(partial[mine, side, last_rows]) + wide(from_core[at, side, last_rows])
        ).astype(jnp.bfloat16)
        if kind:
            for n in range(strips):
                launch(x_sum(at, n))

    def sum_across(j, now=None):
        at = order[j]
        if not late:
            return
        mine = at * CORES + core

        def add(n):
            x_sum(at, n).wait_recv()
            partial[mine, column, last_rows, parts[n]] = (
                wide(partial[mine, column, last_rows, parts[n]]) + wide(from_x[at, :, parts[n]])
            ).astype(jnp.bfloat16)

        for n in range(strips):
            if now is None:
                add(n)
            else:
                pl.when(now)(functools.partial(add, n))
            if now is None or now is outer:
                send_sum(j, 1, n)

    begin()
    for load in loads[3:]:
        load.wait()
    def work(j):
        at = order[j]
        compute_early(at)
        compute_late(at, 0)
        crossed(at)
        compute_late(at, 3)

    def gather_sums(j):
        sum_early(j)
        sum_late(j, 3)
        sum_late(j, 0)

    compute_early(chip)
    compute_late(chip, 0)
    forward(order[1], (0,))
    if chips > 2:
        forward(order[2], (0,), inner)
    crossed(chip)
    compute_late(chip, 3)
    forward(order[1], (1, 2))
    if chips > 2:
        forward(order[2], (1, 2), inner)
    gather_sums(0)
    work(1)
    if chips > 2:
        forward(order[2], (0,), outer)
        forward(order[3], (0,), inner)
        gather_sums(1)
        forward(order[2], (1, 2), outer)
        forward(order[3], (1, 2), inner)
        sum_across(0, outer)
        work(2)
        forward(order[3], (0,), outer)
        gather_sums(2)
        sum_across(0, inner)
        sum_across(1, outer)
        forward(order[3], (1, 2), outer)
        work(3)
        gather_sums(3)
        sum_across(1, inner)
        sum_across(2)
    else:
        gather_sums(1)
        sum_across(0)
    if early:
        for j in range(chips - 2, 0, -1):
            pass_on(j, 0)
    sum_across(chips - 1)
    mine = chip * CORES + core
    ends = (chip, chips) if chips > 2 else (chip,)

    def last(n):
        return remote(
            partial.at[mine, across, first_rows, parts[n]],
            from_x_early.at[:, parts[n]],
            rx_send.at[chips, n],
            rx_recv.at[chips, n],
            beside,
        )

    if early:
        for n in range(strips):
            total = wide(partial[mine, :, first_rows, parts[n]])
            for slot in ends:
                z_landed(slot, 0, n)
                total = total + wide(from_z_early[slot, :, :, parts[n]])
            partial[mine, :, first_rows, parts[n]] = total.astype(jnp.bfloat16)
            launch(last(n))
    if late:
        for j in range(chips - 2, 0, -1):
            pass_on(j, 1)
    for n in range(strips):
        if late:
            total = wide(hidden[last_rows, parts[n]]) + wide(
                partial[mine, column, last_rows, parts[n]]
            )
            for slot in ends:
                z_landed(slot, 1, n)
                total = total + wide(from_z[slot, :, parts[n]])
            out_ref[last_rows, parts[n]] = total.astype(jnp.bfloat16)
        if early:
            last(n).wait_recv()
            out_ref[first_rows, parts[n]] = (
                wide(hidden[first_rows, parts[n]])
                + wide(partial[mine, column, first_rows, parts[n]])
                + wide(from_x_early[:, parts[n]])
            ).astype(jnp.bfloat16)
    for copy, when in sends:
        if when is None:
            copy.wait_send()
        else:
            pl.when(when)(copy.wait_send)


def whole_kernel(chips, group, early, *refs):
    inputs, refs = refs[:16], refs[16:]
    out_ref, attended_ref, share_ref, load_sem, h_send, h_recv = refs[:6]
    first, second = refs[6:29], refs[29:]
    column = lax.axis_index("tp")
    swaps = []

    def swap(head):
        span = pl.ds(head * VALUE_WIDTH, VALUE_WIDTH)
        copy = pltpu.make_async_remote_copy(
            src_ref=attended_ref.at[1 - column, :, span],
            dst_ref=second[0].at[:, span],
            send_sem=h_send.at[head],
            recv_sem=h_recv.at[head],
            device_id={"tp": 1 - column},
        )
        copy.start()
        swaps.append(copy)

    loads = [
        pltpu.make_async_copy(src, dst, load_sem.at[i])
        for i, (src, dst) in enumerate(zip(inputs[10:], second[9:15]))
    ]

    def prefetch():
        for load in loads:
            load.start()

    attention_stage(chips, group, inputs[:10], attended_ref, share_ref, first, prefetch, swap)
    experts_stage(chips, early, attended_ref, out_ref, share_ref, loads, swaps, second)


def run_whole(
    query,
    query_turn,
    latent,
    key_turn,
    latent_gain,
    key_w,
    value_w,
    residual,
    out_w,
    gain,
    gate_w,
    up_w,
    down_w,
    routes,
    route_weights,
):
    group = lax.axis_size("tp")
    chips = lax.axis_size("sp") // CORES
    pairs = chips * CORES
    tokens, latent_width = latent.shape
    rows_dev, model_width = residual.shape
    heads_dev = query.shape[1] // PLAIN_HEAD_WIDTH
    early = EARLY_ROWS if rows_dev > EARLY_ROWS else 0
    late = rows_dev - early
    quarter = QK_ROPE // 4
    freqs = theta ** (-np.arange(quarter, dtype=np.float32) / np.float32(quarter))
    freqs = np.tile(freqs.astype(np.float32), 128 // quarter).reshape(1, 128)
    dma = pltpu.SemaphoreType.DMA
    block = (rows_dev, model_width)
    heads = (group, rows_dev, heads_dev * VALUE_WIDTH)
    sent = latent_width + 128

    def vmem(*shape):
        return pltpu.VMEM(shape, jnp.bfloat16)

    first = (
        latent,
        latent_gain,
        jnp.asarray(freqs),
        key_turn.T,
        routes.T,
        route_weights.T,
        query_turn,
        query,
        key_w,
        value_w,
    )
    second = (residual, gain, out_w, gate_w, up_w, down_w)
    return pl.pallas_call(
        functools.partial(whole_kernel, chips, group, early),
        out_shape=jax.ShapeDtypeStruct(block, jnp.bfloat16),
        in_specs=[pl.BlockSpec(memory_space=pltpu.HBM)] * 16,
        out_specs=pl.BlockSpec(memory_space=pltpu.VMEM),
        scratch_shapes=[
            vmem(*heads),
            pltpu.VMEM((pairs, group, rows_dev, 1), jnp.float32),
            dma((6,)),
            dma((heads_dev,)),
            dma((heads_dev,)),
            vmem(rows_dev, sent),
            vmem(pairs * group, rows_dev, sent),
            vmem(heads_dev, tokens, 256),
            pltpu.VMEM((tokens, 128), jnp.float32),
            pltpu.VMEM((tokens, 128), jnp.float32),
            vmem(tokens, QK_ROPE),
        ]
        + [pltpu.VMEM(array.shape, array.dtype) for array in first]
        + [dma((len(first),))]
        + gather_sems(chips, group)
        + [
            vmem(*heads[1:]),
            vmem(*block),
            vmem(pairs, 2, *block),
            vmem(pairs, 2, *block),
            vmem(chips, 2, *block),
            vmem(chips, late, model_width),
            vmem(max(early, 16), model_width),
            vmem(chips + 1, late, model_width),
            vmem(chips + 1, 2, max(early, 16), model_width),
        ]
        + [pltpu.VMEM(array.shape, array.dtype) for array in second]
        + [
            dma((chips, 3, 2)),
            dma((chips, 3)),
            dma((chips, 2)),
            dma((chips, 2)),
            dma((chips, 4)),
            dma((chips, 4)),
            dma((chips, 4)),
            dma((chips, 4)),
            dma((chips + 1, STRIPS)),
            dma((chips + 1, STRIPS)),
            dma((chips, 2, STRIPS)),
            dma((chips + 1, 2, STRIPS)),
        ],
        compiler_params=pltpu.CompilerParams(
            collective_id=0, has_side_effects=True, vmem_limit_bytes=VMEM_BYTES
        ),
    )(*first, *second)


def experts_fit(tokens, rows_dev, model_width):
    group, places = lax.axis_size("tp"), lax.axis_size("sp")
    chips = places // CORES
    if group != 2 or places % CORES or chips not in (2, 4) or rows_dev % 16:
        return False
    if tokens != group * rows_dev or QK_ROPE + 2 * places > 128:
        return False
    return 3 * places * group * rows_dev * model_width * 2 < VMEM_BYTES // 2


def on_device(
    query_plain,
    query_turn,
    latent,
    key_turn,
    latent_norm_scale,
    plain_key_matrix,
    value_matrix,
    residual,
    out_weight,
    ffn_gain,
    gate_weight,
    up_weight,
    down_weight,
    routes,
    route_weights,
):
    if experts_fit(latent.shape[0], *residual.shape):
        return run_whole(
            query_plain,
            query_turn,
            latent,
            key_turn,
            latent_norm_scale,
            plain_key_matrix,
            value_matrix,
            residual,
            out_weight,
            ffn_gain,
            gate_weight[0],
            up_weight[0],
            down_weight[0],
            routes,
            route_weights,
        )
    tok_dev = latent.shape[0]
    heads_dev = query_plain.shape[1] // PLAIN_HEAD_WIDTH
    model_width = residual.shape[1]
    place = lax.axis_index("sp") * tok_dev + jnp.arange(tok_dev, dtype=jnp.int32)
    grid_row = place // GRID_W
    grid_col = place % GRID_W
    rows_dev, model_width = residual.shape
    group = lax.axis_size("tp")
    count = lax.axis_size("sp")
    expert_ids = jnp.arange(count, dtype=jnp.int32)
    share = jnp.sum(
        route_weights[..., None] * (routes[..., None] == expert_ids).astype(jnp.float32), axis=1
    )
    latent_width = latent.shape[1]
    wide = latent_width + QK_ROPE

    def key_side(latents, turns, at_row, at_col):
        normed_latent = norm_scale(latents, latent_norm_scale).astype(jnp.bfloat16)
        key_rot = turn(turns.astype(jnp.float32), at_row, at_col).astype(jnp.bfloat16)
        return [normed_latent, key_rot]

    sent = jnp.concatenate(key_side(latent, key_turn, grid_row, grid_col), axis=1)
    everyone = lax.all_gather(sent, "sp", axis=0, tiled=True)
    shares = lax.all_gather(share, ("sp", "tp"), axis=0, tiled=True)
    own_share = jnp.sum(
        jnp.where(expert_ids[None, :] == lax.axis_index("sp"), shares, 0.0), axis=1, keepdims=True
    )
    all_latent = everyone[:, :latent_width]
    all_rot = everyone[:, latent_width:wide]
    keys = jnp.dot(all_latent, plain_key_matrix, preferred_element_type=jnp.float32).astype(
        jnp.bfloat16
    )
    values = jnp.dot(all_latent, value_matrix, preferred_element_type=jnp.float32).astype(
        jnp.bfloat16
    )
    query_rot = turn(
        query_turn.astype(jnp.float32).reshape(tok_dev, heads_dev, QK_ROPE), grid_row, grid_col
    ).astype(jnp.bfloat16)
    scale = (PLAIN_HEAD_WIDTH + QK_ROPE) ** (-0.5)
    attended = []
    for head in range(heads_dev):
        span = slice(head * PLAIN_HEAD_WIDTH, (head + 1) * PLAIN_HEAD_WIDTH)
        scores = (
            jnp.einsum(
                "qd,kd->qk", query_plain[:, span], keys[:, span], preferred_element_type=jnp.float32
            )
            + jnp.einsum(
                "qd,kd->qk", query_rot[:, head], all_rot, preferred_element_type=jnp.float32
            )
        ) * scale
        weights = jnp.exp(scores - jnp.max(scores, axis=1, keepdims=True))
        summed = jnp.dot(
            weights.astype(jnp.bfloat16),
            values[:, head * VALUE_WIDTH : (head + 1) * VALUE_WIDTH],
            preferred_element_type=jnp.float32,
        )
        attended.append(
            (summed / jnp.sum(weights, axis=1, keepdims=True)).astype(jnp.bfloat16)
        )
    attended = jnp.concatenate(attended, axis=1)
    swapped = lax.all_to_all(
        attended.reshape(group, rows_dev, heads_dev * VALUE_WIDTH),
        "tp",
        split_axis=0,
        concat_axis=0,
        tiled=True,
    )
    own_rows = jnp.transpose(swapped, (1, 0, 2)).reshape(rows_dev, group * heads_dev * VALUE_WIDTH)
    projected = jnp.dot(own_rows, out_weight, preferred_element_type=jnp.float32)
    hidden = (residual.astype(jnp.float32) + projected).astype(jnp.bfloat16)
    normed = norm_scale(hidden, ffn_gain).astype(jnp.bfloat16)
    rows = lax.all_gather(normed, ("sp", "tp"), axis=0, tiled=True)
    active = expert_active(rows, gate_weight[0], up_weight[0])
    product = jnp.dot(active, down_weight[0], preferred_element_type=jnp.float32)
    mixture = lax.psum_scatter(
        (own_share * product).astype(jnp.bfloat16),
        ("sp", "tp"),
        scatter_dimension=0,
        tiled=True,
    )
    return (hidden.astype(jnp.float32) + mixture.astype(jnp.float32)).astype(jnp.bfloat16)


def solution(mesh):
    placed = (
        P(("grp", "sp"), "tp"),
        P(("grp", "sp"), "tp"),
        P(("grp", "sp"), None),
        P(("grp", "sp"), None),
        P(),
        P(None, "tp"),
        P(None, "tp"),
        P(("grp", "sp", "tp"), None),
        P(),
        P(),
        P("sp", None, "tp"),
        P("sp", None, "tp"),
        P("sp", "tp", None),
        P(("grp", "sp", "tp"), None),
        P(("grp", "sp", "tp"), None),
    )
    return jax.shard_map(
        on_device,
        mesh=mesh,
        in_specs=placed,
        out_specs=P(("grp", "sp", "tp"), None),
        check_vma=False,
    )
```
